32 devices in a mesh: sp: 8 (over z, core), tp: 4 (over y, x).
Axes of the slice: x: 2, y: 2, z: 4, core: 2. Of those that a mesh axis runs over, the one named last changes fastest.
Arguments:
- rec_input: bfloat16 [3072, 3072], P('sp', 'tp'), may hold values from -6 to 6
- gate_input: bfloat16 [3072, 3072], P('sp', 'tp'), may hold values from -6 to 6
- conv_weight: bfloat16 [4, 3072], P(None, 'tp'), may hold values from -3 to 3
- decay_wide: bfloat16 [2, 16, 128, 128], P(None, 'tp'), may hold values from -0.5 to 0.5
- decay_narrow: bfloat16 [2, 16, 64, 64], P(None, 'tp'), may hold values from -0.75 to 0.75
- input_wide: bfloat16 [2, 16, 128, 128], P(None, 'tp'), may hold values from -0.5 to 0.5
- input_narrow: bfloat16 [2, 16, 64, 64], P(None, 'tp'), may hold values from -0.75 to 0.75
- decay_base: float32 [2, 3072], P(None, 'tp'), may hold values from 6.510417e-06 to 8.138021e-05
- decay_extra: float32 [2, 3072, 2, 16], P(None, 'sp', None, 'tp'), may hold values from -1 to 0
- tokens: bfloat16 [3072, 2048], P('sp', 'tp'), may hold values from -16 to 16
- out_weight: bfloat16 [3072, 2048], P(None, 'tp'), may hold values from -0.3125 to 0.3125
- norm_gain: float32 [2048], P('tp'), may hold values from 0.1 to 1.9
- shared_gate: bfloat16 [2048, 2048], P(None, 'tp'), may hold values from -0.125 to 0.125
- shared_up: bfloat16 [2048, 2048], P(None, 'tp'), may hold values from -0.125 to 0.125
- shared_down: bfloat16 [2048, 2048], P(None, 'tp'), may hold values from -0.125 to 0.125
- expert_gate: bfloat16 [8, 2048, 2048], P('sp', None, 'tp'), may hold values from -0.125 to 0.125
- expert_up: bfloat16 [8, 2048, 2048], P('sp', None, 'tp'), may hold values from -0.125 to 0.125
- expert_down: bfloat16 [8, 2048, 2048], P('sp', None, 'tp'), may hold values from -0.125 to 0.125
- routes: int32 [3072, 2], P('sp'), may hold values from 0 to 7, all different within a row; in each aligned block of 384 rows (0 to 383, 384 to 767, ...) at most 144 rows name the same one
- route_weight: float32 [3072, 2], P('sp'), may hold values from 0.2 to 1.5
Outputs:
- layer_out: bfloat16 [3072, 2048], P('sp', 'tp')
The draws below stay inside these ranges and needn't reach their ends.
Inputs may be any that keep to these rules, and one draw needn't show every extreme that they name: `routes`: each row names 2 different experts. The rows of one index of sp name no expert more than 144 times, and in some such block one expert exactly 144 times.
All inputs are finite; a program needn't handle non-finite values.
Results may differ from the reference program's by a relative error of at most 0.0052.
Values may be sent and summed in bfloat16 or wider, within the bound.
A program may use at most 64 MiB of HBM per device.

```python
import math
import jax
import jax.numpy as jnp
import numpy as np
from jax import lax

D = 2048
HEADS = 16
HEAD_WIDE = 128
HEAD_NARROW = 64
CONV = 4
FF = 2048
TOP = 2
TOK_DEV = 384
W = 3072
TOKENS = 3072
EXPERTS = 8
CAP = 144
N_SP = 8


def draw_decay_extra(key, part):
    keys = jax.random.split(key, 5)
    slow_share = 0.5
    slow_heads = (jax.random.uniform(keys[0], (2, 1, 2, HEADS)) < slow_share).astype(jnp.float32)
    quick_decay_rate = jax.random.uniform(keys[1], (2, 1, 2, HEADS), minval=0.02, maxval=0.05)
    block_count = TOKENS // TOK_DEV
    block_factor = jnp.exp(jax.random.uniform(keys[2], (2, block_count, 1, 2, HEADS), minval=0.0, maxval=1.1))
    block_factor = jnp.broadcast_to(block_factor, (2, block_count, TOK_DEV, 2, HEADS)).reshape(2, TOKENS, 2, HEADS)
    slow_rate = block_factor * (0.3 / TOKENS)
    surplus_term = -(slow_heads * slow_rate + (1.0 - slow_heads) * quick_decay_rate)
    target_locations = jax.random.randint(keys[3], (3, 2, 1, 2, HEADS), 0, TOKENS)
    extent_list = jnp.log(jax.random.uniform(keys[4], (3, 2, 1, 2, HEADS), minval=0.5, maxval=0.8))
    token_positions = jnp.arange(TOKENS, dtype=jnp.int32)[None, :, None, None]
    for spike_amount in range(3):
        surplus_term = surplus_term + jnp.where(token_positions == target_locations[spike_amount], extent_list[spike_amount], 0.0)
    return surplus_term.astype(jnp.float32)


def draw_tokens(key, part):
    column = jnp.arange(D, dtype=jnp.float32)[None, :]
    scale = 1.0 + 2.0 * column / D
    base = jnp.clip(jax.random.normal(key, (TOKENS, D)), -5.0, 5.0)
    return (base * scale).astype(jnp.bfloat16)


def steps_of(own_key, shape, cuts, smallest, largest):
    factor_of, own = 1.0, jax.random.fold_in(own_key, 6)
    for axis_at, parts in cuts:
        steps = jnp.exp(jax.random.uniform(jax.random.fold_in(own, axis_at), (parts,), jnp.float32, smallest / len(cuts), largest / len(cuts)))
        factor_of = factor_of * jnp.repeat(steps, shape[axis_at] // parts).reshape([-1 if axis == axis_at else 1 for axis in range(len(shape))])
    return factor_of


def assign_block(own_key, own, number, rows, count, top, bound, lean):
    sequence = jax.random.permutation(own_key, count)
    heavy_load, usual = load_shares(count, rows * top, bound, lean, True), load_shares(count, rows * top, bound, lean, False)
    places = jnp.arange(count)

    def named(tallies, turn):
        used = int((tallies > 0).sum())
        fixed = max(1, used // 4)
        moved = fixed + (places - fixed + turn * (used - fixed)) % max(1, count - fixed)
        return jnp.zeros((count,), jnp.int32).at[sequence[jnp.where(places < fixed, places, moved)]].set(jnp.asarray(tallies, jnp.int32))

    tallies = jnp.where(number % 4 == 0, named(heavy_load, number // 4), named(usual, number - number // 4 - 1))
    mixed = jax.random.permutation(jax.random.fold_in(own, 3), count)
    giver, receiver = mixed[0:count // 2 * 2:2], mixed[1:count // 2 * 2:2]
    slack = jnp.minimum(tallies[giver] - 1, bound - tallies[receiver]) // 2
    slack = jnp.where((giver == sequence[0]) | (receiver == sequence[0]) | (tallies[receiver] == 0), 0, jnp.maximum(slack, 0))
    moved = jax.random.randint(jax.random.fold_in(own, 4), (count // 2,), 0, 1 << 20) % (slack + 1)
    tallies = tallies.at[giver].add(-moved).at[receiver].add(moved)
    labels = jnp.searchsorted(jnp.cumsum(tallies), jnp.arange(rows * top), side="right").astype(jnp.int32)
    grid = labels.reshape(top, rows).T
    grid = grid[jax.random.permutation(jax.random.fold_in(own, 1), rows)]
    turn = jax.random.randint(jax.random.fold_in(own, 2), (rows, 1), 0, top)
    return jnp.take_along_axis(grid, (jnp.arange(top)[None, :] + turn) % top, axis=1)


def load_shares(count, total, most, slope, full):
    loads = [(1 << 20) // math.isqrt(standing ** slope) + 1 for standing in range(1, count + 1)]
    largest = most if full else min(most, max(-(-total // count), total * loads[0] // sum(loads)))
    least = 1 if total - largest >= count - 1 else 0
    given, surplus = [largest] + [least] * (count - 1), total - largest - least * (count - 1)
    while surplus > 0:
        free = [i for i in range(1, count) if given[i] < largest] or [i for i in range(1, count) if given[i] < most]
        whole, remaining = sum([loads[i] for i in free]), surplus
        for i in free:
            more = min(most - given[i], max(1, remaining * loads[i] // whole), surplus)
            given[i] = given[i] + more
            surplus = surplus - more
    return np.array(given)


def bell_draw(own_key, extent, deviation, bound, cuts=(), kind=jnp.bfloat16):
    result = deviation * jax.random.normal(own_key, extent, jnp.float32)
    if cuts:
        result = result * steps_of(own_key, extent, cuts, -0.22, 0.18)
    return jnp.clip(result, -bound, bound).astype(kind)


def setup_inputs(seed: int = 0) -> dict:
    arg_keys = jax.random.split(jax.random.key(seed), 21)
    rec_input = bell_draw(arg_keys[0], (TOKENS, W), 1.0, 6.0, ((0, 8), (1, 4)))
    gate_input = bell_draw(arg_keys[1], (TOKENS, W), 1.0, 6.0, ((0, 8), (1, 4)))
    conv_weight = bell_draw(arg_keys[2], (CONV, W), CONV ** -0.5, 3.0, ((1, 4),))
    decay_wide = bell_draw(arg_keys[3], (2, HEADS, HEAD_WIDE, HEAD_WIDE), HEAD_WIDE ** -0.5, 0.5, ((1, 4),))
    decay_narrow = bell_draw(arg_keys[4], (2, HEADS, HEAD_NARROW, HEAD_NARROW), HEAD_NARROW ** -0.5, 0.75, ((1, 4),))
    input_wide = bell_draw(arg_keys[5], (2, HEADS, HEAD_WIDE, HEAD_WIDE), HEAD_WIDE ** -0.5, 0.5, ((1, 4),))
    input_narrow = bell_draw(arg_keys[6], (2, HEADS, HEAD_NARROW, HEAD_NARROW), HEAD_NARROW ** -0.5, 0.75, ((1, 4),))
    decay_base = jnp.clip(jnp.exp(math.log(8.138021075865254e-05) - 2.5257286 * jax.random.uniform(arg_keys[7], (2, W), jnp.float32) ** steps_of(arg_keys[7], (2, W), ((1, 4),), -0.2, 0.2)), 6.510416824312415e-06, 8.138021075865254e-05)
    decay_extra = draw_decay_extra(jax.random.fold_in(arg_keys[20], 71), 0)
    tokens = draw_tokens(jax.random.fold_in(arg_keys[20], 71), 0)
    out_weight = bell_draw(arg_keys[10], (W, D), (W // 9) ** -0.5, 0.3125, ((1, 4),))
    norm_gain = jnp.clip(1.0 + 0.18 * jax.random.normal(arg_keys[11], (D,), jnp.float32), 0.1, 1.9)
    shared_gate = bell_draw(arg_keys[12], (D, FF), D ** -0.5, 0.125, ((1, 4),))
    shared_up = bell_draw(arg_keys[13], (D, FF), D ** -0.5, 0.125, ((1, 4),))
    shared_down = bell_draw(arg_keys[14], (FF, D), FF ** -0.5, 0.125, ((1, 4),))
    expert_gate = bell_draw(arg_keys[15], (EXPERTS, D, FF), D ** -0.5, 0.125, ((0, 8), (2, 4)))
    expert_up = bell_draw(arg_keys[16], (EXPERTS, D, FF), D ** -0.5, 0.125, ((0, 8), (2, 4)))
    expert_down = bell_draw(arg_keys[17], (EXPERTS, FF, D), FF ** -0.5, 0.125, ((0, 8), (2, 4)))
    routes_keys = jax.random.split(jax.random.fold_in(arg_keys[18], 1), TOKENS // TOK_DEV)
    routes_turns = jax.random.permutation(jax.random.fold_in(arg_keys[18], 3), TOKENS // TOK_DEV)
    routes = jax.vmap(lambda own, number: assign_block(jax.random.fold_in(arg_keys[18], 2), own, number, TOK_DEV, EXPERTS, TOP, CAP, 2))(routes_keys, routes_turns).reshape((TOKENS, TOP))
    route_weight = jnp.clip(0.2 + 1.3 * jax.random.uniform(arg_keys[19], (TOKENS, TOP), jnp.float32) ** steps_of(arg_keys[19], (TOKENS, TOP), ((0, 8),), -0.2, 0.2), 0.2, 1.5)
    return {"rec_input": rec_input, "gate_input": gate_input, "conv_weight": conv_weight, "decay_wide": decay_wide, "decay_narrow": decay_narrow, "input_wide": input_wide, "input_narrow": input_narrow, "decay_base": decay_base, "decay_extra": decay_extra, "tokens": tokens, "out_weight": out_weight, "norm_gain": norm_gain, "shared_gate": shared_gate, "shared_up": shared_up, "shared_down": shared_down, "expert_gate": expert_gate, "expert_up": expert_up, "expert_down": expert_down, "routes": routes, "route_weight": route_weight}


NORM_EPS = 1e-06
RATE_SCALE = 8.0

def link(earlier, latter):
    return (earlier[0] * latter[0], latter[0] * earlier[1] + latter[1])

def run_scan(decays, drives, reverse):
    if reverse:
        decays = jnp.flip(decays, 0)
        drives = jnp.flip(drives, 0)
    cumulative, states = lax.associative_scan(link, (decays, drives), axis=0)
    if reverse:
        states = jnp.flip(states, 0)
    return states

def channels_per_head(per_head):
    row_count = per_head.shape[0]
    head_count = per_head.shape[2]
    wide_part = jnp.broadcast_to(per_head[:, 0, :, None], (row_count, head_count, HEAD_WIDE))
    narrow_part = jnp.broadcast_to(per_head[:, 1, :, None], (row_count, head_count, HEAD_NARROW))
    return jnp.concatenate([wide_part, narrow_part], axis=2).reshape(row_count, -1)

def block_gate(grouped, wide_blocks, narrow_blocks):
    wide_in = grouped[:, :, :HEAD_WIDE]
    narrow_in = grouped[:, :, HEAD_WIDE:]
    wide_out = jnp.einsum('thi,hij->thj', wide_in, wide_blocks.astype(jnp.float32))
    narrow_out = jnp.einsum('thi,hij->thj', narrow_in, narrow_blocks.astype(jnp.float32))
    joined = jnp.concatenate([wide_out, narrow_out], axis=2)
    return jax.nn.sigmoid(joined.reshape(grouped.shape[0], -1))

def reference(rec_input, gate_input, conv_weight, decay_wide, decay_narrow, input_wide, input_narrow, decay_base, decay_extra, tokens, out_weight, norm_gain, shared_gate, shared_up, shared_down, expert_gate, expert_up, expert_down, routes, route_weight):
    row_count = rec_input.shape[0]
    padded = jnp.pad(rec_input.astype(jnp.float32), ((2, 1), (0, 0)))
    conv_sum = padded[0:row_count] * conv_weight[0].astype(jnp.float32)
    for tap_index in range(1, CONV):
        conv_sum = conv_sum + padded[tap_index:tap_index + row_count] * conv_weight[tap_index].astype(jnp.float32)
    conv_out = conv_sum.astype(jnp.bfloat16)
    conv_wide = conv_out.astype(jnp.float32)
    grouped = conv_wide.reshape(row_count, HEADS, HEAD_WIDE + HEAD_NARROW)
    summed = jnp.zeros((row_count, W), jnp.float32)
    for direction in range(2):
        rate = block_gate(grouped, decay_wide[direction], decay_narrow[direction])
        admit = block_gate(grouped, input_wide[direction], input_narrow[direction])
        log_decay = -RATE_SCALE * rate * decay_base[direction][None, :] + channels_per_head(decay_extra[direction])
        drives = jnp.sqrt(-jnp.expm1(2.0 * log_decay)) * admit * conv_wide
        summed = summed + run_scan(jnp.exp(log_decay), drives, direction == 1)
    mixed = (summed * jax.nn.gelu(gate_input.astype(jnp.float32))).astype(jnp.bfloat16)
    resid = tokens.astype(jnp.float32) + jnp.dot(mixed, out_weight, preferred_element_type=jnp.float32)
    scale_row = lax.rsqrt(lax.optimization_barrier(jnp.mean(resid * resid, axis=1, keepdims=True)) + NORM_EPS)
    normed = (resid * scale_row * norm_gain[None, :]).astype(jnp.bfloat16)
    shared_expert_hidden = (jax.nn.silu(jnp.dot(normed, shared_gate, preferred_element_type=jnp.float32)) * jnp.dot(normed, shared_up, preferred_element_type=jnp.float32)).astype(jnp.bfloat16)
    shared_out = jnp.dot(shared_expert_hidden, shared_down, preferred_element_type=jnp.float32)
    most_rows = N_SP * CAP

    def expert_step(routed_sum, inputs):
        gate_weights, up_weights, down_weights, expert_id = inputs
        matches = routes == expert_id
        weight_row = lax.optimization_barrier(jnp.sum(jnp.where(matches, route_weight, 0.0), axis=1))
        selected = jnp.any(matches, axis=1)
        row_index = jnp.nonzero(selected, size=most_rows, fill_value=0)[0].astype(jnp.int32)
        live_count = jnp.sum(selected.astype(jnp.int32))
        is_live = jnp.arange(most_rows, dtype=jnp.int32) < live_count
        picked = normed[row_index]
        hidden = (jax.nn.silu(jnp.dot(picked, gate_weights, preferred_element_type=jnp.float32)) * jnp.dot(picked, up_weights, preferred_element_type=jnp.float32)).astype(jnp.bfloat16)
        expert_out = jnp.dot(hidden, down_weights, preferred_element_type=jnp.float32).astype(jnp.bfloat16).astype(jnp.float32)
        weights = jnp.where(is_live, weight_row[row_index], 0.0)
        routed_sum = routed_sum.at[row_index].add(weights[:, None] * expert_out)
        return (routed_sum, None)
    routed_sum, unused = lax.scan(expert_step, jnp.zeros((row_count, D), jnp.float32), (expert_gate, expert_up, expert_down, jnp.arange(EXPERTS, dtype=jnp.int32)))
    return (resid + shared_out + routed_sum).astype(jnp.bfloat16)
```

```python
import functools

import jax
import jax.numpy as jnp
import numpy as np
from jax import lax
from jax.experimental import pallas as pl
from jax.experimental.pallas import tpu as pltpu
from jax.sharding import PartitionSpec as P

MESH = pl.DeviceIdType.MESH
D = 2048
CONV = 4
NORM_EPS = 1e-06
RATE_SCALE = 8.0
SEG = 8
F32 = jnp.float32
BF16 = jnp.bfloat16
EXACT = lax.Precision.HIGHEST


def rcopy(src, dst, send, recv, **where):
    return pltpu.make_async_remote_copy(
        src_ref=src, dst_ref=dst, send_sem=send, recv_sem=recv, device_id=where, device_id_type=MESH
    )


def greet(n_sp, n_tp):
    sp, tp = lax.axis_index("sp"), lax.axis_index("tp")
    barrier = pltpu.get_barrier_semaphore()
    for k in range(1, n_sp):
        pl.semaphore_signal(
            barrier, inc=1, device_id={"sp": lax.rem(sp + k, n_sp)}, device_id_type=MESH
        )
    for k in range(1, n_tp):
        pl.semaphore_signal(
            barrier, inc=1, device_id={"tp": lax.rem(tp + k, n_tp)}, device_id_type=MESH
        )
    pl.semaphore_wait(barrier, n_sp + n_tp - 2)


def gather_sems(n_tp):
    count = 6 if n_tp == 4 else n_tp
    return [pltpu.SemaphoreType.DMA((count,)), pltpu.SemaphoreType.DMA((count,))]


class Gather:
    def __init__(self, n_tp, slot, send, recv, base=0):
        self.n, self.slot, self.send, self.recv, self.base = n_tp, slot, send, recv, base
        self.t = lax.axis_index("tp")
        if n_tp == 4:
            y, x = self.t // 2, lax.rem(self.t, 2)
            self.xn, self.yn, self.dg = y * 2 + 1 - x, (1 - y) * 2 + x, 3 - self.t

    def piece(self, owner, half, sem, to):
        ref = self.slot(owner, half)
        s = self.base + sem
        return rcopy(ref, ref, self.send.at[s], self.recv.at[s], tp=to)

    def start(self):
        if self.n == 4:
            self.piece(self.t, 0, 0, self.xn).start()
            self.piece(self.t, 1, 3, self.yn).start()
            self.piece(self.t, 1, 1, self.xn).start()
            self.piece(self.t, 0, 2, self.yn).start()
        else:
            for k in range(1, self.n):
                to = lax.rem(self.t + k, self.n)
                self.piece(self.t, None, k, to).start()

    def forward(self):
        if self.n == 4:
            self.piece(self.xn, 0, 0, self.xn).wait_recv()
            self.piece(self.xn, 0, 4, self.yn).start()
            self.piece(self.yn, 1, 3, self.yn).wait_recv()
            self.piece(self.yn, 1, 5, self.xn).start()

    def arrivals(self):
        if self.n == 4:
            self.piece(self.xn, 1, 1, self.xn).wait_recv()
            yield self.xn
            self.piece(self.yn, 0, 2, self.yn).wait_recv()
            yield self.yn
            self.piece(self.dg, 0, 4, self.yn).wait_recv()
            self.piece(self.dg, 1, 5, self.xn).wait_recv()
            yield self.dg
        else:
            for k in range(1, self.n):
                owner = lax.rem(self.t - k + self.n, self.n)
                self.piece(owner, None, k, owner).wait_recv()
                yield owner

    def drain(self):
        if self.n == 4:
            for s, half, owner in (
                (0, 0, self.t), (1, 1, self.t), (2, 0, self.t), (3, 1, self.t),
                (4, 0, self.xn), (5, 1, self.yn),
            ):
                self.piece(owner, half, s, self.xn).wait_send()
        else:
            for k in range(1, self.n):
                to = lax.rem(self.t + k, self.n)
                self.piece(self.t, None, k, to).wait_send()


def minus_expm1(y):
    series = 1.0 + y * (1 / 7.0)
    for d in (6.0, 5.0, 4.0, 3.0, 2.0):
        series = 1.0 + y * (1 / d) * series
    return jnp.where(y > -0.3, -y * series, 1.0 - jnp.exp(y))


class Order:
    def __init__(self, n_sp):
        sp = lax.axis_index("sp")
        chip = sp // 2
        self.core, self.low, self.high, self.n = sp % 2, chip % 2, chip // 2, n_sp // 4

    def at(self, p, sign):
        step = p // 4 + 1
        high = (self.high + (step if sign > 0 else 2 * self.n - step)) % self.n
        low = (self.low + 1 + p // 2) % 2
        return (high * 2 + low) * 2 + (self.core + 1 + p) % 2


class Square:
    def __init__(self):
        t, core = lax.axis_index("tp"), lax.axis_index("sp") % 2
        y, x = t // 2, t % 2
        xn, yn = y * 2 + 1 - x, (1 - y) * 2 + x
        flip = core == 1
        self.gather = jnp.where(flip, yn, xn)
        self.reduce = jnp.where(flip, xn, yn)
        self.place = jnp.where(flip, y, x)
        self.mine = (jnp.where(flip, x, 2 * y), jnp.where(flip, 2 + x, 2 * y + 1))
        self.theirs = (jnp.where(flip, 1 - x, 2 - 2 * y), jnp.where(flip, 3 - x, 3 - 2 * y))


def layer_kernel(
    n_sp, n_tp, cap, direct,
    rec, gate, convw, dw, dn, iw, inn, base, extra, spread, tokens, gain, routes, rweight,
    hbm_outw, hbm_sg, hbm_su, hbm_eg, hbm_eu, hbm_ed, hbm_sd,
    out,
    outw, sg, su, eg, eu, ed, sd, permt, perm, wblk, exs,
    halo, cperm, gperm, av, bv, msg, totals, mixedp, mixed, squares, sqown,
    resid, whole, normed, srow, scol, pos, wts, post, wtt,
    outgoing, outwide, rows_in, hidden, own, psend, precv, answer, returned, shid, spsend, sprecv,
    wsem, xsend, xrecv, hsend, hrecv, tsend, trecv, gsend, grecv, ssend, srecv, nsend, nrecv,
    dsend, drecv, asend, arecv, bsend, brecv, psem, prem, rsend, rrecv, csend, crecv, qsend, qrecv,
):
    two = n_tp == 4
    rows, chan = rec.shape
    heads, wide, narrow = dw.shape[1], dw.shape[2], dn.shape[2]
    groups, gw = wblk.shape[1], wblk.shape[2]
    cols = tokens.shape[1]
    ff = eg.shape[1]
    seglen = rows // SEG
    count = 6 if two else n_tp
    n_far = n_sp - direct
    sp, tp = lax.axis_index("sp"), lax.axis_index("tp")
    mine = pl.ds(pl.multiple_of(tp * cols, 128), cols)
    order = Order(n_sp)
    sq = Square() if two else None

    loads = []

    def load(a, b):
        c = pltpu.make_async_copy(a, b, wsem.at[len(loads)])
        c.start()
        loads.append(c)

    def band(i):
        return pl.ds(pl.multiple_of(i * ff, 128), ff)

    load(hbm_outw, outw)
    load(hbm_sg, sg)
    load(hbm_su, su)
    load(hbm_eg, eg)
    load(hbm_eu, eu)
    if two:
        for hbm, vmem in ((hbm_ed, ed), (hbm_sd, sd)):
            for j in range(2):
                load(hbm.at[band(sq.mine[j])], vmem.at[0, pl.ds(j * ff, ff)])
    else:
        load(hbm_ed, ed)
        load(hbm_sd, sd)
    greet(n_sp, n_tp)
    up, down = lax.rem(sp + 1, n_sp), lax.rem(sp + n_sp - 1, n_sp)
    low = rcopy(rec.at[pl.ds(rows - 16, 16)], halo.at[0], hsend.at[0], hrecv.at[0], sp=up)
    high = rcopy(rec.at[pl.ds(0, 16)], halo.at[1], hsend.at[1], hrecv.at[1], sp=down)
    low.start()
    high.start()
    swaps = []
    if two:
        for hbm, vmem in ((hbm_sd, sd), (hbm_ed, ed)):
            for j in range(2):
                i = len(swaps)
                c = rcopy(
                    hbm.at[band(sq.theirs[j])], vmem.at[1, pl.ds(j * ff, ff)],
                    xsend.at[i], xrecv.at[i], tp=sq.reduce,
                )
                c.start()
                swaps.append(c)

    r = lax.broadcasted_iota(jnp.int32, (rows, rows), 0)
    q = lax.broadcasted_iota(jnp.int32, (rows, rows), 1)
    permt[...] = jnp.where((r % SEG) * seglen + r // SEG == q, 1.0, 0.0).astype(BF16)
    perm[...] = jnp.where((q % SEG) * seglen + q // SEG == r, 1.0, 0.0).astype(BF16)
    wblk[...] = jnp.zeros_like(wblk)
    per = heads // groups
    for d in range(2):
        for k, (w, n) in enumerate(((dw, dn), (iw, inn))):
            for h in range(heads):
                a = (h % per) * (wide + narrow)
                b = a + wide
                wblk[2 * d + k, h // per, a:b, a:b] = w[d, h]
                wblk[2 * d + k, h // per, b : b + narrow, b : b + narrow] = n[d, h]
    for d in range(2):
        exs[d] = jnp.dot(
            permt[...].astype(F32), extra[d], precision=EXACT, preferred_element_type=F32
        )
    gperm[...] = jnp.dot(permt[...], gate[...], preferred_element_type=F32).astype(BF16)

    low.wait()
    high.wait()
    x = rec[...].astype(F32)
    taps = convw[...].astype(F32)
    lo = jnp.where(sp > 0, halo[0].astype(F32), 0.0)
    hi = jnp.where(sp < n_sp - 1, halo[1].astype(F32), 0.0)
    padded = jnp.concatenate([lo[14:16], x, hi[0:1]], axis=0)
    conv = padded[0:rows] * taps[0:1, :]
    for j in range(1, CONV):
        conv = conv + padded[j : j + rows] * taps[j : j + 1, :]
    cperm[...] = jnp.dot(
        permt[...], conv.astype(BF16), preferred_element_type=F32
    ).astype(BF16)

    step = 64

    @pl.loop(0, rows // step)
    def _(r):
        at = pl.ds(pl.multiple_of(r * step, step), step)
        for d in range(2):
            ex = jnp.dot(exs[d, at, :], spread[...], precision=EXACT, preferred_element_type=F32)
            for g in range(groups):
                lanes = slice(g * gw, (g + 1) * gw)
                c = cperm[at, lanes]
                rate = jax.nn.sigmoid(jnp.dot(c, wblk[2 * d, g], preferred_element_type=F32))
                admit = jax.nn.sigmoid(jnp.dot(c, wblk[2 * d + 1, g], preferred_element_type=F32))
                ld = -RATE_SCALE * rate * base[d : d + 1, lanes] + ex[:, lanes]
                bv[d, at, lanes] = jnp.sqrt(minus_expm1(2.0 * ld)) * admit * c.astype(F32)
                av[d, at, lanes] = jnp.exp(ld)

    one = jnp.ones((SEG, chan), F32)
    zero = jnp.zeros((SEG, chan), F32)

    def advance(i, carry):
        got = []
        for d in range(2):
            at = pl.ds(pl.multiple_of((i if d == 0 else seglen - 1 - i) * SEG, SEG), SEG)
            a, b = av[d, at, :], bv[d, at, :]
            cum = carry[2 * d] * a
            state = a * carry[2 * d + 1] + b
            av[d, at, :] = cum
            bv[d, at, :] = state
            got += [cum, state]
        return tuple(got)

    ends = lax.fori_loop(0, seglen, advance, (one, zero, one, zero))

    def run(d, entering):
        seq = range(SEG) if d == 0 else range(SEG - 1, -1, -1)
        inside = [None] * SEG
        c = entering
        for s in seq:
            inside[s] = c
            c = ends[2 * d][s : s + 1] * c + ends[2 * d + 1][s : s + 1]
        return jnp.concatenate(inside, axis=0), c

    for d in range(2):
        prod = ends[2 * d][0:1]
        for s in range(1, SEG):
            prod = prod * ends[2 * d][s : s + 1]
        msg[2 * d : 2 * d + 1, :] = prod
        msg[2 * d + 1 : 2 * d + 2, :] = run(d, jnp.zeros((1, chan), F32))[1]
    msg[4:8, :] = jnp.zeros((4, chan), F32)
    sent = []
    for k in range(1, n_sp):
        to = lax.rem(sp + k, n_sp)
        c = rcopy(msg, totals.at[k], tsend.at[k], trecv.at[k], sp=to)
        c.start()
        sent.append(c)

    part = lax.broadcasted_iota(jnp.int32, (n_sp, rows), 0)
    who = jnp.zeros((n_sp, rows), jnp.int32)
    for p in range(n_sp):
        who = jnp.where(part == p, order.at(p, 1), who)
    hit0 = jnp.where(routes[0:1, :] == who, 1.0, 0.0)
    hit1 = jnp.where(routes[1:2, :] == who, 1.0, 0.0)
    earlier = jnp.where(r < q, 1.0, 0.0).astype(BF16)
    slots = jnp.dot((hit0 + hit1).astype(BF16), earlier, preferred_element_type=F32)
    pos[...] = jnp.where(hit0 + hit1 > 0.0, slots, -1.0)
    wts[...] = hit0 * rweight[0:1, :] + hit1 * rweight[1:2, :]
    post[...] = jnp.transpose(pos[...])
    wtt[...] = jnp.transpose(wts[...])

    for c in sent:
        c.wait()
    carries = []
    zrow = jnp.zeros((1, chan), F32)
    c0, c1 = zrow, zrow
    for k in range(n_sp - 1, 0, -1):
        t = totals[k]
        c0 = jnp.where(k <= sp, t[0:1] * c0 + t[1:2], c0)
    for k in range(1, n_sp):
        t = totals[k]
        c1 = jnp.where(k > sp, t[2:3] * c1 + t[3:4], c1)
    for d, c in ((0, c0), (1, c1)):
        inside = run(d, c)[0]
        carries.append(jnp.concatenate([inside, inside], axis=0))

    @pl.loop(0, rows // 16)
    def _(r):
        at = pl.ds(pl.multiple_of(r * 16, 16), 16)
        total = bv[0, at, :] + av[0, at, :] * carries[0]
        total = total + (bv[1, at, :] + av[1, at, :] * carries[1])
        mixedp[at, :] = (total * jax.nn.gelu(gperm[at, :].astype(F32))).astype(BF16)

    mixed[tp] = jnp.dot(perm[...], mixedp[...], preferred_element_type=F32).astype(BF16)

    half = rows // 2

    def mixed_slot(owner, part):
        return mixed.at[owner] if part is None else mixed.at[owner, pl.ds(part * half, half)]

    g = Gather(n_tp, mixed_slot, gsend, grecv)
    g.start()
    resid[...] = tokens[...].astype(F32)

    def project(owner):
        @pl.loop(0, rows // 128)
        def _(r):
            at = pl.ds(pl.multiple_of(r * 128, 128), 128)
            resid[at, :] += jnp.dot(mixed[owner, at, :], outw[owner], preferred_element_type=F32)

    loads[0].wait()
    project(tp)
    g.forward()
    for owner in g.arrivals():
        project(owner)

    whole[:, mine] = (resid[...] * gain[...]).astype(BF16)

    def whole_slot(owner, part):
        lanes = pl.ds(pl.multiple_of(owner * cols, 128), cols)
        at = pl.ds(0, rows) if part is None else pl.ds(part * half, half)
        return whole.at[at, lanes]

    w = Gather(n_tp, whole_slot, nsend, nrecv)
    r2 = resid[...] * resid[...]
    sqown[...] = lax.dot_general(
        jnp.ones((8, cols), F32), r2, (((1,), (1,)), ((), ())),
        precision=EXACT, preferred_element_type=F32,
    )
    sent = []
    for k in range(1, n_tp):
        c = rcopy(sqown, squares.at[k], ssend.at[k], srecv.at[k], tp=lax.rem(tp + k, n_tp))
        c.start()
        sent.append(c)
    w.start()
    g.drain()
    total = sqown[...]
    for k, c in enumerate(sent):
        c.wait()
        total = total + squares[k + 1]
    srow[...] = lax.rsqrt(total / (n_tp * cols) + NORM_EPS)
    scol[...] = lax.dot_general(
        srow[...], jnp.full((8, 128), 0.125, F32), (((0,), (0,)), ((), ())),
        precision=EXACT, preferred_element_type=F32,
    )
    normed[...] = (resid[...] * scol[:, 0:1] * gain[...]).astype(BF16)

    slot = lax.broadcasted_iota(jnp.int32, (cap, rows), 0).astype(F32)

    def chosen(p):
        return jnp.where(pos[pl.ds(p, 1), :] == slot, 1.0, 0.0)

    def far_copy(p, sign):
        return rcopy(
            outgoing.at[p], rows_in.at[p, :, mine], dsend.at[p], drecv.at[p], sp=order.at(p, sign)
        )

    def near_copy(p, sign):
        return rcopy(
            outwide.at[p - n_far], rows_in.at[p], dsend.at[p], drecv.at[p], sp=order.at(p, sign)
        )

    def reply(p):
        return rcopy(answer.at[p], returned.at[p], rsend.at[p], rrecv.at[p], sp=order.at(p, -1))

    @pl.loop(0, n_far)
    def _(p):
        outgoing[p] = jnp.dot(
            chosen(p).astype(BF16), normed[...], preferred_element_type=F32
        ).astype(BF16)
        far_copy(p, 1).start()

    def rows_gather(p):
        def place(owner, part):
            if part is None:
                return rows_in.at[p, :, pl.ds(pl.multiple_of(owner * cols, 128), cols)]
            first = pl.multiple_of(owner * cols + part * (cols // 2), 128)
            return rows_in.at[p, :, pl.ds(first, cols // 2)]

        return Gather(n_tp, place, asend, arecv, base=p * count)

    def begin_rows(p):
        far_copy(p, -1).wait_recv()
        rows_gather(p).start()

    lead = 2
    w.forward()
    for p in range(lead):
        begin_rows(p)
    for owner in w.arrivals():
        pass

    def wide_pick(p):
        hit = chosen(p)
        scale = jnp.sum(hit * srow[0:1, :], axis=1, keepdims=True)
        picked = jnp.dot(hit.astype(BF16), whole[...], preferred_element_type=F32)
        return (picked * scale).astype(BF16)

    @pl.loop(n_far, n_sp - 1)
    def _(p):
        outwide[p - n_far] = wide_pick(p)
        near_copy(p, 1).start()

    rows_in[n_sp - 1] = wide_pick(n_sp - 1)

    if two:
        here = pl.ds(pl.multiple_of(sq.place * ff, 128), ff)

        def give_hidden(p):
            ref = hidden.at[p, :, here]
            return rcopy(ref, ref, bsend.at[p], brecv.at[p], tp=sq.gather)

        def take_hidden(p):
            ref = hidden.at[p, :, pl.ds(pl.multiple_of((1 - sq.place) * ff, 128), ff)]
            return rcopy(ref, ref, bsend.at[p], brecv.at[p], tp=sq.gather)

        def give_part(p):
            return rcopy(psend.at[p], precv.at[p], psem.at[p], prem.at[p], tp=sq.reduce)

        sref = shid.at[:, here]
        sgive = rcopy(sref, sref, csend.at[0], crecv.at[0], tp=sq.gather)
        sref = shid.at[:, pl.ds(pl.multiple_of((1 - sq.place) * ff, 128), ff)]
        stake = rcopy(sref, sref, csend.at[0], crecv.at[0], tp=sq.gather)
        sgivep = rcopy(spsend, sprecv, qsend.at[0], qrecv.at[0], tp=sq.reduce)
    else:
        here = band(tp)

        def shared_place(owner, part):
            return shid.at[:, band(owner)]

        shared = Gather(n_tp, shared_place, csend, crecv)

        def hidden_gather(p):
            def place(owner, part):
                return hidden.at[p, :, band(owner)]

            return Gather(n_tp, place, bsend, brecv, base=p * count)

    loads[1].wait()
    loads[2].wait()

    @pl.loop(0, rows // 128)
    def _(r):
        at = pl.ds(pl.multiple_of(r * 128, 128), 128)
        x = whole[at, :]
        s = scol[at, 0:1]
        g = jnp.dot(x, sg[...], preferred_element_type=F32) * s
        u = jnp.dot(x, su[...], preferred_element_type=F32) * s
        shid[at, here] = (jax.nn.silu(g) * u).astype(BF16)

    if two:
        sgive.start()
    else:
        shared.start()
    w.drain()
    for c in loads[3:]:
        c.wait()
    for c in swaps:
        c.wait()

    def answer_with(p, y):
        @pl.when(p == n_sp - 1)
        def _():
            returned[p] = y

        @pl.when(p < n_sp - 1)
        def _():
            answer[p] = y
            reply(p).start()

    def combine(p):
        @pl.when(p < n_sp - 1)
        def _():
            reply(p).wait_recv()

        lane = lax.broadcasted_iota(jnp.int32, (128, cap), 1).astype(F32)
        which = lax.broadcasted_iota(jnp.int32, (128, n_sp), 1) == p

        @pl.loop(0, rows // 128)
        def _(r):
            at = pl.ds(pl.multiple_of(r * 128, 128), 128)
            where = jnp.sum(jnp.where(which, post[at, :], 0.0), axis=1, keepdims=True)
            weight = jnp.sum(jnp.where(which, wtt[at, :], 0.0), axis=1, keepdims=True)
            hit = jnp.where(where == lane, 1.0, 0.0).astype(BF16)
            resid[at, :] += weight * jnp.dot(hit, returned[p], preferred_element_type=F32)

    back = 4

    @pl.loop(0, n_sp + 3)
    def _(s):
        @pl.when(s + lead < n_far)
        def _():
            begin_rows(s + lead)

        @pl.when(s == 0)
        def _():
            rows_gather(0).forward()

        @pl.when(s + 1 < n_far)
        def _():
            rows_gather(s + 1).forward()

        @pl.when(s < n_sp)
        def _():
            @pl.when(s < n_far)
            def _():
                for _ in rows_gather(s).arrivals():
                    pass

            @pl.when((s >= n_far) & (s < n_sp - 1))
            def _():
                near_copy(s, -1).wait_recv()

            x = rows_in[s]
            g = jnp.dot(x, eg[...], preferred_element_type=F32)
            u = jnp.dot(x, eu[...], preferred_element_type=F32)
            hidden[s, :, here] = (jax.nn.silu(g) * u).astype(BF16)
            if two:
                give_hidden(s).start()
            else:
                hidden_gather(s).start()

        if two:
            @pl.when(s == 1)
            def _():
                stake.wait_recv()

                @pl.loop(0, rows // 128)
                def _(r):
                    at = pl.ds(pl.multiple_of(r * 128, 128), 128)
                    h = shid[at, :]
                    resid[at, :] += jnp.dot(h, sd[0], preferred_element_type=F32)
                    spsend[at, :] = jnp.dot(h, sd[1], preferred_element_type=F32).astype(BF16)

                sgivep.start()

            @pl.when(s == 3)
            def _():
                sgivep.wait_recv()
                resid[...] += sprecv[...].astype(F32)
        else:
            @pl.when(s == 1)
            def _():
                for _ in shared.arrivals():
                    pass

                @pl.loop(0, rows // 128)
                def _(r):
                    at = pl.ds(pl.multiple_of(r * 128, 128), 128)
                    resid[at, :] += jnp.dot(shid[at, :], sd[...], preferred_element_type=F32)

        @pl.when((s >= 1) & (s < n_sp + 1))
        def _():
            p = s - 1
            if two:
                take_hidden(p).wait_recv()
                h = hidden[p]
                psend[p] = jnp.dot(h, ed[1], preferred_element_type=F32).astype(BF16)
                give_part(p).start()
                own[p] = jnp.dot(h, ed[0], preferred_element_type=F32)
            else:
                for _ in hidden_gather(p).arrivals():
                    pass
                answer_with(
                    p, jnp.dot(hidden[p], ed[...], preferred_element_type=F32).astype(BF16)
                )

        if two:
            @pl.when((s >= 2) & (s < n_sp + 2))
            def _():
                p = s - 2
                give_part(p).wait_recv()
                answer_with(p, (own[p] + precv[p].astype(F32)).astype(BF16))

        @pl.when(s >= back)
        def _():
            combine(s - back)

    @pl.loop(n_sp + 3 - back, n_sp)
    def _(p):
        combine(p)

    out[...] = resid[...].astype(BF16)

    if two:
        sgive.wait_send()
        sgivep.wait_send()
    else:
        shared.drain()

    @pl.loop(0, n_sp)
    def _(p):
        if two:
            give_hidden(p).wait_send()
            give_part(p).wait_send()
        else:
            hidden_gather(p).drain()

        @pl.when(p < n_far)
        def _():
            rows_gather(p).drain()
            far_copy(p, 1).wait_send()

        @pl.when((p >= n_far) & (p < n_sp - 1))
        def _():
            near_copy(p, 1).wait_send()

        @pl.when(p < n_sp - 1)
        def _():
            reply(p).wait_send()


def shards(
    rec_input,
    gate_input,
    conv_weight,
    decay_wide,
    decay_narrow,
    input_wide,
    input_narrow,
    decay_base,
    decay_extra,
    tokens,
    out_weight,
    norm_gain,
    shared_gate,
    shared_up,
    shared_down,
    expert_gate,
    expert_up,
    expert_down,
    routes,
    route_weight,
):
    n_sp, n_tp = lax.axis_size("sp"), lax.axis_size("tp")
    rows, chan = rec_input.shape
    heads, wide, narrow = decay_wide.shape[1], decay_wide.shape[2], decay_narrow.shape[2]
    cols = tokens.shape[1]
    ff = shared_gate.shape[1]
    per = 2 if heads % 2 == 0 else 1
    hw = wide + narrow
    groups, gw = heads // per, per * hw
    cap = 3 * rows * routes.shape[1] // (2 * n_sp)
    direct = 4
    n_far = n_sp - direct
    two = n_tp == 4
    ex = decay_extra.reshape(2, rows, 2 * heads)
    c = np.arange(chan)
    which = (c % hw >= wide) * heads + c // hw
    spread = jnp.asarray((which[None, :] == np.arange(2 * heads)[:, None]).astype(np.float32))
    vm = pl.BlockSpec(memory_space=pltpu.VMEM)
    hbm = pl.BlockSpec(memory_space=pl.ANY)
    sem = pltpu.SemaphoreType.DMA
    count = 6 if two else n_tp
    down = (2, 2 * ff, cols) if two else (n_tp * ff, cols)
    hid = 2 * ff if two else n_tp * ff
    V = pltpu.VMEM
    pairs = [(4,), (2,), (n_sp,), (count,), (n_tp,), (count,), (n_sp,), (n_sp * count,)]
    pairs += [(n_sp,) if two else (n_sp * count,), (n_sp,), (n_sp,), (1,) if two else (count,), (1,)]
    return pl.pallas_call(
        functools.partial(layer_kernel, n_sp, n_tp, cap, direct),
        name="layer",
        out_shape=jax.ShapeDtypeStruct((rows, cols), BF16),
        in_specs=[vm] * 14 + [hbm] * 7,
        out_specs=vm,
        scratch_shapes=[
            V((n_tp, chan, cols), BF16), V(shared_gate.shape, BF16), V(shared_up.shape, BF16),
            V(expert_gate.shape[1:], BF16), V(expert_up.shape[1:], BF16), V(down, BF16), V(down, BF16),
            V((rows, rows), BF16), V((rows, rows), BF16), V((4, groups, gw, gw), BF16),
            V((2, rows, 2 * heads), F32),
            V((2, 16, chan), BF16), V((rows, chan), BF16), V((rows, chan), BF16),
            V((2, rows, chan), F32), V((2, rows, chan), F32),
            V((8, chan), F32), V((n_sp, 8, chan), F32), V((rows, chan), BF16),
            V((n_tp, rows, chan), BF16), V((n_tp, 8, rows), F32), V((8, rows), F32),
            V((rows, cols), F32), V((rows, n_tp * cols), BF16), V((rows, cols), BF16),
            V((8, rows), F32), V((rows, 128), F32),
            V((n_sp, rows), F32), V((n_sp, rows), F32), V((rows, n_sp), F32), V((rows, n_sp), F32),
            V((n_far, cap, cols), BF16), V((direct - 1, cap, n_tp * cols), BF16),
            V((n_sp, cap, n_tp * cols), BF16), V((n_sp, cap, hid), BF16),
            V((n_sp, cap, cols), F32), V((n_sp, cap, cols), BF16), V((n_sp, cap, cols), BF16),
            V((n_sp, cap, cols), BF16), V((n_sp, cap, cols), BF16),
            V((rows, hid), BF16), V((rows, cols), BF16), V((rows, cols), BF16),
            sem((9,)),
        ] + [sem(s) for s in pairs for _ in range(2)],
        compiler_params=pltpu.CompilerParams(
            collective_id=0, has_side_effects=True, vmem_limit_bytes=60 * 1024 * 1024
        ),
    )(
        rec_input, gate_input, conv_weight, decay_wide, decay_narrow, input_wide, input_narrow,
        decay_base, ex, spread, tokens, norm_gain.reshape(1, cols), routes.T, route_weight.T,
        out_weight.reshape(n_tp, chan, cols), shared_gate, shared_up, expert_gate[0], expert_up[0],
        expert_down[0], shared_down,
    )


def solution(mesh):
    placed = (
        P("sp", "tp"),
        P("sp", "tp"),
        P(None, "tp"),
        P(None, "tp", None, None),
        P(None, "tp", None, None),
        P(None, "tp", None, None),
        P(None, "tp", None, None),
        P(None, "tp"),
        P(None, "sp", None, "tp"),
        P("sp", "tp"),
        P(None, "tp"),
        P("tp"),
        P(None, "tp"),
        P(None, "tp"),
        P(None, "tp"),
        P("sp", None, "tp"),
        P("sp", None, "tp"),
        P("sp", None, "tp"),
        P("sp", None),
        P("sp", None),
    )
    return jax.shard_map(
        shards, mesh=mesh, in_specs=placed, out_specs=P("sp", "tp"), check_vma=False
    )
```

```python
import functools

import jax
import jax.numpy as jnp
from jax import lax
from jax.experimental import pallas as pl
from jax.experimental.pallas import tpu as pltpu
from jax.sharding import PartitionSpec as P

MESH = pl.DeviceIdType.MESH
D = 2048
CONV = 4
NORM_EPS = 1e-06
RATE_SCALE = 8.0
SEG = 8
F32 = jnp.float32
BF16 = jnp.bfloat16
EXACT = lax.Precision.HIGHEST


def rcopy(src, dst, send, recv, **where):
    return pltpu.make_async_remote_copy(
        src_ref=src, dst_ref=dst, send_sem=send, recv_sem=recv, device_id=where, device_id_type=MESH
    )


def hello(n_sp, n_tp):
    sp, tp = lax.axis_index("sp"), lax.axis_index("tp")
    barrier = pltpu.get_barrier_semaphore()
    for k in range(1, n_sp):
        pl.semaphore_signal(
            barrier, inc=1, device_id={"sp": lax.rem(sp + k, n_sp)}, device_id_type=MESH
        )
    for k in range(1, n_tp):
        pl.semaphore_signal(
            barrier, inc=1, device_id={"tp": lax.rem(tp + k, n_tp)}, device_id_type=MESH
        )


def met(n_sp, n_tp):
    pl.semaphore_wait(pltpu.get_barrier_semaphore(), n_sp + n_tp - 2)


def gather_sems(n_tp):
    count = 6 if n_tp == 4 else n_tp
    return [pltpu.SemaphoreType.DMA((count,)), pltpu.SemaphoreType.DMA((count,))]


class Gather:
    def __init__(self, n_tp, slot, send, recv, base=0):
        self.n, self.slot, self.send, self.recv, self.base = n_tp, slot, send, recv, base
        self.t = lax.axis_index("tp")
        if n_tp == 4:
            y, x = self.t // 2, lax.rem(self.t, 2)
            self.xn, self.yn, self.dg = y * 2 + 1 - x, (1 - y) * 2 + x, 3 - self.t

    def piece(self, owner, half, sem, to):
        ref = self.slot(owner, half)
        s = self.base + sem
        return rcopy(ref, ref, self.send.at[s], self.recv.at[s], tp=to)

    def start(self):
        if self.n == 4:
            self.piece(self.t, 0, 0, self.xn).start()
            self.piece(self.t, 1, 3, self.yn).start()
            self.piece(self.t, 1, 1, self.xn).start()
            self.piece(self.t, 0, 2, self.yn).start()
        else:
            for k in range(1, self.n):
                to = lax.rem(self.t + k, self.n)
                self.piece(self.t, None, k, to).start()

    def forward(self):
        if self.n == 4:
            self.piece(self.xn, 0, 0, self.xn).wait_recv()
            self.piece(self.xn, 0, 4, self.yn).start()
            self.piece(self.yn, 1, 3, self.yn).wait_recv()
            self.piece(self.yn, 1, 5, self.xn).start()

    def arrivals(self):
        if self.n == 4:
            self.piece(self.xn, 1, 1, self.xn).wait_recv()
            yield self.xn
            self.piece(self.yn, 0, 2, self.yn).wait_recv()
            yield self.yn
            self.piece(self.dg, 0, 4, self.yn).wait_recv()
            self.piece(self.dg, 1, 5, self.xn).wait_recv()
            yield self.dg
        else:
            for k in range(1, self.n):
                owner = lax.rem(self.t - k + self.n, self.n)
                self.piece(owner, None, k, owner).wait_recv()
                yield owner

    def drain(self):
        if self.n == 4:
            for s, half, owner in (
                (0, 0, self.t), (1, 1, self.t), (2, 0, self.t), (3, 1, self.t),
                (4, 0, self.xn), (5, 1, self.yn),
            ):
                self.piece(owner, half, s, self.xn).wait_send()
        else:
            for k in range(1, self.n):
                to = lax.rem(self.t + k, self.n)
                self.piece(self.t, None, k, to).wait_send()


def logistic(x):
    return 0.5 * jnp.tanh(0.5 * x) + 0.5


class Order:
    def __init__(self, n_sp):
        sp = lax.axis_index("sp")
        chip = sp // 2
        self.core, self.low, self.high, self.n = sp % 2, chip % 2, chip // 2, n_sp // 4

    def at(self, p, sign):
        step = p // 4 + 1
        high = (self.high + (step if sign > 0 else 2 * self.n - step)) % self.n
        low = (self.low + 1 + p // 2) % 2
        return (high * 2 + low) * 2 + (self.core + 1 + p) % 2


class Square:
    def __init__(self):
        t, core = lax.axis_index("tp"), lax.axis_index("sp") % 2
        y, x = t // 2, t % 2
        xn, yn = y * 2 + 1 - x, (1 - y) * 2 + x
        flip = core == 1
        self.gather = jnp.where(flip, yn, xn)
        self.reduce = jnp.where(flip, xn, yn)
        self.place = jnp.where(flip, y, x)
        self.mine = (jnp.where(flip, x, 2 * y), jnp.where(flip, 2 + x, 2 * y + 1))
        self.theirs = (jnp.where(flip, 1 - x, 2 - 2 * y), jnp.where(flip, 3 - x, 3 - 2 * y))


def layer_kernel(
    n_sp, n_tp, cap, direct,
    h_rec, h_gate, h_convw, h_dw, h_dn, h_iw, h_inn, h_base, h_extra, h_tokens, h_gain, h_routes,
    h_rweight, hbm_outw, hbm_sg, hbm_su, hbm_eg, hbm_eu, hbm_ed, hbm_sd,
    out,
    rec, gate, convw, dw, dn, iw, inn, base, extra, tokens, gain, routes, rweight,
    outw, sg, su, eg, eu, ed, sd, permt, perm, wblk, exs,
    halo, cperm, gperm, av, bv, msg, totals, mixedp, mixed, squares, sqown,
    resid, whole, srow, scol, smsg, sgot, pos, wts, post, wtt,
    outgoing, outwide, rows_in, hidden, own, psend, precv, answer, returned, shid,
    isem, wsem, xsend, xrecv, hsend, hrecv, tsend, trecv, gsend, grecv, ssend, srecv, nsend, nrecv,
    dsend, drecv, asend, arecv, bsend, brecv, psem, prem, rsend, rrecv, csend, crecv, lsend, lrecv,
):
    two = n_tp == 4
    rows, chan = rec.shape
    heads, wide, narrow = dw.shape[1], dw.shape[2], dn.shape[2]
    groups, gw = wblk.shape[1], wblk.shape[2]
    cols = tokens.shape[1]
    ff = eg.shape[1]
    seglen = rows // SEG
    count = 6 if two else n_tp
    n_far = n_sp - direct
    sp, tp = lax.axis_index("sp"), lax.axis_index("tp")
    mine = pl.ds(pl.multiple_of(tp * cols, 128), cols)
    order = Order(n_sp)
    sq = Square() if two else None

    loads = []

    def load(a, b):
        c = pltpu.make_async_copy(a, b, wsem.at[len(loads)])
        c.start()
        loads.append(c)

    def band(i):
        return pl.ds(pl.multiple_of(i * ff, 128), ff)

    ready = []
    for i, (a, b) in enumerate((
        (h_rec, rec), (h_convw, convw), (h_extra, extra), (h_gate, gate), (h_dw, dw), (h_dn, dn),
        (h_iw, iw), (h_inn, inn), (h_base, base), (h_tokens, tokens), (h_gain, gain),
        (h_routes, routes), (h_rweight, rweight),
    )):
        c = pltpu.make_async_copy(a, b, isem.at[i])
        c.start()
        ready.append(c)
    hello(n_sp, n_tp)
    load(hbm_outw, outw)
    load(hbm_sg, sg)
    load(hbm_su, su)
    load(hbm_eg, eg)
    load(hbm_eu, eu)
    load(hbm_sd, sd)
    if two:
        for j in range(2):
            load(hbm_ed.at[band(sq.mine[j])], ed.at[0, pl.ds(j * ff, ff)])
    else:
        load(hbm_ed, ed)
    ready[0].wait()
    met(n_sp, n_tp)
    up, down = lax.rem(sp + 1, n_sp), lax.rem(sp + n_sp - 1, n_sp)
    low = rcopy(rec.at[pl.ds(rows - 16, 16)], halo.at[0], hsend.at[0], hrecv.at[0], sp=up)
    high = rcopy(rec.at[pl.ds(0, 16)], halo.at[1], hsend.at[1], hrecv.at[1], sp=down)
    low.start()
    high.start()
    swaps = []
    if two:
        for j in range(2):
            c = rcopy(
                hbm_ed.at[band(sq.theirs[j])], ed.at[1, pl.ds(j * ff, ff)],
                xsend.at[j], xrecv.at[j], tp=sq.reduce,
            )
            c.start()
            swaps.append(c)
    for c in ready[1:]:
        c.wait()

    r = lax.broadcasted_iota(jnp.int32, (rows, rows), 0)
    q = lax.broadcasted_iota(jnp.int32, (rows, rows), 1)
    permt[...] = jnp.where((r % SEG) * seglen + r // SEG == q, 1.0, 0.0).astype(BF16)
    perm[...] = jnp.where((q % SEG) * seglen + q // SEG == r, 1.0, 0.0).astype(BF16)
    wblk[...] = jnp.zeros_like(wblk)
    per = heads // groups
    for d in range(2):
        for k, (w, n) in enumerate(((dw, dn), (iw, inn))):
            for h in range(heads):
                a = (h % per) * (wide + narrow)
                b = a + wide
                wblk[2 * d + k, h // per, a:b, a:b] = w[d, h]
                wblk[2 * d + k, h // per, b : b + narrow, b : b + narrow] = n[d, h]
    for d in range(2):
        left, terms = extra[d], []
        for _ in range(3):
            terms.append(left.astype(BF16))
            left = left - terms[-1].astype(F32)
        exs[d] = jnp.dot(
            permt[...], jnp.concatenate(terms, axis=1), preferred_element_type=F32
        ).astype(BF16)
    gperm[...] = jnp.dot(permt[...], gate[...], preferred_element_type=F32).astype(BF16)

    low.wait()
    high.wait()
    x = rec[...].astype(F32)
    taps = convw[...].astype(F32)
    lo = jnp.where(sp > 0, halo[0].astype(F32), 0.0)
    hi = jnp.where(sp < n_sp - 1, halo[1].astype(F32), 0.0)
    padded = jnp.concatenate([lo[14:16], x, hi[0:1]], axis=0)
    conv = padded[0:rows] * taps[0:1, :]
    for j in range(1, CONV):
        conv = conv + padded[j : j + rows] * taps[j : j + 1, :]
    cperm[...] = jnp.dot(
        permt[...], conv.astype(BF16), preferred_element_type=F32
    ).astype(BF16)

    hw = wide + narrow
    ch = lax.broadcasted_iota(jnp.int32, (6 * heads, chan), 1)
    head, within = ch // hw, ch % hw
    term = lax.broadcasted_iota(jnp.int32, (6 * heads, chan), 0) % (2 * heads)
    spread = jnp.where(term == jnp.where(within >= wide, heads, 0) + head, 1.0, 0.0).astype(BF16)
    step = rows // 2

    @pl.loop(0, rows // step)
    def _(r):
        at = pl.ds(pl.multiple_of(r * step, step), step)
        for d in range(2):
            ex = jnp.dot(exs[d, at, :], spread, preferred_element_type=F32)
            for g in range(groups):
                lanes = slice(g * gw, (g + 1) * gw)
                c = cperm[at, lanes]
                rate = logistic(jnp.dot(c, wblk[2 * d, g], preferred_element_type=F32))
                admit = logistic(jnp.dot(c, wblk[2 * d + 1, g], preferred_element_type=F32))
                ld = jnp.minimum(ex[:, lanes] - rate * (RATE_SCALE * base[d : d + 1, lanes]), 0.0)
                a = jnp.exp(ld)
                bv[d, at, lanes] = jnp.sqrt(jnp.tanh(-ld) * (1.0 + a * a)) * admit * c.astype(F32)
                av[d, at, lanes] = a

    one = jnp.ones((SEG, chan), F32)
    zero = jnp.zeros((SEG, chan), F32)

    def advance(i, carry):
        got = []
        for d in range(2):
            at = pl.ds(pl.multiple_of((i if d == 0 else seglen - 1 - i) * SEG, SEG), SEG)
            a, b = av[d, at, :], bv[d, at, :]
            cum = carry[2 * d] * a
            state = a * carry[2 * d + 1] + b
            av[d, at, :] = cum
            bv[d, at, :] = state
            got += [cum, state]
        return tuple(got)

    ends = lax.fori_loop(0, seglen, advance, (one, zero, one, zero))

    def run(d, entering):
        seq = range(SEG) if d == 0 else range(SEG - 1, -1, -1)
        inside = [None] * SEG
        c = entering
        for s in seq:
            inside[s] = c
            c = ends[2 * d][s : s + 1] * c + ends[2 * d + 1][s : s + 1]
        return jnp.concatenate(inside, axis=0), c

    for d in range(2):
        prod = ends[2 * d][0:1]
        for s in range(1, SEG):
            prod = prod * ends[2 * d][s : s + 1]
        msg[d, 0:1, :] = prod
        msg[d, 1:2, :] = run(d, jnp.zeros((1, chan), F32))[1]
    sent = []
    for k in range(1, n_sp):
        to = lax.rem(sp + k, n_sp)
        c = rcopy(
            msg.at[jnp.where(to > sp, 0, 1)], totals.at[k], tsend.at[k], trecv.at[k], sp=to
        )
        c.start()
        sent.append(c)

    part = lax.broadcasted_iota(jnp.int32, (n_sp, rows), 0)
    who = jnp.zeros((n_sp, rows), jnp.int32)
    for p in range(n_sp):
        who = jnp.where(part == p, order.at(p, 1), who)
    hit0 = jnp.where(routes[0:1, :] == who, 1.0, 0.0)
    hit1 = jnp.where(routes[1:2, :] == who, 1.0, 0.0)
    earlier = jnp.where(r < q, 1.0, 0.0).astype(BF16)
    slots = jnp.dot((hit0 + hit1).astype(BF16), earlier, preferred_element_type=F32)
    pos[...] = jnp.where(hit0 + hit1 > 0.0, slots, -1.0)
    wts[...] = hit0 * rweight[0:1, :] + hit1 * rweight[1:2, :]
    post[...] = jnp.transpose(pos[...])
    wtt[...] = jnp.transpose(wts[...])

    for c in sent:
        c.wait()
    carries = []
    zrow = jnp.zeros((1, chan), F32)
    c0, c1 = zrow, zrow
    for k in range(n_sp - 1, 0, -1):
        t = totals[k]
        c0 = jnp.where(k <= sp, t[0:1] * c0 + t[1:2], c0)
    for k in range(1, n_sp):
        t = totals[k]
        c1 = jnp.where(k > sp, t[0:1] * c1 + t[1:2], c1)
    for d, c in ((0, c0), (1, c1)):
        inside = run(d, c)[0]
        carries.append(jnp.concatenate([inside, inside], axis=0))

    @pl.loop(0, rows // 16)
    def _(r):
        at = pl.ds(pl.multiple_of(r * 16, 16), 16)
        total = bv[0, at, :] + av[0, at, :] * carries[0]
        total = total + (bv[1, at, :] + av[1, at, :] * carries[1])
        mixedp[at, :] = (total * jax.nn.gelu(gperm[at, :].astype(F32))).astype(BF16)

    mixed[tp] = jnp.dot(perm[...], mixedp[...], preferred_element_type=F32).astype(BF16)

    half, quarter = rows // 2, rows // 4

    def rows_of(i, part):
        return pl.ds(i * half, half) if part is None else pl.ds(i * half + part * quarter, quarter)

    def mixed_slot(i):
        return lambda owner, part: mixed.at[owner, rows_of(i, part)]

    def whole_slot(i):
        return lambda owner, part: whole.at[
            rows_of(i, part), pl.ds(pl.multiple_of(owner * cols, 128), cols)
        ]

    g = [Gather(n_tp, mixed_slot(i), gsend, grecv, base=i * count) for i in range(2)]
    w = [Gather(n_tp, whole_slot(i), nsend, nrecv, base=i * count) for i in range(2)]

    def project(owner, i):
        at = pl.ds(i * half, half)
        resid[at, :] += jnp.dot(mixed[owner, at, :], outw[owner], preferred_element_type=F32)

    def publish(i):
        at = pl.ds(i * half, half)
        whole[at, mine] = (resid[at, :] * gain[...]).astype(BF16)

    g[0].start()
    resid[...] = tokens[...].astype(F32)
    loads[0].wait()
    project(tp, 0)
    project(tp, 1)
    g[0].forward()
    g[1].start()
    for owner in g[0].arrivals():
        project(owner, 0)
    publish(0)
    g[1].forward()
    w[0].start()
    for owner in g[1].arrivals():
        project(owner, 1)
    publish(1)
    w[0].forward()
    r2 = resid[...] * resid[...]
    sqown[...] = lax.dot_general(
        jnp.ones((8, cols), F32), r2, (((1,), (1,)), ((), ())),
        precision=EXACT, preferred_element_type=F32,
    )
    sent = []
    for k in range(1, n_tp):
        c = rcopy(sqown, squares.at[k], ssend.at[k], srecv.at[k], tp=lax.rem(tp + k, n_tp))
        c.start()
        sent.append(c)
    w[1].start()

    slot = lax.broadcasted_iota(jnp.int32, (cap, rows), 0).astype(F32)

    def chosen(p):
        return jnp.where(pos[pl.ds(p, 1), :] == slot, 1.0, 0.0)

    def far_copy(p, sign):
        return rcopy(
            outgoing.at[p], rows_in.at[p, :, mine], dsend.at[p], drecv.at[p], sp=order.at(p, sign)
        )

    def near_copy(p, sign):
        return rcopy(
            outwide.at[p - n_far], rows_in.at[p], dsend.at[p], drecv.at[p], sp=order.at(p, sign)
        )

    def reply(p):
        return rcopy(answer.at[p], returned.at[p], rsend.at[p], rrecv.at[p], sp=order.at(p, -1))

    def scale_copy(p, sign):
        return rcopy(smsg.at[p], sgot.at[p], lsend.at[p], lrecv.at[p], sp=order.at(p, sign))

    def dispatch(p):
        outgoing[p] = jnp.dot(
            chosen(p).astype(BF16), whole[:, mine], preferred_element_type=F32
        ).astype(BF16)
        far_copy(p, 1).start()

    dispatch(0)
    total = sqown[...]
    for k, c in enumerate(sent):
        c.wait()
        total = total + squares[k + 1]
    srow[...] = lax.rsqrt(total / (n_tp * cols) + NORM_EPS)

    def scales(p):
        return lax.dot_general(
            srow[...], chosen(p), (((1,), (1,)), ((), ())),
            precision=EXACT, preferred_element_type=F32,
        )

    @pl.loop(0, n_sp - 1)
    def _(p):
        smsg[p] = scales(p)
        scale_copy(p, 1).start()

    sgot[n_sp - 1] = scales(n_sp - 1)

    @pl.loop(1, n_far)
    def _(p):
        dispatch(p)

    scol[...] = lax.dot_general(
        srow[...], jnp.full((8, 128), 0.125, F32), (((0,), (0,)), ((), ())),
        precision=EXACT, preferred_element_type=F32,
    )
    for i in range(2):
        g[i].drain()

    def rows_gather(p):
        def place(owner, part):
            if part is None:
                return rows_in.at[p, :, pl.ds(pl.multiple_of(owner * cols, 128), cols)]
            first = pl.multiple_of(owner * cols + part * (cols // 2), 128)
            return rows_in.at[p, :, pl.ds(first, cols // 2)]

        return Gather(n_tp, place, asend, arecv, base=p * count)

    def begin_rows(p):
        far_copy(p, -1).wait_recv()
        rows_gather(p).start()

    w[1].forward()
    begin_rows(0)
    for i in range(2):
        for owner in w[i].arrivals():
            pass

    def wide_pick(p):
        return jnp.dot(
            chosen(p).astype(BF16), whole[...], preferred_element_type=F32
        ).astype(BF16)

    @pl.loop(0, direct - 1)
    def _(i):
        p = n_sp - 2 - i
        outwide[p - n_far] = wide_pick(p)
        near_copy(p, 1).start()

    rows_in[n_sp - 1] = wide_pick(n_sp - 1)

    if two:
        here = pl.ds(pl.multiple_of(sq.place * ff, 128), ff)

        def give_hidden(p):
            ref = hidden.at[p, :, here]
            return rcopy(ref, ref, bsend.at[p], brecv.at[p], tp=sq.gather)

        def take_hidden(p):
            ref = hidden.at[p, :, pl.ds(pl.multiple_of((1 - sq.place) * ff, 128), ff)]
            return rcopy(ref, ref, bsend.at[p], brecv.at[p], tp=sq.gather)

        def give_part(p):
            return rcopy(psend.at[p], precv.at[p], psem.at[p], prem.at[p], tp=sq.reduce)

    else:
        here = band(tp)

        def hidden_gather(p):
            def place(owner, part):
                return hidden.at[p, :, band(owner)]

            return Gather(n_tp, place, bsend, brecv, base=p * count)

    def shared_place(owner, part):
        if part is None:
            return shid.at[:, band(owner)]
        return shid.at[:, pl.ds(pl.multiple_of(owner * ff + part * (ff // 2), 128), ff // 2)]

    shared = Gather(n_tp, shared_place, csend, crecv)
    loads[1].wait()
    loads[2].wait()

    @pl.loop(0, rows // 128)
    def _(r):
        at = pl.ds(pl.multiple_of(r * 128, 128), 128)
        x = whole[at, :]
        s = scol[at, 0:1]
        g = jnp.dot(x, sg[...], preferred_element_type=F32) * s
        u = jnp.dot(x, su[...], preferred_element_type=F32) * s
        shid[at, band(tp)] = (jax.nn.silu(g) * u).astype(BF16)

    shared.start()
    for i in range(2):
        w[i].drain()
    for c in loads[3:]:
        c.wait()
    for c in swaps:
        c.wait()

    def answer_with(p, y):
        @pl.when(p == n_sp - 1)
        def _():
            returned[p] = y

        @pl.when(p < n_sp - 1)
        def _():
            answer[p] = y
            reply(p).start()

    def combine(p):
        @pl.when(p < n_sp - 1)
        def _():
            reply(p).wait_recv()

        lane = lax.broadcasted_iota(jnp.int32, (128, cap), 1).astype(F32)
        which = lax.broadcasted_iota(jnp.int32, (128, n_sp), 1) == p

        @pl.loop(0, rows // 128)
        def _(r):
            at = pl.ds(pl.multiple_of(r * 128, 128), 128)
            where = jnp.sum(jnp.where(which, post[at, :], 0.0), axis=1, keepdims=True)
            weight = jnp.sum(jnp.where(which, wtt[at, :], 0.0), axis=1, keepdims=True)
            hit = jnp.where(where == lane, 1.0, 0.0).astype(BF16)
            resid[at, :] += weight * jnp.dot(hit, returned[p], preferred_element_type=F32)

    def turn(s):
        return jnp.where(s == 0, n_sp - 2, jnp.where(s == n_sp - 1, n_sp - 1, s - 1))

    back = 4

    @pl.loop(0, n_sp + 3)
    def _(s):
        @pl.when(s < n_sp)
        def _():
            p = turn(s)

            @pl.when(p < n_far)
            def _():
                for _ in rows_gather(p).arrivals():
                    pass

            @pl.when((p >= n_far) & (p < n_sp - 1))
            def _():
                near_copy(p, -1).wait_recv()

            @pl.when(p < n_sp - 1)
            def _():
                scale_copy(p, -1).wait_recv()

            scale = lax.dot_general(
                sgot[p], jnp.full((8, 128), 0.125, F32), (((0,), (0,)), ((), ())),
                precision=EXACT, preferred_element_type=F32,
            )[:, 0:1]
            x = rows_in[p]
            g = jnp.dot(x, eg[...], preferred_element_type=F32) * scale
            u = jnp.dot(x, eu[...], preferred_element_type=F32) * scale
            hidden[p, :, here] = (jax.nn.silu(g) * u).astype(BF16)
            if two:
                give_hidden(p).start()
            else:
                hidden_gather(p).start()

        @pl.when(s < n_far)
        def _():
            rows_gather(s).forward()

        @pl.when(s == 0)
        def _():
            shared.forward()

        @pl.when((s >= 1) & (s < n_sp + 1))
        def _():
            p = turn(s - 1)
            if two:
                take_hidden(p).wait_recv()
                h = hidden[p]
                psend[p] = jnp.dot(h, ed[1], preferred_element_type=F32).astype(BF16)
                give_part(p).start()
                own[p] = jnp.dot(h, ed[0], preferred_element_type=F32)
            else:
                for _ in hidden_gather(p).arrivals():
                    pass
                answer_with(
                    p, jnp.dot(hidden[p], ed[...], preferred_element_type=F32).astype(BF16)
                )

        if two:
            @pl.when((s >= 2) & (s < n_sp + 2))
            def _():
                p = turn(s - 2)
                give_part(p).wait_recv()
                answer_with(p, (own[p] + precv[p].astype(F32)).astype(BF16))

        @pl.when(s + 1 < n_far)
        def _():
            begin_rows(s + 1)

        @pl.when(s == 3)
        def _():
            for _ in shared.arrivals():
                pass

            @pl.loop(0, rows // 128)
            def _(r):
                at = pl.ds(pl.multiple_of(r * 128, 128), 128)
                resid[at, :] += jnp.dot(shid[at, :], sd[...], preferred_element_type=F32)

        @pl.when(s >= back)
        def _():
            combine(turn(s - back))

    @pl.loop(n_sp + 3 - back, n_sp)
    def _(s):
        combine(turn(s))

    out[...] = resid[...].astype(BF16)

    shared.drain()

    @pl.loop(0, n_sp)
    def _(p):
        if two:
            give_hidden(p).wait_send()
            give_part(p).wait_send()
        else:
            hidden_gather(p).drain()

        @pl.when(p < n_far)
        def _():
            rows_gather(p).drain()
            far_copy(p, 1).wait_send()

        @pl.when((p >= n_far) & (p < n_sp - 1))
        def _():
            near_copy(p, 1).wait_send()

        @pl.when(p < n_sp - 1)
        def _():
            reply(p).wait_send()
            scale_copy(p, 1).wait_send()


def shards(
    rec_input,
    gate_input,
    conv_weight,
    decay_wide,
    decay_narrow,
    input_wide,
    input_narrow,
    decay_base,
    decay_extra,
    tokens,
    out_weight,
    norm_gain,
    shared_gate,
    shared_up,
    shared_down,
    expert_gate,
    expert_up,
    expert_down,
    routes,
    route_weight,
):
    n_sp, n_tp = lax.axis_size("sp"), lax.axis_size("tp")
    rows, chan = rec_input.shape
    heads, wide, narrow = decay_wide.shape[1], decay_wide.shape[2], decay_narrow.shape[2]
    cols = tokens.shape[1]
    ff = shared_gate.shape[1]
    per = 2 if heads % 2 == 0 else 1
    hw = wide + narrow
    groups, gw = heads // per, per * hw
    cap = 3 * rows * routes.shape[1] // (2 * n_sp)
    direct = 4
    n_far = n_sp - direct
    two = n_tp == 4
    ex = decay_extra.reshape(2, rows, 2 * heads)
    vm = pl.BlockSpec(memory_space=pltpu.VMEM)
    hbm = pl.BlockSpec(memory_space=pl.ANY)
    sem = pltpu.SemaphoreType.DMA
    count = 6 if two else n_tp
    down = (2, 2 * ff, cols) if two else (n_tp * ff, cols)
    hid = 2 * ff if two else n_tp * ff
    V = pltpu.VMEM
    pairs = [(2,), (2,), (n_sp,), (2 * count,), (n_tp,), (2 * count,), (n_sp,), (n_sp * count,)]
    pairs += [(n_sp,) if two else (n_sp * count,), (n_sp,), (n_sp,), (count,), (n_sp,)]
    ins = (
        rec_input, gate_input, conv_weight, decay_wide, decay_narrow, input_wide, input_narrow,
        decay_base, ex, tokens, norm_gain.reshape(1, cols), routes.T, route_weight.T,
    )
    return pl.pallas_call(
        functools.partial(layer_kernel, n_sp, n_tp, cap, direct),
        name="layer",
        out_shape=jax.ShapeDtypeStruct((rows, cols), BF16),
        in_specs=[hbm] * (len(ins) + 7),
        out_specs=vm,
        scratch_shapes=[V(a.shape, a.dtype) for a in ins] + [
            V((n_tp, chan, cols), BF16), V(shared_gate.shape, BF16), V(shared_up.shape, BF16),
            V(expert_gate.shape[1:], BF16), V(expert_up.shape[1:], BF16), V(down, BF16),
            V((n_tp * ff, cols), BF16),
            V((rows, rows), BF16), V((rows, rows), BF16), V((4, groups, gw, gw), BF16),
            V((2, rows, 6 * heads), BF16),
            V((2, 16, chan), BF16), V((rows, chan), BF16), V((rows, chan), BF16),
            V((2, rows, chan), F32), V((2, rows, chan), F32),
            V((2, 2, chan), F32), V((n_sp, 2, chan), F32), V((rows, chan), BF16),
            V((n_tp, rows, chan), BF16), V((n_tp, 8, rows), F32), V((8, rows), F32),
            V((rows, cols), F32), V((rows, n_tp * cols), BF16),
            V((8, rows), F32), V((rows, 128), F32), V((n_sp, 8, cap), F32), V((n_sp, 8, cap), F32),
            V((n_sp, rows), F32), V((n_sp, rows), F32), V((rows, n_sp), F32), V((rows, n_sp), F32),
            V((n_far, cap, cols), BF16), V((direct - 1, cap, n_tp * cols), BF16),
            V((n_sp, cap, n_tp * cols), BF16), V((n_sp, cap, hid), BF16),
            V((n_sp, cap, cols), F32), V((n_sp, cap, cols), BF16), V((n_sp, cap, cols), BF16),
            V((n_sp, cap, cols), BF16), V((n_sp, cap, cols), BF16),
            V((rows, n_tp * ff), BF16),
            sem((len(ins),)), sem((8,)),
        ] + [sem(s) for s in pairs for _ in range(2)],
        compiler_params=pltpu.CompilerParams(
            collective_id=0, has_side_effects=True, vmem_limit_bytes=60 * 1024 * 1024
        ),
    )(
        *ins, out_weight.reshape(n_tp, chan, cols), shared_gate, shared_up, expert_gate[0], expert_up[0],
        expert_down[0], shared_down,
    )


def solution(mesh):
    placed = (
        P("sp", "tp"),
        P("sp", "tp"),
        P(None, "tp"),
        P(None, "tp", None, None),
        P(None, "tp", None, None),
        P(None, "tp", None, None),
        P(None, "tp", None, None),
        P(None, "tp"),
        P(None, "sp", None, "tp"),
        P("sp", "tp"),
        P(None, "tp"),
        P("tp"),
        P(None, "tp"),
        P(None, "tp"),
        P(None, "tp"),
        P("sp", None, "tp"),
        P("sp", None, "tp"),
        P("sp", None, "tp"),
        P("sp", None),
        P("sp", None),
    )
    return jax.shard_map(
        shards, mesh=mesh, in_specs=placed, out_specs=P("sp", "tp"), check_vma=False
    )
```

```python
import functools

import jax
import jax.numpy as jnp
from jax import lax
from jax.experimental import pallas as pl
from jax.experimental.pallas import tpu as pltpu
from jax.sharding import PartitionSpec as P

MESH = pl.DeviceIdType.MESH
D = 2048
CONV = 4
NORM_EPS = 1e-06
RATE_SCALE = 8.0
SEG = 8
F32 = jnp.float32
BF16 = jnp.bfloat16
EXACT = lax.Precision.HIGHEST


def rcopy(src, dst, send, recv, **where):
    return pltpu.make_async_remote_copy(
        src_ref=src, dst_ref=dst, send_sem=send, recv_sem=recv, device_id=where, device_id_type=MESH
    )


def hello(n_sp, n_tp):
    sp, tp = lax.axis_index("sp"), lax.axis_index("tp")
    barrier = pltpu.get_barrier_semaphore()
    for k in range(1, n_sp):
        pl.semaphore_signal(
            barrier, inc=1, device_id={"sp": lax.rem(sp + k, n_sp)}, device_id_type=MESH
        )
    for k in range(1, n_tp):
        pl.semaphore_signal(
            barrier, inc=1, device_id={"tp": lax.rem(tp + k, n_tp)}, device_id_type=MESH
        )


def met(n_sp, n_tp):
    pl.semaphore_wait(pltpu.get_barrier_semaphore(), n_sp + n_tp - 2)


def gather_sems(n_tp):
    count = 6 if n_tp == 4 else n_tp
    return [pltpu.SemaphoreType.DMA((count,)), pltpu.SemaphoreType.DMA((count,))]


class Gather:
    def __init__(self, n_tp, slot, send, recv, base=0):
        self.n, self.slot, self.send, self.recv, self.base = n_tp, slot, send, recv, base
        self.t = lax.axis_index("tp")
        if n_tp == 4:
            y, x = self.t // 2, lax.rem(self.t, 2)
            self.xn, self.yn, self.dg = y * 2 + 1 - x, (1 - y) * 2 + x, 3 - self.t

    def piece(self, owner, half, sem, to):
        ref = self.slot(owner, half)
        s = self.base + sem
        return rcopy(ref, ref, self.send.at[s], self.recv.at[s], tp=to)

    def start(self):
        if self.n == 4:
            self.piece(self.t, 0, 0, self.xn).start()
            self.piece(self.t, 1, 3, self.yn).start()
            self.piece(self.t, 1, 1, self.xn).start()
            self.piece(self.t, 0, 2, self.yn).start()
        else:
            for k in range(1, self.n):
                to = lax.rem(self.t + k, self.n)
                self.piece(self.t, None, k, to).start()

    def forward(self):
        if self.n == 4:
            self.piece(self.xn, 0, 0, self.xn).wait_recv()
            self.piece(self.xn, 0, 4, self.yn).start()
            self.piece(self.yn, 1, 3, self.yn).wait_recv()
            self.piece(self.yn, 1, 5, self.xn).start()

    def arrivals(self):
        if self.n == 4:
            self.piece(self.xn, 1, 1, self.xn).wait_recv()
            yield self.xn
            self.piece(self.yn, 0, 2, self.yn).wait_recv()
            yield self.yn
            self.piece(self.dg, 0, 4, self.yn).wait_recv()
            self.piece(self.dg, 1, 5, self.xn).wait_recv()
            yield self.dg
        else:
            for k in range(1, self.n):
                owner = lax.rem(self.t - k + self.n, self.n)
                self.piece(owner, None, k, owner).wait_recv()
                yield owner

    def drain(self):
        if self.n == 4:
            for s, half, owner in (
                (0, 0, self.t), (1, 1, self.t), (2, 0, self.t), (3, 1, self.t),
                (4, 0, self.xn), (5, 1, self.yn),
            ):
                self.piece(owner, half, s, self.xn).wait_send()
        else:
            for k in range(1, self.n):
                to = lax.rem(self.t + k, self.n)
                self.piece(self.t, None, k, to).wait_send()


def logistic(x):
    return 0.5 * jnp.tanh(0.5 * x) + 0.5


class Order:
    def __init__(self, n_sp):
        sp = lax.axis_index("sp")
        chip = sp // 2
        self.core, self.low, self.high, self.n = sp % 2, chip % 2, chip // 2, n_sp // 4

    def at(self, p, sign):
        step = p // 4 + 1
        high = (self.high + (step if sign > 0 else 2 * self.n - step)) % self.n
        low = (self.low + 1 + p // 2) % 2
        return (high * 2 + low) * 2 + (self.core + 1 + p) % 2


class Square:
    def __init__(self):
        t, core = lax.axis_index("tp"), lax.axis_index("sp") % 2
        y, x = t // 2, t % 2
        xn, yn = y * 2 + 1 - x, (1 - y) * 2 + x
        flip = core == 1
        self.gather = jnp.where(flip, yn, xn)
        self.reduce = jnp.where(flip, xn, yn)
        self.place = jnp.where(flip, y, x)
        self.mine = (jnp.where(flip, x, 2 * y), jnp.where(flip, 2 + x, 2 * y + 1))
        self.theirs = (jnp.where(flip, 1 - x, 2 - 2 * y), jnp.where(flip, 3 - x, 3 - 2 * y))


def layer_kernel(
    n_sp, n_tp, cap, direct,
    h_rec, h_gate, h_convw, h_dw, h_dn, h_iw, h_inn, h_base, h_extra, h_tokens, h_gain, h_routes,
    h_rweight, hbm_outw, hbm_sg, hbm_su, hbm_eg, hbm_eu, hbm_ed, hbm_sd,
    out,
    rec, gate, convw, dw, dn, iw, inn, base, extra, tokens, gain, routes, rweight,
    outw, sg, su, eg, eu, ed, sd, permt, perm, wblk, exs,
    halo, cperm, gperm, av, bv, msg, totals, mixedp, mixed, squares, sqown,
    resid, whole, srow, scol, smsg, sgot, pos, wts, post, wtt,
    outgoing, outwide, rows_in, hidden, own, psend, precv, answer, returned, shid,
    isem, wsem, xsend, xrecv, hsend, hrecv, tsend, trecv, gsend, grecv, ssend, srecv, nsend, nrecv,
    dsend, drecv, asend, arecv, bsend, brecv, psem, prem, rsend, rrecv, csend, crecv, lsend, lrecv,
):
    two = n_tp == 4
    rows, chan = rec.shape
    heads, wide, narrow = dw.shape[1], dw.shape[2], dn.shape[2]
    groups, gw = wblk.shape[1], wblk.shape[2]
    cols = tokens.shape[1]
    ff = eg.shape[1]
    seglen = rows // SEG
    count = 6 if two else n_tp
    n_far = n_sp - direct
    sp, tp = lax.axis_index("sp"), lax.axis_index("tp")
    mine = pl.ds(pl.multiple_of(tp * cols, 128), cols)
    order = Order(n_sp)
    sq = Square() if two else None

    loads = []

    def load(a, b):
        c = pltpu.make_async_copy(a, b, wsem.at[len(loads)])
        c.start()
        loads.append(c)

    def band(i):
        return pl.ds(pl.multiple_of(i * ff, 128), ff)

    ready = []
    for i, (a, b) in enumerate((
        (h_rec, rec), (h_convw, convw), (h_extra, extra), (h_gate, gate), (h_dw, dw), (h_dn, dn),
        (h_iw, iw), (h_inn, inn), (h_base, base), (h_tokens, tokens), (h_gain, gain),
        (h_routes, routes), (h_rweight, rweight),
    )):
        c = pltpu.make_async_copy(a, b, isem.at[i])
        c.start()
        ready.append(c)
    hello(n_sp, n_tp)
    load(hbm_outw, outw)
    load(hbm_sg, sg)
    load(hbm_su, su)
    load(hbm_eg, eg)
    load(hbm_eu, eu)
    load(hbm_sd, sd)
    if two:
        for j in range(2):
            load(hbm_ed.at[band(sq.mine[j])], ed.at[0, pl.ds(j * ff, ff)])
    else:
        load(hbm_ed, ed)
    ready[0].wait()
    met(n_sp, n_tp)
    up, down = lax.rem(sp + 1, n_sp), lax.rem(sp + n_sp - 1, n_sp)
    low = rcopy(rec.at[pl.ds(rows - 16, 16)], halo.at[0], hsend.at[0], hrecv.at[0], sp=up)
    high = rcopy(rec.at[pl.ds(0, 16)], halo.at[1], hsend.at[1], hrecv.at[1], sp=down)
    low.start()
    high.start()
    swaps = []
    if two:
        for j in range(2):
            c = rcopy(
                hbm_ed.at[band(sq.theirs[j])], ed.at[1, pl.ds(j * ff, ff)],
                xsend.at[j], xrecv.at[j], tp=sq.reduce,
            )
            c.start()
            swaps.append(c)
    for c in ready[1:]:
        c.wait()

    r = lax.broadcasted_iota(jnp.int32, (rows, rows), 0)
    q = lax.broadcasted_iota(jnp.int32, (rows, rows), 1)
    permt[...] = jnp.where((r % SEG) * seglen + r // SEG == q, 1.0, 0.0).astype(BF16)
    perm[...] = jnp.where((q % SEG) * seglen + q // SEG == r, 1.0, 0.0).astype(BF16)
    wblk[...] = jnp.zeros_like(wblk)
    per = heads // groups
    for d in range(2):
        for k, (w, n) in enumerate(((dw, dn), (iw, inn))):
            for h in range(heads):
                a = (h % per) * (wide + narrow)
                b = a + wide
                wblk[2 * d + k, h // per, a:b, a:b] = w[d, h]
                wblk[2 * d + k, h // per, b : b + narrow, b : b + narrow] = n[d, h]
    for d in range(2):
        left, terms = extra[d], []
        for _ in range(3):
            terms.append(left.astype(BF16).astype(F32))
            left = left - terms[-1]
        exs[d] = lax.dot_general(
            permt[...], jnp.concatenate(terms, axis=0).astype(BF16), (((1,), (1,)), ((), ())),
            preferred_element_type=F32,
        ).astype(BF16)
    gperm[...] = jnp.dot(permt[...], gate[...], preferred_element_type=F32).astype(BF16)

    taps = convw[...].astype(F32)

    def convolve(padded, n):
        conv = padded[0:n] * taps[0:1, :]
        for j in range(1, CONV):
            conv = conv + padded[j : j + n] * taps[j : j + 1, :]
        return conv.astype(BF16)

    x = rec[...].astype(F32)
    gap = jnp.zeros((2, chan), F32)
    mixedp[...] = convolve(jnp.concatenate([gap, x, gap[0:1]], axis=0), rows)
    low.wait()
    high.wait()
    lo = jnp.where(sp > 0, halo[0].astype(F32), 0.0)
    hi = jnp.where(sp < n_sp - 1, halo[1].astype(F32), 0.0)
    first, last = rec[0:32, :].astype(F32), rec[rows - 32 : rows, :].astype(F32)
    mixedp[0:16, :] = convolve(jnp.concatenate([lo[14:16], first[0:17]], axis=0), 16)
    mixedp[rows - 16 : rows, :] = convolve(jnp.concatenate([last[14:32], hi[0:1]], axis=0), 16)
    cperm[...] = jnp.dot(permt[...], mixedp[...], preferred_element_type=F32).astype(BF16)

    hw = wide + narrow
    ch = lax.broadcasted_iota(jnp.int32, (6 * heads, chan), 1)
    head, within = ch // hw, ch % hw
    term = lax.broadcasted_iota(jnp.int32, (6 * heads, chan), 0) % (2 * heads)
    spread = jnp.where(term == jnp.where(within >= wide, heads, 0) + head, 1.0, 0.0).astype(BF16)
    step = rows // 2

    @pl.loop(0, rows // step)
    def _(r):
        at = pl.ds(pl.multiple_of(r * step, step), step)
        for d in range(2):
            ex = jnp.dot(exs[d, at, :], spread, preferred_element_type=F32)
            for g in range(groups):
                lanes = slice(g * gw, (g + 1) * gw)
                c = cperm[at, lanes]
                rate = logistic(jnp.dot(c, wblk[2 * d, g], preferred_element_type=F32))
                admit = logistic(jnp.dot(c, wblk[2 * d + 1, g], preferred_element_type=F32))
                ld = jnp.minimum(ex[:, lanes] - rate * (RATE_SCALE * base[d : d + 1, lanes]), 0.0)
                a = jnp.exp(ld)
                bv[d, at, lanes] = jnp.sqrt(jnp.tanh(-ld) * (1.0 + a * a)) * admit * c.astype(F32)
                av[d, at, lanes] = a

    one = jnp.ones((SEG, chan), F32)
    zero = jnp.zeros((SEG, chan), F32)

    def advance(i, carry):
        got = []
        for d in range(2):
            at = pl.ds(pl.multiple_of((i if d == 0 else seglen - 1 - i) * SEG, SEG), SEG)
            a, b = av[d, at, :], bv[d, at, :]
            cum = carry[2 * d] * a
            state = a * carry[2 * d + 1] + b
            av[d, at, :] = cum
            bv[d, at, :] = state
            got += [cum, state]
        return tuple(got)

    ends = lax.fori_loop(0, seglen, advance, (one, zero, one, zero))

    def run(d, entering):
        seq = range(SEG) if d == 0 else range(SEG - 1, -1, -1)
        inside = [None] * SEG
        c = entering
        for s in seq:
            inside[s] = c
            c = ends[2 * d][s : s + 1] * c + ends[2 * d + 1][s : s + 1]
        return jnp.concatenate(inside, axis=0), c

    for d in range(2):
        prod = ends[2 * d][0:1]
        for s in range(1, SEG):
            prod = prod * ends[2 * d][s : s + 1]
        msg[d, 0:1, :] = prod
        msg[d, 1:2, :] = run(d, jnp.zeros((1, chan), F32))[1]
    sent = []
    for k in range(1, n_sp):
        to = lax.rem(sp + k, n_sp)
        c = rcopy(
            msg.at[jnp.where(to > sp, 0, 1)], totals.at[k], tsend.at[k], trecv.at[k], sp=to
        )
        c.start()
        sent.append(c)

    part = lax.broadcasted_iota(jnp.int32, (n_sp, rows), 0)
    who = jnp.zeros((n_sp, rows), jnp.int32)
    for p in range(n_sp):
        who = jnp.where(part == p, order.at(p, 1), who)
    hit0 = jnp.where(routes[0:1, :] == who, 1.0, 0.0)
    hit1 = jnp.where(routes[1:2, :] == who, 1.0, 0.0)
    earlier = jnp.where(r < q, 1.0, 0.0).astype(BF16)
    slots = jnp.dot((hit0 + hit1).astype(BF16), earlier, preferred_element_type=F32)
    pos[...] = jnp.where(hit0 + hit1 > 0.0, slots, -1.0)
    wts[...] = hit0 * rweight[0:1, :] + hit1 * rweight[1:2, :]
    post[...] = jnp.transpose(pos[...])
    wtt[...] = jnp.transpose(wts[...])

    @pl.loop(0, rows // 16)
    def _(r):
        at = pl.ds(pl.multiple_of(r * 16, 16), 16)
        bv[0, at, :] = bv[0, at, :] + bv[1, at, :]
        bv[1, at, :] = jax.nn.gelu(gperm[at, :].astype(F32))

    for c in sent:
        c.wait()
    carries = []
    zrow = jnp.zeros((1, chan), F32)
    c0, c1 = zrow, zrow
    for k in range(n_sp - 1, 0, -1):
        t = totals[k]
        c0 = jnp.where(k <= sp, t[0:1] * c0 + t[1:2], c0)
    for k in range(1, n_sp):
        t = totals[k]
        c1 = jnp.where(k > sp, t[0:1] * c1 + t[1:2], c1)
    for d, c in ((0, c0), (1, c1)):
        inside = run(d, c)[0]
        carries.append(jnp.concatenate([inside, inside], axis=0))

    @pl.loop(0, rows // 16)
    def _(r):
        at = pl.ds(pl.multiple_of(r * 16, 16), 16)
        total = bv[0, at, :] + av[0, at, :] * carries[0] + av[1, at, :] * carries[1]
        mixedp[at, :] = (total * bv[1, at, :]).astype(BF16)

    mixed[tp] = jnp.dot(perm[...], mixedp[...], preferred_element_type=F32).astype(BF16)

    half, quarter = rows // 2, rows // 4

    def rows_of(i, part):
        return pl.ds(i * half, half) if part is None else pl.ds(i * half + part * quarter, quarter)

    def mixed_slot(i):
        return lambda owner, part: mixed.at[owner, rows_of(i, part)]

    def whole_slot(i):
        return lambda owner, part: whole.at[
            rows_of(i, part), pl.ds(pl.multiple_of(owner * cols, 128), cols)
        ]

    g = [Gather(n_tp, mixed_slot(i), gsend, grecv, base=i * count) for i in range(2)]
    w = [Gather(n_tp, whole_slot(i), nsend, nrecv, base=i * count) for i in range(2)]

    def project(owner, i):
        at = pl.ds(i * half, half)
        resid[at, :] += jnp.dot(mixed[owner, at, :], outw[owner], preferred_element_type=F32)

    def publish(i):
        at = pl.ds(i * half, half)
        whole[at, mine] = (resid[at, :] * gain[...]).astype(BF16)

    g[0].start()
    resid[...] = tokens[...].astype(F32)
    loads[0].wait()
    project(tp, 0)
    project(tp, 1)
    g[0].forward()
    g[1].start()
    for owner in g[0].arrivals():
        project(owner, 0)
    publish(0)
    g[1].forward()
    w[0].start()
    for owner in g[1].arrivals():
        project(owner, 1)
    publish(1)
    w[0].forward()
    r2 = resid[...] * resid[...]
    sqown[...] = lax.dot_general(
        jnp.ones((8, cols), F32), r2, (((1,), (1,)), ((), ())),
        precision=EXACT, preferred_element_type=F32,
    )
    sent = []
    for k in range(1, n_tp):
        c = rcopy(sqown, squares.at[k], ssend.at[k], srecv.at[k], tp=lax.rem(tp + k, n_tp))
        c.start()
        sent.append(c)
    w[1].start()

    slot = lax.broadcasted_iota(jnp.int32, (cap, rows), 0).astype(F32)

    def chosen(p):
        return jnp.where(pos[pl.ds(p, 1), :] == slot, 1.0, 0.0)

    def far_copy(p, sign):
        return rcopy(
            outgoing.at[p], rows_in.at[p, :, mine], dsend.at[p], drecv.at[p], sp=order.at(p, sign)
        )

    def near_copy(p, sign):
        return rcopy(
            outwide.at[p - n_far], rows_in.at[p], dsend.at[p], drecv.at[p], sp=order.at(p, sign)
        )

    def reply(p):
        return rcopy(answer.at[p], returned.at[p], rsend.at[p], rrecv.at[p], sp=order.at(p, -1))

    def scale_copy(p, sign):
        return rcopy(smsg.at[p], sgot.at[p], lsend.at[p], lrecv.at[p], sp=order.at(p, sign))

    def dispatch(p):
        outgoing[p] = jnp.dot(
            chosen(p).astype(BF16), whole[:, mine], preferred_element_type=F32
        ).astype(BF16)
        far_copy(p, 1).start()

    dispatch(0)
    total = sqown[...]
    for k, c in enumerate(sent):
        c.wait()
        total = total + squares[k + 1]
    w[1].forward()
    left = lax.rsqrt(total / (n_tp * cols) + NORM_EPS)
    line = lax.broadcasted_iota(jnp.int32, left.shape, 0)
    terms = jnp.zeros_like(left)
    for i in range(3):
        term = left.astype(BF16).astype(F32)
        terms = jnp.where(line == i, term, terms)
        left = left - term
    srow[...] = jnp.concatenate([terms, jnp.zeros_like(terms)], axis=0).astype(BF16)

    def scales(p):
        return lax.dot_general(
            srow[...], chosen(p).astype(BF16), (((1,), (1,)), ((), ())),
            preferred_element_type=F32,
        ).astype(BF16)

    def column(terms):
        return lax.dot_general(
            terms, jnp.ones((16, 128), BF16), (((0,), (0,)), ((), ())), preferred_element_type=F32
        )

    def tell(p):
        smsg[p] = scales(p)
        scale_copy(p, 1).start()

    tell(0)

    @pl.loop(1, n_far)
    def _(p):
        tell(p)
        dispatch(p)

    scol[...] = column(srow[...])
    for i in range(2):
        g[i].drain()

    def rows_gather(p):
        def place(owner, part):
            if part is None:
                return rows_in.at[p, :, pl.ds(pl.multiple_of(owner * cols, 128), cols)]
            first = pl.multiple_of(owner * cols + part * (cols // 2), 128)
            return rows_in.at[p, :, pl.ds(first, cols // 2)]

        return Gather(n_tp, place, asend, arecv, base=p * count)

    def begin_rows(p):
        far_copy(p, -1).wait_recv()
        rows_gather(p).start()

    def shared_slot(i):
        def place(owner, part):
            at = pl.ds(i * half, half)
            if part is None:
                return shid.at[at, band(owner)]
            return shid.at[at, pl.ds(pl.multiple_of(owner * ff + part * (ff // 2), 128), ff // 2)]

        return place

    shared = [Gather(n_tp, shared_slot(i), csend, crecv, base=i * count) for i in range(2)]

    def shared_units(i):
        at = pl.ds(i * half, half)
        x = whole[at, :]
        s = scol[at, 0:1]
        g = jnp.dot(x, sg[...], preferred_element_type=F32) * s
        u = jnp.dot(x, su[...], preferred_element_type=F32) * s
        shid[at, band(tp)] = (jax.nn.silu(g) * u).astype(BF16)
        shared[i].start()

    for owner in w[0].arrivals():
        pass
    for c in loads[1:]:
        c.wait()
    shared_units(0)
    for owner in w[1].arrivals():
        pass

    def wide_pick(p):
        return jnp.dot(
            chosen(p).astype(BF16), whole[...], preferred_element_type=F32
        ).astype(BF16)

    def near(p):
        outwide[p - n_far] = wide_pick(p)
        tell(p)
        near_copy(p, 1).start()

    if two:
        here = pl.ds(pl.multiple_of(sq.place * ff, 128), ff)

        def give_hidden(p):
            ref = hidden.at[p, :, here]
            return rcopy(ref, ref, bsend.at[p], brecv.at[p], tp=sq.gather)

        def take_hidden(p):
            ref = hidden.at[p, :, pl.ds(pl.multiple_of((1 - sq.place) * ff, 128), ff)]
            return rcopy(ref, ref, bsend.at[p], brecv.at[p], tp=sq.gather)

        def give_part(p):
            return rcopy(psend.at[p], precv.at[p], psem.at[p], prem.at[p], tp=sq.reduce)

    else:
        here = band(tp)

        def hidden_gather(p):
            def place(owner, part):
                return hidden.at[p, :, band(owner)]

            return Gather(n_tp, place, bsend, brecv, base=p * count)

    near(n_sp - 2)
    shared_units(1)

    @pl.loop(n_far, n_sp - 2)
    def _(p):
        near(p)

    rows_in[n_sp - 1] = wide_pick(n_sp - 1)
    sgot[n_sp - 1] = scales(n_sp - 1)
    for i in range(2):
        w[i].drain()
    for c in swaps:
        c.wait()

    def answer_with(p, y):
        @pl.when(p == n_sp - 1)
        def _():
            returned[p] = y

        @pl.when(p < n_sp - 1)
        def _():
            answer[p] = y
            reply(p).start()

    def combine(p):
        @pl.when(p < n_sp - 1)
        def _():
            reply(p).wait_recv()

        which = lax.broadcasted_iota(jnp.int32, (rows, n_sp), 1) == p
        where = jnp.sum(jnp.where(which, post[...], 0.0), axis=1, keepdims=True)
        weight = jnp.sum(jnp.where(which, wtt[...], 0.0), axis=1, keepdims=True)
        lane = lax.broadcasted_iota(jnp.int32, (rows, cap), 1).astype(F32)
        hit = jnp.where(where == lane, 1.0, 0.0).astype(BF16)
        resid[...] += weight * jnp.dot(hit, returned[p], preferred_element_type=F32)

    def turn(s):
        return jnp.where(s == 0, n_sp - 2, jnp.where(s == n_sp - 1, n_sp - 1, s - 1))

    back = 5

    @pl.loop(0, n_sp + 3)
    def _(s):
        @pl.when(s < n_sp)
        def _():
            p = turn(s)

            @pl.when(p < n_far)
            def _():
                for _ in rows_gather(p).arrivals():
                    pass

            @pl.when((p >= n_far) & (p < n_sp - 1))
            def _():
                near_copy(p, -1).wait_recv()

            @pl.when(p < n_sp - 1)
            def _():
                scale_copy(p, -1).wait_recv()

            scale = column(sgot[p])[:, 0:1]
            x = rows_in[p]
            g = jnp.dot(x, eg[...], preferred_element_type=F32) * scale
            u = jnp.dot(x, eu[...], preferred_element_type=F32) * scale
            hidden[p, :, here] = (jax.nn.silu(g) * u).astype(BF16)
            if two:
                give_hidden(p).start()
            else:
                hidden_gather(p).start()

        @pl.when(s == 0)
        def _():
            shared[0].forward()
            shared[1].forward()
            begin_rows(0)
            begin_rows(1)

        @pl.when(s < n_far)
        def _():
            rows_gather(s).forward()

        @pl.when((s >= 1) & (s < n_sp + 1))
        def _():
            p = turn(s - 1)
            if two:
                take_hidden(p).wait_recv()
                h = hidden[p]
                psend[p] = jnp.dot(h, ed[1], preferred_element_type=F32).astype(BF16)
                give_part(p).start()
                own[p] = jnp.dot(h, ed[0], preferred_element_type=F32)
            else:
                for _ in hidden_gather(p).arrivals():
                    pass
                answer_with(
                    p, jnp.dot(hidden[p], ed[...], preferred_element_type=F32).astype(BF16)
                )

        @pl.when((s > 0) & (s + 1 < n_far))
        def _():
            begin_rows(s + 1)

        if two:
            @pl.when((s >= 2) & (s < n_sp + 2))
            def _():
                p = turn(s - 2)
                give_part(p).wait_recv()
                answer_with(p, (own[p] + precv[p].astype(F32)).astype(BF16))

        @pl.when(s == 3)
        def _():
            for i in range(2):
                for _ in shared[i].arrivals():
                    pass

            @pl.loop(0, rows // 128)
            def _(r):
                at = pl.ds(pl.multiple_of(r * 128, 128), 128)
                resid[at, :] += jnp.dot(shid[at, :], sd[...], preferred_element_type=F32)

        @pl.when(s >= back)
        def _():
            combine(turn(s - back))

    @pl.loop(n_sp + 3 - back, n_sp)
    def _(s):
        combine(turn(s))

    out[...] = resid[...].astype(BF16)

    for i in range(2):
        shared[i].drain()

    @pl.loop(0, n_sp)
    def _(p):
        if two:
            give_hidden(p).wait_send()
            give_part(p).wait_send()
        else:
            hidden_gather(p).drain()

        @pl.when(p < n_far)
        def _():
            rows_gather(p).drain()
            far_copy(p, 1).wait_send()

        @pl.when((p >= n_far) & (p < n_sp - 1))
        def _():
            near_copy(p, 1).wait_send()

        @pl.when(p < n_sp - 1)
        def _():
            reply(p).wait_send()
            scale_copy(p, 1).wait_send()


def shards(
    rec_input,
    gate_input,
    conv_weight,
    decay_wide,
    decay_narrow,
    input_wide,
    input_narrow,
    decay_base,
    decay_extra,
    tokens,
    out_weight,
    norm_gain,
    shared_gate,
    shared_up,
    shared_down,
    expert_gate,
    expert_up,
    expert_down,
    routes,
    route_weight,
):
    n_sp, n_tp = lax.axis_size("sp"), lax.axis_size("tp")
    rows, chan = rec_input.shape
    heads, wide, narrow = decay_wide.shape[1], decay_wide.shape[2], decay_narrow.shape[2]
    cols = tokens.shape[1]
    ff = shared_gate.shape[1]
    per = 2 if heads % 2 == 0 else 1
    hw = wide + narrow
    groups, gw = heads // per, per * hw
    cap = 3 * rows * routes.shape[1] // (2 * n_sp)
    direct = 4
    n_far = n_sp - direct
    two = n_tp == 4
    ex = decay_extra.transpose(0, 2, 3, 1).reshape(2, 2 * heads, rows)
    vm = pl.BlockSpec(memory_space=pltpu.VMEM)
    hbm = pl.BlockSpec(memory_space=pl.ANY)
    sem = pltpu.SemaphoreType.DMA
    count = 6 if two else n_tp
    down = (2, 2 * ff, cols) if two else (n_tp * ff, cols)
    hid = 2 * ff if two else n_tp * ff
    V = pltpu.VMEM
    pairs = [(2,), (2,), (n_sp,), (2 * count,), (n_tp,), (2 * count,), (n_sp,), (n_sp * count,)]
    pairs += [(n_sp,) if two else (n_sp * count,), (n_sp,), (n_sp,), (2 * count,), (n_sp,)]
    ins = (
        rec_input, gate_input, conv_weight, decay_wide, decay_narrow, input_wide, input_narrow,
        decay_base, ex, tokens, norm_gain.reshape(1, cols), routes.T, route_weight.T,
    )
    return pl.pallas_call(
        functools.partial(layer_kernel, n_sp, n_tp, cap, direct),
        name="layer",
        out_shape=jax.ShapeDtypeStruct((rows, cols), BF16),
        in_specs=[hbm] * (len(ins) + 7),
        out_specs=vm,
        scratch_shapes=[V(a.shape, a.dtype) for a in ins] + [
            V((n_tp, chan, cols), BF16), V(shared_gate.shape, BF16), V(shared_up.shape, BF16),
            V(expert_gate.shape[1:], BF16), V(expert_up.shape[1:], BF16), V(down, BF16),
            V((n_tp * ff, cols), BF16),
            V((rows, rows), BF16), V((rows, rows), BF16), V((4, groups, gw, gw), BF16),
            V((2, rows, 6 * heads), BF16),
            V((2, 16, chan), BF16), V((rows, chan), BF16), V((rows, chan), BF16),
            V((2, rows, chan), F32), V((2, rows, chan), F32),
            V((2, 2, chan), F32), V((n_sp, 2, chan), F32), V((rows, chan), BF16),
            V((n_tp, rows, chan), BF16), V((n_tp, 8, rows), F32), V((8, rows), F32),
            V((rows, cols), F32), V((rows, n_tp * cols), BF16),
            V((16, rows), BF16), V((rows, 128), F32), V((n_sp, 16, cap), BF16), V((n_sp, 16, cap), BF16),
            V((n_sp, rows), F32), V((n_sp, rows), F32), V((rows, n_sp), F32), V((rows, n_sp), F32),
            V((n_far, cap, cols), BF16), V((direct - 1, cap, n_tp * cols), BF16),
            V((n_sp, cap, n_tp * cols), BF16), V((n_sp, cap, hid), BF16),
            V((n_sp, cap, cols), F32), V((n_sp, cap, cols), BF16), V((n_sp, cap, cols), BF16),
            V((n_sp, cap, cols), BF16), V((n_sp, cap, cols), BF16),
            V((rows, n_tp * ff), BF16),
            sem((len(ins),)), sem((8,)),
        ] + [sem(s) for s in pairs for _ in range(2)],
        compiler_params=pltpu.CompilerParams(
            collective_id=0, has_side_effects=True, vmem_limit_bytes=60 * 1024 * 1024
        ),
    )(
        *ins, out_weight.reshape(n_tp, chan, cols), shared_gate, shared_up, expert_gate[0], expert_up[0],
        expert_down[0], shared_down,
    )


def solution(mesh):
    placed = (
        P("sp", "tp"),
        P("sp", "tp"),
        P(None, "tp"),
        P(None, "tp", None, None),
        P(None, "tp", None, None),
        P(None, "tp", None, None),
        P(None, "tp", None, None),
        P(None, "tp"),
        P(None, "sp", None, "tp"),
        P("sp", "tp"),
        P(None, "tp"),
        P("tp"),
        P(None, "tp"),
        P(None, "tp"),
        P(None, "tp"),
        P("sp", None, "tp"),
        P("sp", None, "tp"),
        P("sp", None, "tp"),
        P("sp", None),
        P("sp", None),
    )
    return jax.shard_map(
        shards, mesh=mesh, in_specs=placed, out_specs=P("sp", "tp"), check_vma=False
    )
```

```python
import functools

import jax
import jax.numpy as jnp
from jax import lax
from jax.experimental import pallas as pl
from jax.experimental.pallas import tpu as pltpu
from jax.sharding import PartitionSpec as P

MESH = pl.DeviceIdType.MESH
D = 2048
CONV = 4
NORM_EPS = 1e-06
RATE_SCALE = 8.0
SEG = 8
F32 = jnp.float32
BF16 = jnp.bfloat16
EXACT = lax.Precision.HIGHEST


def rcopy(src, dst, send, recv, **where):
    return pltpu.make_async_remote_copy(
        src_ref=src, dst_ref=dst, send_sem=send, recv_sem=recv, device_id=where, device_id_type=MESH
    )


def hello(n_sp, n_tp):
    sp, tp = lax.axis_index("sp"), lax.axis_index("tp")
    barrier = pltpu.get_barrier_semaphore()
    for k in range(1, n_sp):
        pl.semaphore_signal(
            barrier, inc=1, device_id={"sp": lax.rem(sp + k, n_sp)}, device_id_type=MESH
        )
    for k in range(1, n_tp):
        pl.semaphore_signal(
            barrier, inc=1, device_id={"tp": lax.rem(tp + k, n_tp)}, device_id_type=MESH
        )


def met(n_sp, n_tp):
    pl.semaphore_wait(pltpu.get_barrier_semaphore(), n_sp + n_tp - 2)


def gather_sems(n_tp):
    count = 6 if n_tp == 4 else n_tp
    return [pltpu.SemaphoreType.DMA((count,)), pltpu.SemaphoreType.DMA((count,))]


class Gather:
    def __init__(self, n_tp, slot, send, recv, base=0):
        self.n, self.slot, self.send, self.recv, self.base = n_tp, slot, send, recv, base
        self.t = lax.axis_index("tp")
        if n_tp == 4:
            y, x = self.t // 2, lax.rem(self.t, 2)
            self.xn, self.yn, self.dg = y * 2 + 1 - x, (1 - y) * 2 + x, 3 - self.t

    def piece(self, owner, half, sem, to):
        ref = self.slot(owner, half)
        s = self.base + sem
        return rcopy(ref, ref, self.send.at[s], self.recv.at[s], tp=to)

    def start(self):
        if self.n == 4:
            self.piece(self.t, 0, 0, self.xn).start()
            self.piece(self.t, 1, 3, self.yn).start()
            self.piece(self.t, 1, 1, self.xn).start()
            self.piece(self.t, 0, 2, self.yn).start()
        else:
            for k in range(1, self.n):
                to = lax.rem(self.t + k, self.n)
                self.piece(self.t, None, k, to).start()

    def forward(self):
        if self.n == 4:
            self.piece(self.xn, 0, 0, self.xn).wait_recv()
            self.piece(self.xn, 0, 4, self.yn).start()
            self.piece(self.yn, 1, 3, self.yn).wait_recv()
            self.piece(self.yn, 1, 5, self.xn).start()

    def arrivals(self):
        if self.n == 4:
            self.piece(self.xn, 1, 1, self.xn).wait_recv()
            yield self.xn
            self.piece(self.yn, 0, 2, self.yn).wait_recv()
            yield self.yn
            self.piece(self.dg, 0, 4, self.yn).wait_recv()
            self.piece(self.dg, 1, 5, self.xn).wait_recv()
            yield self.dg
        else:
            for k in range(1, self.n):
                owner = lax.rem(self.t - k + self.n, self.n)
                self.piece(owner, None, k, owner).wait_recv()
                yield owner

    def drain(self):
        if self.n == 4:
            for s, half, owner in (
                (0, 0, self.t), (1, 1, self.t), (2, 0, self.t), (3, 1, self.t),
                (4, 0, self.xn), (5, 1, self.yn),
            ):
                self.piece(owner, half, s, self.xn).wait_send()
        else:
            for k in range(1, self.n):
                to = lax.rem(self.t + k, self.n)
                self.piece(self.t, None, k, to).wait_send()


def logistic(x):
    return 0.5 * jnp.tanh(0.5 * x) + 0.5


class Order:
    def __init__(self, n_sp):
        sp = lax.axis_index("sp")
        chip = sp // 2
        self.core, self.low, self.high, self.n = sp % 2, chip % 2, chip // 2, n_sp // 4

    def at(self, p, sign):
        step = p // 4 + 1
        high = (self.high + (step if sign > 0 else 2 * self.n - step)) % self.n
        low = (self.low + 1 + p // 2) % 2
        return (high * 2 + low) * 2 + (self.core + 1 + p) % 2


class Square:
    def __init__(self):
        t, core = lax.axis_index("tp"), lax.axis_index("sp") % 2
        y, x = t // 2, t % 2
        xn, yn = y * 2 + 1 - x, (1 - y) * 2 + x
        flip = core == 1
        self.gather = jnp.where(flip, yn, xn)
        self.reduce = jnp.where(flip, xn, yn)
        self.place = jnp.where(flip, y, x)
        self.mine = (jnp.where(flip, x, 2 * y), jnp.where(flip, 2 + x, 2 * y + 1))
        self.theirs = (jnp.where(flip, 1 - x, 2 - 2 * y), jnp.where(flip, 3 - x, 3 - 2 * y))


def layer_kernel(
    n_sp, n_tp, cap, direct,
    h_rec, h_gate, h_convw, h_dw, h_dn, h_iw, h_inn, h_base, h_extra, h_tokens, h_gain, h_routes,
    h_rweight, hbm_outw, hbm_sg, hbm_su, hbm_eg, hbm_eu, hbm_ed, hbm_sd,
    out,
    rec, gate, convw, dw, dn, iw, inn, base, extra, tokens, gain, routes, rweight,
    outw, sg, su, eg, eu, ed, sd, permt, perm, wblk, exs,
    halo, cperm, gperm, av, bv, msg, totals, mixedp, mixed, squares, sqown,
    resid, whole, srow, scol, smsg, sgot, pos, wts, post, wtt,
    outgoing, outwide, rows_in, hidden, own, psend, precv, answer, returned, shid,
    isem, wsem, xsend, xrecv, hsend, hrecv, tsend, trecv, gsend, grecv, ssend, srecv, nsend, nrecv,
    dsend, drecv, asend, arecv, bsend, brecv, psem, prem, rsend, rrecv, csend, crecv, lsend, lrecv,
):
    two = n_tp == 4
    rows, chan = rec.shape
    heads, wide, narrow = dw.shape[1], dw.shape[2], dn.shape[2]
    groups, gw = wblk.shape[1], wblk.shape[2]
    cols = tokens.shape[1]
    ff = eg.shape[1]
    seglen = rows // SEG
    count = 6 if two else n_tp
    n_far = n_sp - direct
    sp, tp = lax.axis_index("sp"), lax.axis_index("tp")
    mine = pl.ds(pl.multiple_of(tp * cols, 128), cols)
    order = Order(n_sp)
    sq = Square() if two else None

    loads = []

    def load(a, b):
        c = pltpu.make_async_copy(a, b, wsem.at[len(loads)])
        c.start()
        loads.append(c)

    def band(i):
        return pl.ds(pl.multiple_of(i * ff, 128), ff)

    ready = []
    for i, (a, b) in enumerate((
        (h_rec, rec), (h_convw, convw), (h_extra, extra), (h_gate, gate), (h_dw, dw), (h_dn, dn),
        (h_iw, iw), (h_inn, inn), (h_base, base), (h_tokens, tokens), (h_gain, gain),
        (h_routes, routes), (h_rweight, rweight),
    )):
        c = pltpu.make_async_copy(a, b, isem.at[i])
        c.start()
        ready.append(c)
    hello(n_sp, n_tp)
    load(hbm_outw, outw)
    load(hbm_sg, sg)
    load(hbm_su, su)
    load(hbm_eg, eg)
    load(hbm_eu, eu)
    load(hbm_sd, sd)
    if two:
        for j in range(2):
            load(hbm_ed.at[band(sq.mine[j])], ed.at[0, pl.ds(j * ff, ff)])
    else:
        load(hbm_ed, ed)
    ready[0].wait()
    met(n_sp, n_tp)
    up, down = lax.rem(sp + 1, n_sp), lax.rem(sp + n_sp - 1, n_sp)
    low = rcopy(rec.at[pl.ds(rows - 16, 16)], halo.at[0], hsend.at[0], hrecv.at[0], sp=up)
    high = rcopy(rec.at[pl.ds(0, 16)], halo.at[1], hsend.at[1], hrecv.at[1], sp=down)
    low.start()
    high.start()
    swaps = []
    if two:
        for j in range(2):
            c = rcopy(
                hbm_ed.at[band(sq.theirs[j])], ed.at[1, pl.ds(j * ff, ff)],
                xsend.at[j], xrecv.at[j], tp=sq.reduce,
            )
            c.start()
            swaps.append(c)
    for c in ready[1:]:
        c.wait()

    r = lax.broadcasted_iota(jnp.int32, (rows, rows), 0)
    q = lax.broadcasted_iota(jnp.int32, (rows, rows), 1)
    permt[...] = jnp.where((r % SEG) * seglen + r // SEG == q, 1.0, 0.0).astype(BF16)
    perm[...] = jnp.where((q % SEG) * seglen + q // SEG == r, 1.0, 0.0).astype(BF16)
    wblk[...] = jnp.zeros_like(wblk)
    per = heads // groups
    for d in range(2):
        for k, (w, n) in enumerate(((dw, dn), (iw, inn))):
            for h in range(heads):
                a = (h % per) * (wide + narrow)
                b = a + wide
                wblk[2 * d + k, h // per, a:b, a:b] = w[d, h]
                wblk[2 * d + k, h // per, b : b + narrow, b : b + narrow] = n[d, h]
    for d in range(2):
        left, terms = extra[d], []
        for _ in range(3):
            terms.append(left.astype(BF16).astype(F32))
            left = left - terms[-1]
        exs[d] = lax.dot_general(
            permt[...], jnp.concatenate(terms, axis=0).astype(BF16), (((1,), (1,)), ((), ())),
            preferred_element_type=F32,
        ).astype(BF16)
    gperm[...] = jnp.dot(permt[...], gate[...], preferred_element_type=F32).astype(BF16)

    taps = convw[...].astype(F32)

    def convolve(padded, n):
        conv = padded[0:n] * taps[0:1, :]
        for j in range(1, CONV):
            conv = conv + padded[j : j + n] * taps[j : j + 1, :]
        return conv.astype(BF16)

    x = rec[...].astype(F32)
    gap = jnp.zeros((2, chan), F32)
    mixedp[...] = convolve(jnp.concatenate([gap, x, gap[0:1]], axis=0), rows)
    low.wait()
    high.wait()
    lo = jnp.where(sp > 0, halo[0].astype(F32), 0.0)
    hi = jnp.where(sp < n_sp - 1, halo[1].astype(F32), 0.0)
    first, last = rec[0:32, :].astype(F32), rec[rows - 32 : rows, :].astype(F32)
    mixedp[0:16, :] = convolve(jnp.concatenate([lo[14:16], first[0:17]], axis=0), 16)
    mixedp[rows - 16 : rows, :] = convolve(jnp.concatenate([last[14:32], hi[0:1]], axis=0), 16)
    cperm[...] = jnp.dot(permt[...], mixedp[...], preferred_element_type=F32).astype(BF16)

    hw = wide + narrow
    ch = lax.broadcasted_iota(jnp.int32, (6 * heads, chan), 1)
    head, within = ch // hw, ch % hw
    term = lax.broadcasted_iota(jnp.int32, (6 * heads, chan), 0) % (2 * heads)
    spread = jnp.where(term == jnp.where(within >= wide, heads, 0) + head, 1.0, 0.0).astype(BF16)
    step = rows // 2

    @pl.loop(0, rows // step)
    def _(r):
        at = pl.ds(pl.multiple_of(r * step, step), step)
        for d in range(2):
            ex = jnp.dot(exs[d, at, :], spread, preferred_element_type=F32)
            for g in range(groups):
                lanes = slice(g * gw, (g + 1) * gw)
                c = cperm[at, lanes]
                rate = logistic(jnp.dot(c, wblk[2 * d, g], preferred_element_type=F32))
                admit = logistic(jnp.dot(c, wblk[2 * d + 1, g], preferred_element_type=F32))
                ld = jnp.minimum(ex[:, lanes] - rate * (RATE_SCALE * base[d : d + 1, lanes]), 0.0)
                a = jnp.exp(ld)
                bv[d, at, lanes] = jnp.sqrt(jnp.tanh(-ld) * (1.0 + a * a)) * admit * c.astype(F32)
                av[d, at, lanes] = a

    one = jnp.ones((SEG, chan), F32)
    zero = jnp.zeros((SEG, chan), F32)

    def advance(i, carry):
        got = []
        for d in range(2):
            at = pl.ds(pl.multiple_of((i if d == 0 else seglen - 1 - i) * SEG, SEG), SEG)
            a, b = av[d, at, :], bv[d, at, :]
            cum = carry[2 * d] * a
            state = a * carry[2 * d + 1] + b
            av[d, at, :] = cum
            bv[d, at, :] = state
            got += [cum, state]
        return tuple(got)

    ends = lax.fori_loop(0, seglen, advance, (one, zero, one, zero))

    def run(d, entering):
        seq = range(SEG) if d == 0 else range(SEG - 1, -1, -1)
        inside = [None] * SEG
        c = entering
        for s in seq:
            inside[s] = c
            c = ends[2 * d][s : s + 1] * c + ends[2 * d + 1][s : s + 1]
        return jnp.concatenate(inside, axis=0), c

    for d in range(2):
        prod = ends[2 * d][0:1]
        for s in range(1, SEG):
            prod = prod * ends[2 * d][s : s + 1]
        msg[d, 0:1, :] = prod
        msg[d, 1:2, :] = run(d, jnp.zeros((1, chan), F32))[1]
    sent = []
    for k in range(1, n_sp):
        to = lax.rem(sp + k, n_sp)
        c = rcopy(
            msg.at[jnp.where(to > sp, 0, 1)], totals.at[k], tsend.at[k], trecv.at[k], sp=to
        )
        c.start()
        sent.append(c)

    part = lax.broadcasted_iota(jnp.int32, (n_sp, rows), 0)
    who = jnp.zeros((n_sp, rows), jnp.int32)
    for p in range(n_sp):
        who = jnp.where(part == p, order.at(p, 1), who)
    hit0 = jnp.where(routes[0:1, :] == who, 1.0, 0.0)
    hit1 = jnp.where(routes[1:2, :] == who, 1.0, 0.0)
    earlier = jnp.where(r < q, 1.0, 0.0).astype(BF16)
    slots = jnp.dot((hit0 + hit1).astype(BF16), earlier, preferred_element_type=F32)
    pos[...] = jnp.where(hit0 + hit1 > 0.0, slots, -1.0)
    wts[...] = hit0 * rweight[0:1, :] + hit1 * rweight[1:2, :]
    post[...] = jnp.transpose(pos[...])
    wtt[...] = jnp.transpose(wts[...])

    @pl.loop(0, rows // 16)
    def _(r):
        at = pl.ds(pl.multiple_of(r * 16, 16), 16)
        bv[0, at, :] = bv[0, at, :] + bv[1, at, :]
        bv[1, at, :] = jax.nn.gelu(gperm[at, :].astype(F32))

    for c in sent:
        c.wait()
    carries = []
    zrow = jnp.zeros((1, chan), F32)
    c0, c1 = zrow, zrow
    for k in range(n_sp - 1, 0, -1):
        t = totals[k]
        c0 = jnp.where(k <= sp, t[0:1] * c0 + t[1:2], c0)
    for k in range(1, n_sp):
        t = totals[k]
        c1 = jnp.where(k > sp, t[0:1] * c1 + t[1:2], c1)
    for d, c in ((0, c0), (1, c1)):
        inside = run(d, c)[0]
        carries.append(jnp.concatenate([inside, inside], axis=0))

    @pl.loop(0, rows // 16)
    def _(r):
        at = pl.ds(pl.multiple_of(r * 16, 16), 16)
        total = bv[0, at, :] + av[0, at, :] * carries[0] + av[1, at, :] * carries[1]
        mixedp[at, :] = (total * bv[1, at, :]).astype(BF16)

    mixed[tp] = jnp.dot(perm[...], mixedp[...], preferred_element_type=F32).astype(BF16)

    half, quarter = rows // 2, rows // 4

    def rows_of(i, part):
        return pl.ds(i * half, half) if part is None else pl.ds(i * half + part * quarter, quarter)

    def mixed_slot(i):
        return lambda owner, part: mixed.at[owner, rows_of(i, part)]

    def whole_slot(i):
        return lambda owner, part: whole.at[
            rows_of(i, part), pl.ds(pl.multiple_of(owner * cols, 128), cols)
        ]

    g = [Gather(n_tp, mixed_slot(i), gsend, grecv, base=i * count) for i in range(2)]
    w = [Gather(n_tp, whole_slot(i), nsend, nrecv, base=i * count) for i in range(2)]

    def project(owner, i):
        at = pl.ds(i * half, half)
        resid[at, :] += jnp.dot(mixed[owner, at, :], outw[owner], preferred_element_type=F32)

    def publish(i):
        at = pl.ds(i * half, half)
        whole[at, mine] = (resid[at, :] * gain[...]).astype(BF16)

    g[0].start()
    resid[...] = tokens[...].astype(F32)
    loads[0].wait()
    project(tp, 0)
    project(tp, 1)
    g[0].forward()
    g[1].start()
    for owner in g[0].arrivals():
        project(owner, 0)
    publish(0)
    g[1].forward()
    w[0].start()
    for owner in g[1].arrivals():
        project(owner, 1)
    publish(1)
    w[0].forward()
    r2 = resid[...] * resid[...]
    sqown[...] = lax.dot_general(
        jnp.ones((8, cols), F32), r2, (((1,), (1,)), ((), ())),
        precision=EXACT, preferred_element_type=F32,
    )
    sent = []
    for k in range(1, n_tp):
        c = rcopy(sqown, squares.at[k], ssend.at[k], srecv.at[k], tp=lax.rem(tp + k, n_tp))
        c.start()
        sent.append(c)
    w[1].start()

    slot = lax.broadcasted_iota(jnp.int32, (cap, rows), 0).astype(F32)

    def chosen(p):
        return jnp.where(pos[pl.ds(p, 1), :] == slot, 1.0, 0.0)

    def far_copy(p, sign):
        return rcopy(
            outgoing.at[p], rows_in.at[p, :, mine], dsend.at[p], drecv.at[p], sp=order.at(p, sign)
        )

    def near_copy(p, sign):
        return rcopy(
            outwide.at[p - n_far], rows_in.at[p], dsend.at[p], drecv.at[p], sp=order.at(p, sign)
        )

    def reply(p):
        return rcopy(answer.at[p], returned.at[p], rsend.at[p], rrecv.at[p], sp=order.at(p, -1))

    def scale_copy(p, sign):
        return rcopy(smsg.at[p], sgot.at[p], lsend.at[p], lrecv.at[p], sp=order.at(p, sign))

    def dispatch(p):
        outgoing[p] = jnp.dot(
            chosen(p).astype(BF16), whole[:, mine], preferred_element_type=F32
        ).astype(BF16)
        far_copy(p, 1).start()

    dispatch(0)
    total = sqown[...]
    for k, c in enumerate(sent):
        c.wait()
        total = total + squares[k + 1]
    w[1].forward()
    left = lax.rsqrt(total / (n_tp * cols) + NORM_EPS)
    line = lax.broadcasted_iota(jnp.int32, left.shape, 0)
    terms = jnp.zeros_like(left)
    for i in range(3):
        term = left.astype(BF16).astype(F32)
        terms = jnp.where(line == i, term, terms)
        left = left - term
    srow[...] = jnp.concatenate([terms, jnp.zeros_like(terms)], axis=0).astype(BF16)

    def scales(p):
        return lax.dot_general(
            srow[...], chosen(p).astype(BF16), (((1,), (1,)), ((), ())),
            preferred_element_type=F32,
        ).astype(BF16)

    def column(terms):
        return lax.dot_general(
            terms, jnp.ones((16, 128), BF16), (((0,), (0,)), ((), ())), preferred_element_type=F32
        )

    def tell(p):
        smsg[p] = scales(p)
        scale_copy(p, 1).start()

    tell(0)

    @pl.loop(1, n_far)
    def _(p):
        tell(p)
        dispatch(p)

    scol[...] = column(srow[...])
    for i in range(2):
        g[i].drain()

    def rows_gather(p):
        def place(owner, part):
            if part is None:
                return rows_in.at[p, :, pl.ds(pl.multiple_of(owner * cols, 128), cols)]
            first = pl.multiple_of(owner * cols + part * (cols // 2), 128)
            return rows_in.at[p, :, pl.ds(first, cols // 2)]

        return Gather(n_tp, place, asend, arecv, base=p * count)

    def begin_rows(p):
        far_copy(p, -1).wait_recv()
        rows_gather(p).start()

    def shared_slot(i):
        def place(owner, part):
            at = pl.ds(i * half, half)
            if part is None:
                return shid.at[at, band(owner)]
            return shid.at[at, pl.ds(pl.multiple_of(owner * ff + part * (ff // 2), 128), ff // 2)]

        return place

    shared = [Gather(n_tp, shared_slot(i), csend, crecv, base=i * count) for i in range(2)]

    def shared_units(i):
        at = pl.ds(i * half, half)
        x = whole[at, :]
        s = scol[at, 0:1]
        g = jnp.dot(x, sg[...], preferred_element_type=F32) * s
        u = jnp.dot(x, su[...], preferred_element_type=F32) * s
        shid[at, band(tp)] = (jax.nn.silu(g) * u).astype(BF16)
        shared[i].start()

    for owner in w[0].arrivals():
        pass
    for c in loads[1:]:
        c.wait()
    shared_units(0)
    for owner in w[1].arrivals():
        pass

    def wide_pick(p):
        return jnp.dot(
            chosen(p).astype(BF16), whole[...], preferred_element_type=F32
        ).astype(BF16)

    def near(p):
        outwide[p - n_far] = wide_pick(p)
        tell(p)
        near_copy(p, 1).start()

    if two:
        here = pl.ds(pl.multiple_of(sq.place * ff, 128), ff)

        def give_hidden(p):
            ref = hidden.at[p, :, here]
            return rcopy(ref, ref, bsend.at[p], brecv.at[p], tp=sq.gather)

        def take_hidden(p):
            ref = hidden.at[p, :, pl.ds(pl.multiple_of((1 - sq.place) * ff, 128), ff)]
            return rcopy(ref, ref, bsend.at[p], brecv.at[p], tp=sq.gather)

        def give_part(p):
            return rcopy(psend.at[p], precv.at[p], psem.at[p], prem.at[p], tp=sq.reduce)

    else:
        here = band(tp)

        def hidden_gather(p):
            def place(owner, part):
                return hidden.at[p, :, band(owner)]

            return Gather(n_tp, place, bsend, brecv, base=p * count)

    @pl.loop(n_far, n_sp - 2)
    def _(p):
        near(p)

    shared_units(1)
    shared[0].forward()
    near(n_sp - 2)
    rows_in[n_sp - 1] = wide_pick(n_sp - 1)
    sgot[n_sp - 1] = scales(n_sp - 1)
    shared[1].forward()
    begin_rows(0)
    begin_rows(1)
    rows_gather(0).forward()
    for i in range(2):
        w[i].drain()
    for c in swaps:
        c.wait()

    def answer_with(p, y):
        @pl.when(p == n_sp - 1)
        def _():
            returned[p] = y

        @pl.when(p < n_sp - 1)
        def _():
            answer[p] = y
            reply(p).start()

    def combine(p):
        @pl.when(p < n_sp - 1)
        def _():
            reply(p).wait_recv()

        which = lax.broadcasted_iota(jnp.int32, (rows, n_sp), 1) == p
        where = jnp.sum(jnp.where(which, post[...], 0.0), axis=1, keepdims=True)
        weight = jnp.sum(jnp.where(which, wtt[...], 0.0), axis=1, keepdims=True)
        lane = lax.broadcasted_iota(jnp.int32, (rows, cap), 1).astype(F32)
        hit = jnp.where(where == lane, 1.0, 0.0).astype(BF16)
        resid[...] += weight * jnp.dot(hit, returned[p], preferred_element_type=F32)

    back = 5

    @pl.loop(0, n_sp + 3)
    def _(s):
        @pl.when(s < n_sp)
        def _():
            p = s

            @pl.when(p < n_far)
            def _():
                for _ in rows_gather(p).arrivals():
                    pass

            @pl.when((p >= n_far) & (p < n_sp - 1))
            def _():
                near_copy(p, -1).wait_recv()

            @pl.when(p < n_sp - 1)
            def _():
                scale_copy(p, -1).wait_recv()

            scale = column(sgot[p])[:, 0:1]
            x = rows_in[p]
            g = jnp.dot(x, eg[...], preferred_element_type=F32) * scale
            u = jnp.dot(x, eu[...], preferred_element_type=F32) * scale
            hidden[p, :, here] = (jax.nn.silu(g) * u).astype(BF16)
            if two:
                give_hidden(p).start()
            else:
                hidden_gather(p).start()

        @pl.when(s + 1 < n_far)
        def _():
            rows_gather(s + 1).forward()

        @pl.when((s >= 1) & (s < n_sp + 1))
        def _():
            p = s - 1
            if two:
                take_hidden(p).wait_recv()
                h = hidden[p]
                psend[p] = jnp.dot(h, ed[1], preferred_element_type=F32).astype(BF16)
                give_part(p).start()
                own[p] = jnp.dot(h, ed[0], preferred_element_type=F32)
            else:
                for _ in hidden_gather(p).arrivals():
                    pass
                answer_with(
                    p, jnp.dot(hidden[p], ed[...], preferred_element_type=F32).astype(BF16)
                )

        @pl.when(s + 2 < n_far)
        def _():
            begin_rows(s + 2)

        if two:
            @pl.when((s >= 2) & (s < n_sp + 2))
            def _():
                p = s - 2
                give_part(p).wait_recv()
                answer_with(p, (own[p] + precv[p].astype(F32)).astype(BF16))

        @pl.when(s == 2)
        def _():
            for i in range(2):
                for _ in shared[i].arrivals():
                    pass

            @pl.loop(0, rows // 128)
            def _(r):
                at = pl.ds(pl.multiple_of(r * 128, 128), 128)
                resid[at, :] += jnp.dot(shid[at, :], sd[...], preferred_element_type=F32)

        @pl.when(s >= back)
        def _():
            combine(s - back)

    for i in range(2):
        shared[i].drain()

    @pl.loop(0, n_sp)
    def _(p):
        if two:
            give_hidden(p).wait_send()
            give_part(p).wait_send()
        else:
            hidden_gather(p).drain()

        @pl.when(p < n_far)
        def _():
            rows_gather(p).drain()
            far_copy(p, 1).wait_send()

        @pl.when((p >= n_far) & (p < n_sp - 1))
        def _():
            near_copy(p, 1).wait_send()

        @pl.when(p < n_sp - 1)
        def _():
            reply(p).wait_send()
            scale_copy(p, 1).wait_send()

    @pl.loop(n_sp + 3 - back, n_sp)
    def _(s):
        combine(s)

    out[...] = resid[...].astype(BF16)


def shards(
    rec_input,
    gate_input,
    conv_weight,
    decay_wide,
    decay_narrow,
    input_wide,
    input_narrow,
    decay_base,
    decay_extra,
    tokens,
    out_weight,
    norm_gain,
    shared_gate,
    shared_up,
    shared_down,
    expert_gate,
    expert_up,
    expert_down,
    routes,
    route_weight,
):
    n_sp, n_tp = lax.axis_size("sp"), lax.axis_size("tp")
    rows, chan = rec_input.shape
    heads, wide, narrow = decay_wide.shape[1], decay_wide.shape[2], decay_narrow.shape[2]
    cols = tokens.shape[1]
    ff = shared_gate.shape[1]
    per = 2 if heads % 2 == 0 else 1
    hw = wide + narrow
    groups, gw = heads // per, per * hw
    cap = 3 * rows * routes.shape[1] // (2 * n_sp)
    direct = 4
    n_far = n_sp - direct
    two = n_tp == 4
    ex = decay_extra.transpose(0, 2, 3, 1).reshape(2, 2 * heads, rows)
    vm = pl.BlockSpec(memory_space=pltpu.VMEM)
    hbm = pl.BlockSpec(memory_space=pl.ANY)
    sem = pltpu.SemaphoreType.DMA
    count = 6 if two else n_tp
    down = (2, 2 * ff, cols) if two else (n_tp * ff, cols)
    hid = 2 * ff if two else n_tp * ff
    V = pltpu.VMEM
    pairs = [(2,), (2,), (n_sp,), (2 * count,), (n_tp,), (2 * count,), (n_sp,), (n_sp * count,)]
    pairs += [(n_sp,) if two else (n_sp * count,), (n_sp,), (n_sp,), (2 * count,), (n_sp,)]
    ins = (
        rec_input, gate_input, conv_weight, decay_wide, decay_narrow, input_wide, input_narrow,
        decay_base, ex, tokens, norm_gain.reshape(1, cols), routes.T, route_weight.T,
    )
    return pl.pallas_call(
        functools.partial(layer_kernel, n_sp, n_tp, cap, direct),
        name="layer",
        out_shape=jax.ShapeDtypeStruct((rows, cols), BF16),
        in_specs=[hbm] * (len(ins) + 7),
        out_specs=vm,
        scratch_shapes=[V(a.shape, a.dtype) for a in ins] + [
            V((n_tp, chan, cols), BF16), V(shared_gate.shape, BF16), V(shared_up.shape, BF16),
            V(expert_gate.shape[1:], BF16), V(expert_up.shape[1:], BF16), V(down, BF16),
            V((n_tp * ff, cols), BF16),
            V((rows, rows), BF16), V((rows, rows), BF16), V((4, groups, gw, gw), BF16),
            V((2, rows, 6 * heads), BF16),
            V((2, 16, chan), BF16), V((rows, chan), BF16), V((rows, chan), BF16),
            V((2, rows, chan), F32), V((2, rows, chan), F32),
            V((2, 2, chan), F32), V((n_sp, 2, chan), F32), V((rows, chan), BF16),
            V((n_tp, rows, chan), BF16), V((n_tp, 8, rows), F32), V((8, rows), F32),
            V((rows, cols), F32), V((rows, n_tp * cols), BF16),
            V((16, rows), BF16), V((rows, 128), F32), V((n_sp, 16, cap), BF16), V((n_sp, 16, cap), BF16),
            V((n_sp, rows), F32), V((n_sp, rows), F32), V((rows, n_sp), F32), V((rows, n_sp), F32),
            V((n_far, cap, cols), BF16), V((direct - 1, cap, n_tp * cols), BF16),
            V((n_sp, cap, n_tp * cols), BF16), V((n_sp, cap, hid), BF16),
            V((n_sp, cap, cols), F32), V((n_sp, cap, cols), BF16), V((n_sp, cap, cols), BF16),
            V((n_sp, cap, cols), BF16), V((n_sp, cap, cols), BF16),
            V((rows, n_tp * ff), BF16),
            sem((len(ins),)), sem((8,)),
        ] + [sem(s) for s in pairs for _ in range(2)],
        compiler_params=pltpu.CompilerParams(
            collective_id=0, has_side_effects=True, vmem_limit_bytes=60 * 1024 * 1024
        ),
    )(
        *ins, out_weight.reshape(n_tp, chan, cols), shared_gate, shared_up, expert_gate[0], expert_up[0],
        expert_down[0], shared_down,
    )


def solution(mesh):
    placed = (
        P("sp", "tp"),
        P("sp", "tp"),
        P(None, "tp"),
        P(None, "tp", None, None),
        P(None, "tp", None, None),
        P(None, "tp", None, None),
        P(None, "tp", None, None),
        P(None, "tp"),
        P(None, "sp", None, "tp"),
        P("sp", "tp"),
        P(None, "tp"),
        P("tp"),
        P(None, "tp"),
        P(None, "tp"),
        P(None, "tp"),
        P("sp", None, "tp"),
        P("sp", None, "tp"),
        P("sp", None, "tp"),
        P("sp", None),
        P("sp", None),
    )
    return jax.shard_map(
        shards, mesh=mesh, in_specs=placed, out_specs=P("sp", "tp"), check_vma=False
    )
```

```python
import functools

import jax
import jax.numpy as jnp
from jax import lax
from jax.experimental import pallas as pl
from jax.experimental.pallas import tpu as pltpu
from jax.sharding import PartitionSpec as P

MESH = pl.DeviceIdType.MESH
D = 2048
CONV = 4
NORM_EPS = 1e-06
RATE_SCALE = 8.0
SEG = 8
F32 = jnp.float32
BF16 = jnp.bfloat16
EXACT = lax.Precision.HIGHEST


def rcopy(src, dst, send, recv, **where):
    return pltpu.make_async_remote_copy(
        src_ref=src, dst_ref=dst, send_sem=send, recv_sem=recv, device_id=where, device_id_type=MESH
    )


def hello(n_sp, n_tp):
    sp, tp = lax.axis_index("sp"), lax.axis_index("tp")
    barrier = pltpu.get_barrier_semaphore()
    for k in range(1, n_sp):
        pl.semaphore_signal(
            barrier, inc=1, device_id={"sp": lax.rem(sp + k, n_sp)}, device_id_type=MESH
        )
    for k in range(1, n_tp):
        pl.semaphore_signal(
            barrier, inc=1, device_id={"tp": lax.rem(tp + k, n_tp)}, device_id_type=MESH
        )


def met(n_sp, n_tp):
    pl.semaphore_wait(pltpu.get_barrier_semaphore(), n_sp + n_tp - 2)


def gather_sems(n_tp):
    count = 6 if n_tp == 4 else n_tp
    return [pltpu.SemaphoreType.DMA((count,)), pltpu.SemaphoreType.DMA((count,))]


class Gather:
    def __init__(self, n_tp, slot, send, recv, base=0):
        self.n, self.slot, self.send, self.recv, self.base = n_tp, slot, send, recv, base
        self.t = lax.axis_index("tp")
        if n_tp == 4:
            y, x = self.t // 2, lax.rem(self.t, 2)
            self.xn, self.yn, self.dg = y * 2 + 1 - x, (1 - y) * 2 + x, 3 - self.t

    def piece(self, owner, half, sem, to):
        ref = self.slot(owner, half)
        s = self.base + sem
        return rcopy(ref, ref, self.send.at[s], self.recv.at[s], tp=to)

    def start(self):
        if self.n == 4:
            self.piece(self.t, 0, 0, self.xn).start()
            self.piece(self.t, 1, 3, self.yn).start()
            self.piece(self.t, 1, 1, self.xn).start()
            self.piece(self.t, 0, 2, self.yn).start()
        else:
            for k in range(1, self.n):
                to = lax.rem(self.t + k, self.n)
                self.piece(self.t, None, k, to).start()

    def forward(self):
        if self.n == 4:
            self.piece(self.xn, 0, 0, self.xn).wait_recv()
            self.piece(self.xn, 0, 4, self.yn).start()
            self.piece(self.yn, 1, 3, self.yn).wait_recv()
            self.piece(self.yn, 1, 5, self.xn).start()

    def arrivals(self):
        if self.n == 4:
            self.piece(self.xn, 1, 1, self.xn).wait_recv()
            yield self.xn
            self.piece(self.yn, 0, 2, self.yn).wait_recv()
            yield self.yn
            self.piece(self.dg, 0, 4, self.yn).wait_recv()
            self.piece(self.dg, 1, 5, self.xn).wait_recv()
            yield self.dg
        else:
            for k in range(1, self.n):
                owner = lax.rem(self.t - k + self.n, self.n)
                self.piece(owner, None, k, owner).wait_recv()
                yield owner

    def drain(self):
        if self.n == 4:
            for s, half, owner in (
                (0, 0, self.t), (1, 1, self.t), (2, 0, self.t), (3, 1, self.t),
                (4, 0, self.xn), (5, 1, self.yn),
            ):
                self.piece(owner, half, s, self.xn).wait_send()
        else:
            for k in range(1, self.n):
                to = lax.rem(self.t + k, self.n)
                self.piece(self.t, None, k, to).wait_send()


def logistic(x):
    return 0.5 * jnp.tanh(0.5 * x) + 0.5


class Order:
    def __init__(self, n_sp):
        sp = lax.axis_index("sp")
        chip = sp // 2
        self.core, self.low, self.high, self.n = sp % 2, chip % 2, chip // 2, n_sp // 4

    def at(self, p, sign):
        step = p // 4 + 1
        high = (self.high + (step if sign > 0 else 2 * self.n - step)) % self.n
        low = (self.low + 1 + p // 2) % 2
        return (high * 2 + low) * 2 + (self.core + 1 + p) % 2


class Square:
    def __init__(self):
        t, core = lax.axis_index("tp"), lax.axis_index("sp") % 2
        y, x = t // 2, t % 2
        xn, yn = y * 2 + 1 - x, (1 - y) * 2 + x
        flip = core == 1
        self.gather = jnp.where(flip, yn, xn)
        self.reduce = jnp.where(flip, xn, yn)
        self.place = jnp.where(flip, y, x)
        self.mine = (jnp.where(flip, x, 2 * y), jnp.where(flip, 2 + x, 2 * y + 1))
        self.theirs = (jnp.where(flip, 1 - x, 2 - 2 * y), jnp.where(flip, 3 - x, 3 - 2 * y))


def layer_kernel(
    n_sp, n_tp, cap, direct,
    h_rec, h_gate, h_convw, h_dw, h_dn, h_iw, h_inn, h_base, h_extra, h_tokens, h_gain, h_routes,
    h_rweight, hbm_outw, hbm_sg, hbm_su, hbm_eg, hbm_eu, hbm_ed, hbm_sd,
    out,
    rec, gate, convw, dw, dn, iw, inn, base, extra, tokens, gain, routes, rweight,
    outw, sg, su, eg, eu, ed, sd, permt, perm, wblk, exs,
    halo, cperm, gperm, av, bv, msg, totals, mixedp, mixed, squares, sqown,
    resid, whole, srow, scol, smsg, sgot, pos, wts, post, wtt,
    outgoing, outwide, rows_in, hidden, own, psend, precv, answer, returned, shid,
    isem, wsem, xsend, xrecv, hsend, hrecv, tsend, trecv, gsend, grecv, ssend, srecv, nsend, nrecv,
    dsend, drecv, asend, arecv, bsend, brecv, psem, prem, rsend, rrecv, csend, crecv, lsend, lrecv,
):
    two = n_tp == 4
    rows, chan = rec.shape
    heads, wide, narrow = dw.shape[1], dw.shape[2], dn.shape[2]
    groups, gw = wblk.shape[1], wblk.shape[2]
    cols = tokens.shape[1]
    ff = eg.shape[1]
    seglen = rows // SEG
    count = 6 if two else n_tp
    n_far = n_sp - direct
    sp, tp = lax.axis_index("sp"), lax.axis_index("tp")
    mine = pl.ds(pl.multiple_of(tp * cols, 128), cols)
    order = Order(n_sp)
    sq = Square() if two else None

    loads = []

    def load(a, b):
        c = pltpu.make_async_copy(a, b, wsem.at[len(loads)])
        c.start()
        loads.append(c)

    def band(i):
        return pl.ds(pl.multiple_of(i * ff, 128), ff)

    ready = []
    for i, (a, b) in enumerate((
        (h_rec, rec), (h_convw, convw), (h_extra, extra), (h_gate, gate), (h_dw, dw), (h_dn, dn),
        (h_iw, iw), (h_inn, inn), (h_base, base), (h_tokens, tokens), (h_gain, gain),
        (h_routes, routes), (h_rweight, rweight),
    )):
        c = pltpu.make_async_copy(a, b, isem.at[i])
        c.start()
        ready.append(c)
    hello(n_sp, n_tp)
    load(hbm_outw, outw)
    load(hbm_sg, sg)
    load(hbm_su, su)
    load(hbm_eg, eg)
    load(hbm_eu, eu)
    load(hbm_sd, sd)
    if two:
        for j in range(2):
            load(hbm_ed.at[band(sq.mine[j])], ed.at[0, pl.ds(j * ff, ff)])
    else:
        load(hbm_ed, ed)
    ready[0].wait()
    met(n_sp, n_tp)
    up, down = lax.rem(sp + 1, n_sp), lax.rem(sp + n_sp - 1, n_sp)
    low = rcopy(rec.at[pl.ds(rows - 16, 16)], halo.at[0], hsend.at[0], hrecv.at[0], sp=up)
    high = rcopy(rec.at[pl.ds(0, 16)], halo.at[1], hsend.at[1], hrecv.at[1], sp=down)
    low.start()
    high.start()
    swaps = []
    if two:
        for j in range(2):
            c = rcopy(
                hbm_ed.at[band(sq.theirs[j])], ed.at[1, pl.ds(j * ff, ff)],
                xsend.at[j], xrecv.at[j], tp=sq.reduce,
            )
            c.start()
            swaps.append(c)
    for c in ready[1:]:
        c.wait()

    r = lax.broadcasted_iota(jnp.int32, (rows, rows), 0)
    q = lax.broadcasted_iota(jnp.int32, (rows, rows), 1)
    permt[...] = jnp.where((r % SEG) * seglen + r // SEG == q, 1.0, 0.0).astype(BF16)
    perm[...] = jnp.where((q % SEG) * seglen + q // SEG == r, 1.0, 0.0).astype(BF16)
    wblk[...] = jnp.zeros_like(wblk)
    per = heads // groups
    for d in range(2):
        for k, (w, n) in enumerate(((dw, dn), (iw, inn))):
            for h in range(heads):
                a = (h % per) * (wide + narrow)
                b = a + wide
                wblk[2 * d + k, h // per, a:b, a:b] = w[d, h]
                wblk[2 * d + k, h // per, b : b + narrow, b : b + narrow] = n[d, h]
    for d in range(2):
        left, terms = jnp.concatenate([extra[d, 0], extra[d, 1]], axis=0), []
        for _ in range(3):
            terms.append(left.astype(BF16).astype(F32))
            left = left - terms[-1]
        exs[d] = lax.dot_general(
            permt[...], jnp.concatenate(terms, axis=0).astype(BF16), (((1,), (1,)), ((), ())),
            preferred_element_type=F32,
        ).astype(BF16)
    gperm[...] = jnp.dot(permt[...], gate[...], preferred_element_type=F32).astype(BF16)

    taps = convw[...].astype(F32)

    def convolve(padded, n):
        conv = padded[0:n] * taps[0:1, :]
        for j in range(1, CONV):
            conv = conv + padded[j : j + n] * taps[j : j + 1, :]
        return conv.astype(BF16)

    x = rec[...].astype(F32)
    gap = jnp.zeros((2, chan), F32)
    mixedp[...] = convolve(jnp.concatenate([gap, x, gap[0:1]], axis=0), rows)
    low.wait()
    high.wait()
    lo = jnp.where(sp > 0, halo[0].astype(F32), 0.0)
    hi = jnp.where(sp < n_sp - 1, halo[1].astype(F32), 0.0)
    first, last = rec[0:32, :].astype(F32), rec[rows - 32 : rows, :].astype(F32)
    mixedp[0:16, :] = convolve(jnp.concatenate([lo[14:16], first[0:17]], axis=0), 16)
    mixedp[rows - 16 : rows, :] = convolve(jnp.concatenate([last[14:32], hi[0:1]], axis=0), 16)
    cperm[...] = jnp.dot(permt[...], mixedp[...], preferred_element_type=F32).astype(BF16)

    hw = wide + narrow
    ch = lax.broadcasted_iota(jnp.int32, (6 * heads, chan), 1)
    head, within = ch // hw, ch % hw
    term = lax.broadcasted_iota(jnp.int32, (6 * heads, chan), 0) % (2 * heads)
    spread = jnp.where(term == jnp.where(within >= wide, heads, 0) + head, 1.0, 0.0).astype(BF16)
    cuts = ((0, wide), (wide, gw)) if per == 2 and wide % 128 == 0 else ((0, gw),)
    pieces = [(g, a, b) for g in range(groups) for a, b in cuts]
    step = rows // 2

    @pl.loop(0, rows // step)
    def _(r):
        at = pl.ds(pl.multiple_of(r * step, step), step)
        for d in range(2):
            ex = jnp.dot(exs[d, at, :], spread, preferred_element_type=F32)
            for g, a, b in pieces:
                lanes, blk = slice(g * gw + a, g * gw + b), slice(a, b)
                c = cperm[at, lanes]
                rate, admit = (
                    logistic(jnp.dot(c, wblk[2 * d + k, g, blk, blk], preferred_element_type=F32))
                    for k in range(2)
                )
                ld = jnp.minimum(ex[:, lanes] - rate * (RATE_SCALE * base[d : d + 1, lanes]), 0.0)
                a = jnp.exp(ld)
                bv[d, at, lanes] = jnp.sqrt(jnp.tanh(-ld) * (1.0 + a * a)) * admit * c.astype(F32)
                av[d, at, lanes] = a

    one = jnp.ones((SEG, chan), F32)
    zero = jnp.zeros((SEG, chan), F32)

    def advance(i, carry):
        got = []
        for d in range(2):
            at = pl.ds(pl.multiple_of((i if d == 0 else seglen - 1 - i) * SEG, SEG), SEG)
            a, b = av[d, at, :], bv[d, at, :]
            cum = carry[2 * d] * a
            state = a * carry[2 * d + 1] + b
            av[d, at, :] = cum
            bv[d, at, :] = state
            got += [cum, state]
        return tuple(got)

    ends = lax.fori_loop(0, seglen, advance, (one, zero, one, zero))

    def run(d, entering):
        seq = range(SEG) if d == 0 else range(SEG - 1, -1, -1)
        inside = [None] * SEG
        c = entering
        for s in seq:
            inside[s] = c
            c = ends[2 * d][s : s + 1] * c + ends[2 * d + 1][s : s + 1]
        return jnp.concatenate(inside, axis=0), c

    for d in range(2):
        prod = ends[2 * d][0:1]
        for s in range(1, SEG):
            prod = prod * ends[2 * d][s : s + 1]
        msg[d, 0:1, :] = prod
        msg[d, 1:2, :] = run(d, jnp.zeros((1, chan), F32))[1]
    sent = []
    for k in range(1, n_sp):
        to = lax.rem(sp + k, n_sp)
        c = rcopy(
            msg.at[jnp.where(to > sp, 0, 1)], totals.at[k], tsend.at[k], trecv.at[k], sp=to
        )
        c.start()
        sent.append(c)

    part = lax.broadcasted_iota(jnp.int32, (n_sp, rows), 0)
    who = jnp.zeros((n_sp, rows), jnp.int32)
    for p in range(n_sp):
        who = jnp.where(part == p, order.at(p, 1), who)
    hit0 = jnp.where(routes[0:1, :] == who, 1.0, 0.0)
    hit1 = jnp.where(routes[1:2, :] == who, 1.0, 0.0)
    earlier = jnp.where(r < q, 1.0, 0.0).astype(BF16)
    slots = jnp.dot((hit0 + hit1).astype(BF16), earlier, preferred_element_type=F32)
    pos[...] = jnp.where(hit0 + hit1 > 0.0, slots, -1.0)
    wts[...] = hit0 * rweight[0:1, :] + hit1 * rweight[1:2, :]
    post[...] = jnp.transpose(pos[...])
    wtt[...] = jnp.transpose(wts[...])

    @pl.loop(0, rows // 16)
    def _(r):
        at = pl.ds(pl.multiple_of(r * 16, 16), 16)
        bv[0, at, :] = bv[0, at, :] + bv[1, at, :]
        bv[1, at, :] = jax.nn.gelu(gperm[at, :].astype(F32))

    for c in sent:
        c.wait()
    carries = []
    zrow = jnp.zeros((1, chan), F32)
    c0, c1 = zrow, zrow
    for k in range(n_sp - 1, 0, -1):
        t = totals[k]
        c0 = jnp.where(k <= sp, t[0:1] * c0 + t[1:2], c0)
    for k in range(1, n_sp):
        t = totals[k]
        c1 = jnp.where(k > sp, t[0:1] * c1 + t[1:2], c1)
    for d, c in ((0, c0), (1, c1)):
        inside = run(d, c)[0]
        carries.append(jnp.concatenate([inside, inside], axis=0))

    @pl.loop(0, rows // 16)
    def _(r):
        at = pl.ds(pl.multiple_of(r * 16, 16), 16)
        total = bv[0, at, :] + av[0, at, :] * carries[0] + av[1, at, :] * carries[1]
        mixedp[at, :] = (total * bv[1, at, :]).astype(BF16)

    half, quarter = rows // 2, rows // 4

    def rows_of(i, part):
        return pl.ds(i * half, half) if part is None else pl.ds(i * half + part * quarter, quarter)

    def mixed_slot(i):
        return lambda owner, part: mixed.at[owner, rows_of(i, part)]

    def whole_slot(i):
        return lambda owner, part: whole.at[
            rows_of(i, part), pl.ds(pl.multiple_of(owner * cols, 128), cols)
        ]

    g = [Gather(n_tp, mixed_slot(i), gsend, grecv, base=i * count) for i in range(2)]
    w = [Gather(n_tp, whole_slot(i), nsend, nrecv, base=i * count) for i in range(2)]

    def project(owner, i):
        at = pl.ds(i * half, half)
        resid[at, :] += jnp.dot(mixed[owner, at, :], outw[owner], preferred_element_type=F32)

    def publish(i):
        at = pl.ds(i * half, half)
        whole[at, mine] = (resid[at, :] * gain[...]).astype(BF16)

    def unscramble(i):
        at = pl.ds(i * half, half)
        mixed[tp, at, :] = jnp.dot(
            perm[at, :], mixedp[...], preferred_element_type=F32
        ).astype(BF16)

    unscramble(0)
    g[0].start()
    unscramble(1)
    resid[...] = tokens[...].astype(F32)
    loads[0].wait()
    project(tp, 0)
    project(tp, 1)
    g[0].forward()
    g[1].start()
    for owner in g[0].arrivals():
        project(owner, 0)
    publish(0)
    g[1].forward()
    w[0].start()
    for owner in g[1].arrivals():
        project(owner, 1)
    publish(1)
    w[0].forward()
    r2 = resid[...] * resid[...]
    sqown[...] = lax.dot_general(
        jnp.ones((8, cols), F32), r2, (((1,), (1,)), ((), ())),
        precision=EXACT, preferred_element_type=F32,
    )
    sent = []
    for k in range(1, n_tp):
        c = rcopy(sqown, squares.at[k], ssend.at[k], srecv.at[k], tp=lax.rem(tp + k, n_tp))
        c.start()
        sent.append(c)
    w[1].start()

    slot = lax.broadcasted_iota(jnp.int32, (cap, rows), 0).astype(F32)

    def chosen(p):
        return jnp.where(pos[pl.ds(p, 1), :] == slot, 1.0, 0.0)

    def far_copy(p, sign):
        return rcopy(
            outgoing.at[p], rows_in.at[p, :, mine], dsend.at[p], drecv.at[p], sp=order.at(p, sign)
        )

    def near_copy(p, sign):
        return rcopy(
            outwide.at[p - n_far], rows_in.at[p], dsend.at[p], drecv.at[p], sp=order.at(p, sign)
        )

    def reply(p):
        return rcopy(answer.at[p], returned.at[p], rsend.at[p], rrecv.at[p], sp=order.at(p, -1))

    def scale_copy(p, sign):
        return rcopy(smsg.at[p], sgot.at[p], lsend.at[p], lrecv.at[p], sp=order.at(p, sign))

    def dispatch(p):
        outgoing[p] = jnp.dot(
            chosen(p).astype(BF16), whole[:, mine], preferred_element_type=F32
        ).astype(BF16)
        far_copy(p, 1).start()

    dispatch(0)
    total = sqown[...]
    for k, c in enumerate(sent):
        c.wait()
        total = total + squares[k + 1]
    w[1].forward()
    left = lax.rsqrt(total / (n_tp * cols) + NORM_EPS)
    line = lax.broadcasted_iota(jnp.int32, left.shape, 0)
    terms = jnp.zeros_like(left)
    for i in range(3):
        term = left.astype(BF16).astype(F32)
        terms = jnp.where(line == i, term, terms)
        left = left - term
    srow[...] = jnp.concatenate([terms, jnp.zeros_like(terms)], axis=0).astype(BF16)

    def scales(p):
        return lax.dot_general(
            srow[...], chosen(p).astype(BF16), (((1,), (1,)), ((), ())),
            preferred_element_type=F32,
        ).astype(BF16)

    def column(terms):
        return lax.dot_general(
            terms, jnp.ones((16, 128), BF16), (((0,), (0,)), ((), ())), preferred_element_type=F32
        )

    def tell(p):
        smsg[p] = scales(p)
        scale_copy(p, 1).start()

    tell(0)

    @pl.loop(1, n_far)
    def _(p):
        tell(p)
        dispatch(p)

    scol[...] = column(srow[...])
    for i in range(2):
        g[i].drain()

    def rows_gather(p):
        def place(owner, part):
            if part is None:
                return rows_in.at[p, :, pl.ds(pl.multiple_of(owner * cols, 128), cols)]
            first = pl.multiple_of(owner * cols + part * (cols // 2), 128)
            return rows_in.at[p, :, pl.ds(first, cols // 2)]

        return Gather(n_tp, place, asend, arecv, base=p * count)

    def begin_rows(p):
        far_copy(p, -1).wait_recv()
        rows_gather(p).start()

    def shared_slot(i):
        def place(owner, part):
            at = pl.ds(i * half, half)
            if part is None:
                return shid.at[at, band(owner)]
            return shid.at[at, pl.ds(pl.multiple_of(owner * ff + part * (ff // 2), 128), ff // 2)]

        return place

    shared = [Gather(n_tp, shared_slot(i), csend, crecv, base=i * count) for i in range(2)]

    def shared_units(i):
        at = pl.ds(i * half, half)
        x = whole[at, :]
        s = scol[at, 0:1]
        g = jnp.dot(x, sg[...], preferred_element_type=F32) * s
        u = jnp.dot(x, su[...], preferred_element_type=F32) * s
        shid[at, band(tp)] = (jax.nn.silu(g) * u).astype(BF16)
        shared[i].start()

    for owner in w[0].arrivals():
        pass
    for c in loads[1:]:
        c.wait()
    shared_units(0)
    for owner in w[1].arrivals():
        pass

    def wide_pick(p):
        return jnp.dot(
            chosen(p).astype(BF16), whole[...], preferred_element_type=F32
        ).astype(BF16)

    def near(p):
        outwide[p - n_far] = wide_pick(p)
        tell(p)
        near_copy(p, 1).start()

    if two:
        here = pl.ds(pl.multiple_of(sq.place * ff, 128), ff)

        def give_hidden(p):
            ref = hidden.at[p, :, here]
            return rcopy(ref, ref, bsend.at[p], brecv.at[p], tp=sq.gather)

        def take_hidden(p):
            ref = hidden.at[p, :, pl.ds(pl.multiple_of((1 - sq.place) * ff, 128), ff)]
            return rcopy(ref, ref, bsend.at[p], brecv.at[p], tp=sq.gather)

        def give_part(p):
            return rcopy(psend.at[p], precv.at[p], psem.at[p], prem.at[p], tp=sq.reduce)

    else:
        here = band(tp)

        def hidden_gather(p):
            def place(owner, part):
                return hidden.at[p, :, band(owner)]

            return Gather(n_tp, place, bsend, brecv, base=p * count)

    @pl.loop(n_far, n_sp - 2)
    def _(p):
        near(p)

    shared_units(1)
    shared[0].forward()
    near(n_sp - 2)
    rows_in[n_sp - 1] = wide_pick(n_sp - 1)
    sgot[n_sp - 1] = scales(n_sp - 1)
    shared[1].forward()
    begin_rows(0)
    begin_rows(1)
    rows_gather(0).forward()
    for i in range(2):
        w[i].drain()
    for c in swaps:
        c.wait()

    def answer_with(p, y):
        @pl.when(p == n_sp - 1)
        def _():
            returned[p] = y

        @pl.when(p < n_sp - 1)
        def _():
            answer[p] = y
            reply(p).start()

    def combine(p):
        @pl.when(p < n_sp - 1)
        def _():
            reply(p).wait_recv()

        which = lax.broadcasted_iota(jnp.int32, (rows, n_sp), 1) == p
        where = jnp.sum(jnp.where(which, post[...], 0.0), axis=1, keepdims=True)
        weight = jnp.sum(jnp.where(which, wtt[...], 0.0), axis=1, keepdims=True)
        lane = lax.broadcasted_iota(jnp.int32, (rows, cap), 1).astype(F32)
        hit = jnp.where(where == lane, 1.0, 0.0).astype(BF16)
        resid[...] += weight * jnp.dot(hit, returned[p], preferred_element_type=F32)

    def units(p):

        @pl.when(p < n_far)
        def _():
            for _ in rows_gather(p).arrivals():
                pass

        @pl.when((p >= n_far) & (p < n_sp - 1))
        def _():
            near_copy(p, -1).wait_recv()

        @pl.when(p < n_sp - 1)
        def _():
            scale_copy(p, -1).wait_recv()

        scale = column(sgot[p])[:, 0:1]
        x = rows_in[p]
        g = jnp.dot(x, eg[...], preferred_element_type=F32) * scale
        u = jnp.dot(x, eu[...], preferred_element_type=F32) * scale
        hidden[p, :, here] = (jax.nn.silu(g) * u).astype(BF16)
        if two:
            give_hidden(p).start()
        else:
            hidden_gather(p).start()

    back = 5

    @pl.loop(0, n_sp + 3)
    def _(s):
        @pl.when(s <= n_far)
        def _():
            units(s)

        @pl.when(s + 1 < n_far)
        def _():
            rows_gather(s + 1).forward()

        @pl.when((s >= 1) & (s < n_sp + 1))
        def _():
            p = s - 1
            if two:
                take_hidden(p).wait_recv()
                h = hidden[p]
                psend[p] = jnp.dot(h, ed[1], preferred_element_type=F32).astype(BF16)
                give_part(p).start()
                own[p] = jnp.dot(h, ed[0], preferred_element_type=F32)
            else:
                for _ in hidden_gather(p).arrivals():
                    pass
                answer_with(
                    p, jnp.dot(hidden[p], ed[...], preferred_element_type=F32).astype(BF16)
                )

        @pl.when((s >= n_far) & (s + 1 < n_sp))
        def _():
            units(s + 1)

        @pl.when(s + 2 < n_far)
        def _():
            begin_rows(s + 2)

        if two:
            @pl.when((s >= 2) & (s < n_sp + 2))
            def _():
                p = s - 2
                give_part(p).wait_recv()
                answer_with(p, (own[p] + precv[p].astype(F32)).astype(BF16))

        @pl.when(s == 2)
        def _():
            for i in range(2):
                for _ in shared[i].arrivals():
                    pass

            @pl.loop(0, rows // 128)
            def _(r):
                at = pl.ds(pl.multiple_of(r * 128, 128), 128)
                resid[at, :] += jnp.dot(shid[at, :], sd[...], preferred_element_type=F32)

        @pl.when(s >= back)
        def _():
            combine(s - back)

    for i in range(2):
        shared[i].drain()

    @pl.loop(0, n_sp)
    def _(p):
        if two:
            give_hidden(p).wait_send()
            give_part(p).wait_send()
        else:
            hidden_gather(p).drain()

        @pl.when(p < n_far)
        def _():
            rows_gather(p).drain()
            far_copy(p, 1).wait_send()

        @pl.when((p >= n_far) & (p < n_sp - 1))
        def _():
            near_copy(p, 1).wait_send()

        @pl.when(p < n_sp - 1)
        def _():
            reply(p).wait_send()
            scale_copy(p, 1).wait_send()

    @pl.loop(n_sp + 3 - back, n_sp)
    def _(s):
        combine(s)

    out[...] = resid[...].astype(BF16)


def shards(
    rec_input,
    gate_input,
    conv_weight,
    decay_wide,
    decay_narrow,
    input_wide,
    input_narrow,
    decay_base,
    decay_extra,
    tokens,
    out_weight,
    norm_gain,
    shared_gate,
    shared_up,
    shared_down,
    expert_gate,
    expert_up,
    expert_down,
    routes,
    route_weight,
):
    n_sp, n_tp = lax.axis_size("sp"), lax.axis_size("tp")
    rows, chan = rec_input.shape
    heads, wide, narrow = decay_wide.shape[1], decay_wide.shape[2], decay_narrow.shape[2]
    cols = tokens.shape[1]
    ff = shared_gate.shape[1]
    per = 2 if heads % 2 == 0 else 1
    hw = wide + narrow
    groups, gw = heads // per, per * hw
    cap = 3 * rows * routes.shape[1] // (2 * n_sp)
    direct = 4
    n_far = n_sp - direct
    two = n_tp == 4
    ex = decay_extra.transpose(0, 2, 3, 1)
    vm = pl.BlockSpec(memory_space=pltpu.VMEM)
    hbm = pl.BlockSpec(memory_space=pl.ANY)
    sem = pltpu.SemaphoreType.DMA
    count = 6 if two else n_tp
    down = (2, 2 * ff, cols) if two else (n_tp * ff, cols)
    hid = 2 * ff if two else n_tp * ff
    V = pltpu.VMEM
    pairs = [(2,), (2,), (n_sp,), (2 * count,), (n_tp,), (2 * count,), (n_sp,), (n_far * count,)]
    pairs += [(n_sp,) if two else (n_sp * count,), (n_sp,), (n_sp,), (2 * count,), (n_sp,)]
    ins = (
        rec_input, gate_input, conv_weight, decay_wide, decay_narrow, input_wide, input_narrow,
        decay_base, ex, tokens, norm_gain.reshape(1, cols), routes.T, route_weight.T,
    )
    return pl.pallas_call(
        functools.partial(layer_kernel, n_sp, n_tp, cap, direct),
        name="layer",
        out_shape=jax.ShapeDtypeStruct((rows, cols), BF16),
        in_specs=[hbm] * (len(ins) + 7),
        out_specs=vm,
        scratch_shapes=[V(a.shape, a.dtype) for a in ins] + [
            V((n_tp, chan, cols), BF16), V(shared_gate.shape, BF16), V(shared_up.shape, BF16),
            V(expert_gate.shape[1:], BF16), V(expert_up.shape[1:], BF16), V(down, BF16),
            V((n_tp * ff, cols), BF16),
            V((rows, rows), BF16), V((rows, rows), BF16), V((4, groups, gw, gw), BF16),
            V((2, rows, 6 * heads), BF16),
            V((2, 16, chan), BF16), V((rows, chan), BF16), V((rows, chan), BF16),
            V((2, rows, chan), F32), V((2, rows, chan), F32),
            V((2, 2, chan), F32), V((n_sp, 2, chan), F32), V((rows, chan), BF16),
            V((n_tp, rows, chan), BF16), V((n_tp, 8, rows), F32), V((8, rows), F32),
            V((rows, cols), F32), V((rows, n_tp * cols), BF16),
            V((16, rows), BF16), V((rows, 128), F32), V((n_sp, 16, cap), BF16), V((n_sp, 16, cap), BF16),
            V((n_sp, rows), F32), V((n_sp, rows), F32), V((rows, n_sp), F32), V((rows, n_sp), F32),
            V((n_far, cap, cols), BF16), V((direct - 1, cap, n_tp * cols), BF16),
            V((n_sp, cap, n_tp * cols), BF16), V((n_sp, cap, hid), BF16),
            V((n_sp, cap, cols), F32), V((n_sp, cap, cols), BF16), V((n_sp, cap, cols), BF16),
            V((n_sp, cap, cols), BF16), V((n_sp, cap, cols), BF16),
            V((rows, n_tp * ff), BF16),
            sem((len(ins),)), sem((8,)),
        ] + [sem(s) for s in pairs for _ in range(2)],
        compiler_params=pltpu.CompilerParams(
            collective_id=0, has_side_effects=True, vmem_limit_bytes=60 * 1024 * 1024
        ),
    )(
        *ins, out_weight.reshape(n_tp, chan, cols), shared_gate, shared_up, expert_gate[0], expert_up[0],
        expert_down[0], shared_down,
    )


def solution(mesh):
    placed = (
        P("sp", "tp"),
        P("sp", "tp"),
        P(None, "tp"),
        P(None, "tp", None, None),
        P(None, "tp", None, None),
        P(None, "tp", None, None),
        P(None, "tp", None, None),
        P(None, "tp"),
        P(None, "sp", None, "tp"),
        P("sp", "tp"),
        P(None, "tp"),
        P("tp"),
        P(None, "tp"),
        P(None, "tp"),
        P(None, "tp"),
        P("sp", None, "tp"),
        P("sp", None, "tp"),
        P("sp", None, "tp"),
        P("sp", None),
        P("sp", None),
    )
    return jax.shard_map(
        shards, mesh=mesh, in_specs=placed, out_specs=P("sp", "tp"), check_vma=False
    )
```

```python
import functools

import jax
import jax.numpy as jnp
from jax import lax
from jax.experimental import pallas as pl
from jax.experimental.pallas import tpu as pltpu
from jax.sharding import PartitionSpec as P

MESH = pl.DeviceIdType.MESH
D = 2048
CONV = 4
NORM_EPS = 1e-06
RATE_SCALE = 8.0
SEG = 8
F32 = jnp.float32
BF16 = jnp.bfloat16
EXACT = lax.Precision.HIGHEST


def rcopy(src, dst, send, recv, **where):
    return pltpu.make_async_remote_copy(
        src_ref=src, dst_ref=dst, send_sem=send, recv_sem=recv, device_id=where, device_id_type=MESH
    )


def hello(n_sp, n_tp):
    sp, tp = lax.axis_index("sp"), lax.axis_index("tp")
    barrier = pltpu.get_barrier_semaphore()
    for k in range(1, n_sp):
        pl.semaphore_signal(
            barrier, inc=1, device_id={"sp": lax.rem(sp + k, n_sp)}, device_id_type=MESH
        )
    for k in range(1, n_tp):
        pl.semaphore_signal(
            barrier, inc=1, device_id={"tp": lax.rem(tp + k, n_tp)}, device_id_type=MESH
        )


def met(n_sp, n_tp):
    pl.semaphore_wait(pltpu.get_barrier_semaphore(), n_sp + n_tp - 2)


def gather_sems(n_tp):
    count = 6 if n_tp == 4 else n_tp
    return [pltpu.SemaphoreType.DMA((count,)), pltpu.SemaphoreType.DMA((count,))]


class Gather:
    def __init__(self, n_tp, slot, send, recv, base=0):
        self.n, self.slot, self.send, self.recv, self.base = n_tp, slot, send, recv, base
        self.t = lax.axis_index("tp")
        if n_tp == 4:
            y, x = self.t // 2, lax.rem(self.t, 2)
            self.xn, self.yn, self.dg = y * 2 + 1 - x, (1 - y) * 2 + x, 3 - self.t

    def piece(self, owner, half, sem, to):
        ref = self.slot(owner, half)
        s = self.base + sem
        return rcopy(ref, ref, self.send.at[s], self.recv.at[s], tp=to)

    def start(self):
        if self.n == 4:
            self.piece(self.t, 0, 0, self.xn).start()
            self.piece(self.t, 1, 3, self.yn).start()
            self.piece(self.t, 1, 1, self.xn).start()
            self.piece(self.t, 0, 2, self.yn).start()
        else:
            for k in range(1, self.n):
                to = lax.rem(self.t + k, self.n)
                self.piece(self.t, None, k, to).start()

    def forward(self):
        if self.n == 4:
            self.piece(self.xn, 0, 0, self.xn).wait_recv()
            self.piece(self.xn, 0, 4, self.yn).start()
            self.piece(self.yn, 1, 3, self.yn).wait_recv()
            self.piece(self.yn, 1, 5, self.xn).start()

    def arrivals(self):
        if self.n == 4:
            self.piece(self.xn, 1, 1, self.xn).wait_recv()
            yield self.xn
            self.piece(self.yn, 0, 2, self.yn).wait_recv()
            yield self.yn
            self.piece(self.dg, 0, 4, self.yn).wait_recv()
            self.piece(self.dg, 1, 5, self.xn).wait_recv()
            yield self.dg
        else:
            for k in range(1, self.n):
                owner = lax.rem(self.t - k + self.n, self.n)
                self.piece(owner, None, k, owner).wait_recv()
                yield owner

    def drain(self):
        if self.n == 4:
            for s, half, owner in (
                (0, 0, self.t), (1, 1, self.t), (2, 0, self.t), (3, 1, self.t),
                (4, 0, self.xn), (5, 1, self.yn),
            ):
                self.piece(owner, half, s, self.xn).wait_send()
        else:
            for k in range(1, self.n):
                to = lax.rem(self.t + k, self.n)
                self.piece(self.t, None, k, to).wait_send()


def logistic(x):
    return 0.5 * jnp.tanh(0.5 * x) + 0.5


class Order:
    def __init__(self, n_sp):
        sp = lax.axis_index("sp")
        chip = sp // 2
        self.core, self.low, self.high, self.n = sp % 2, chip % 2, chip // 2, n_sp // 4

    def at(self, p, sign):
        step = p // 4 + 1
        high = (self.high + (step if sign > 0 else 2 * self.n - step)) % self.n
        low = (self.low + 1 + p // 2) % 2
        return (high * 2 + low) * 2 + (self.core + 1 + p) % 2


class Square:
    def __init__(self):
        t, core = lax.axis_index("tp"), lax.axis_index("sp") % 2
        y, x = t // 2, t % 2
        xn, yn = y * 2 + 1 - x, (1 - y) * 2 + x
        flip = core == 1
        self.gather = jnp.where(flip, yn, xn)
        self.reduce = jnp.where(flip, xn, yn)
        self.place = jnp.where(flip, y, x)
        self.mine = (jnp.where(flip, x, 2 * y), jnp.where(flip, 2 + x, 2 * y + 1))
        self.theirs = (jnp.where(flip, 1 - x, 2 - 2 * y), jnp.where(flip, 3 - x, 3 - 2 * y))


def layer_kernel(
    n_sp, n_tp, cap, direct,
    h_rec, h_gate, h_convw, h_dw, h_dn, h_iw, h_inn, h_base, h_extra, h_tokens, h_gain, h_routes,
    h_rweight, hbm_outw, hbm_sg, hbm_su, hbm_eg, hbm_eu, hbm_ed, hbm_sd,
    out,
    rec, gate, convw, dw, dn, iw, inn, base, extra, tokens, gain, routes, rweight,
    outw, sg, su, eg, eu, ed, sd, permt, perm, wblk, exs,
    halo, cperm, gperm, av, bv, msg, totals, mixedp, mixed, squares, sqown,
    resid, whole, srow, scol, smsg, sgot, pos, wts, post, wtt,
    outgoing, outwide, rows_in, hidden, own, psend, precv, answer, returned, shid,
    isem, wsem, xsend, xrecv, hsend, hrecv, tsend, trecv, gsend, grecv, ssend, srecv, nsend, nrecv,
    dsend, drecv, asend, arecv, bsend, brecv, psem, prem, rsend, rrecv, csend, crecv, lsend, lrecv,
):
    two = n_tp == 4
    rows, chan = rec.shape
    heads, wide, narrow = dw.shape[1], dw.shape[2], dn.shape[2]
    groups, gw = wblk.shape[1], wblk.shape[2]
    cols = tokens.shape[1]
    ff = eg.shape[1]
    seglen = rows // SEG
    count = 6 if two else n_tp
    n_far = n_sp - direct
    sp, tp = lax.axis_index("sp"), lax.axis_index("tp")
    mine = pl.ds(pl.multiple_of(tp * cols, 128), cols)
    order = Order(n_sp)
    sq = Square() if two else None

    loads = []

    def load(a, b):
        c = pltpu.make_async_copy(a, b, wsem.at[len(loads)])
        c.start()
        loads.append(c)

    def band(i):
        return pl.ds(pl.multiple_of(i * ff, 128), ff)

    ready = []
    for i, (a, b) in enumerate((
        (h_rec, rec), (h_convw, convw), (h_extra, extra), (h_gate, gate), (h_dw, dw), (h_dn, dn),
        (h_iw, iw), (h_inn, inn), (h_base, base), (h_tokens, tokens), (h_gain, gain),
        (h_routes, routes), (h_rweight, rweight),
    )):
        c = pltpu.make_async_copy(a, b, isem.at[i])
        c.start()
        ready.append(c)
    hello(n_sp, n_tp)
    load(hbm_outw, outw)
    load(hbm_sg, sg)
    load(hbm_su, su)
    load(hbm_eg, eg)
    load(hbm_eu, eu)
    load(hbm_sd, sd)
    if two:
        for j in range(2):
            load(hbm_ed.at[band(sq.mine[j])], ed.at[0, pl.ds(j * ff, ff)])
    else:
        load(hbm_ed, ed)
    ready[0].wait()
    met(n_sp, n_tp)
    up, down = lax.rem(sp + 1, n_sp), lax.rem(sp + n_sp - 1, n_sp)
    low = rcopy(rec.at[pl.ds(rows - 16, 16)], halo.at[0], hsend.at[0], hrecv.at[0], sp=up)
    high = rcopy(rec.at[pl.ds(0, 16)], halo.at[1], hsend.at[1], hrecv.at[1], sp=down)
    low.start()
    high.start()
    swaps = []
    if two:
        for j in range(2):
            c = rcopy(
                hbm_ed.at[band(sq.theirs[j])], ed.at[1, pl.ds(j * ff, ff)],
                xsend.at[j], xrecv.at[j], tp=sq.reduce,
            )
            c.start()
            swaps.append(c)
    for c in ready[1:]:
        c.wait()

    r = lax.broadcasted_iota(jnp.int32, (rows, rows), 0)
    q = lax.broadcasted_iota(jnp.int32, (rows, rows), 1)
    permt[...] = jnp.where((r % SEG) * seglen + r // SEG == q, 1.0, 0.0).astype(BF16)
    perm[...] = jnp.where((q % SEG) * seglen + q // SEG == r, 1.0, 0.0).astype(BF16)
    wblk[...] = jnp.zeros_like(wblk)
    per = heads // groups
    for d in range(2):
        for k, (w, n) in enumerate(((dw, dn), (iw, inn))):
            for h in range(heads):
                a = (h % per) * (wide + narrow)
                b = a + wide
                wblk[2 * d + k, h // per, a:b, a:b] = w[d, h]
                wblk[2 * d + k, h // per, b : b + narrow, b : b + narrow] = n[d, h]
    for d in range(2):
        left, terms = jnp.concatenate([extra[d, 0], extra[d, 1]], axis=0), []
        for _ in range(3):
            terms.append(left.astype(BF16).astype(F32))
            left = left - terms[-1]
        exs[d] = lax.dot_general(
            permt[...], jnp.concatenate(terms, axis=0).astype(BF16), (((1,), (1,)), ((), ())),
            preferred_element_type=F32,
        ).astype(BF16)
    gperm[...] = jnp.dot(permt[...], gate[...], preferred_element_type=F32).astype(BF16)

    taps = convw[...].astype(F32)

    def convolve(padded, n):
        conv = padded[0:n] * taps[0:1, :]
        for j in range(1, CONV):
            conv = conv + padded[j : j + n] * taps[j : j + 1, :]
        return conv.astype(BF16)

    x = rec[...].astype(F32)
    gap = jnp.zeros((2, chan), F32)
    mixedp[...] = convolve(jnp.concatenate([gap, x, gap[0:1]], axis=0), rows)
    low.wait()
    high.wait()
    lo = jnp.where(sp > 0, halo[0].astype(F32), 0.0)
    hi = jnp.where(sp < n_sp - 1, halo[1].astype(F32), 0.0)
    first, last = rec[0:32, :].astype(F32), rec[rows - 32 : rows, :].astype(F32)
    mixedp[0:16, :] = convolve(jnp.concatenate([lo[14:16], first[0:17]], axis=0), 16)
    mixedp[rows - 16 : rows, :] = convolve(jnp.concatenate([last[14:32], hi[0:1]], axis=0), 16)
    cperm[...] = jnp.dot(permt[...], mixedp[...], preferred_element_type=F32).astype(BF16)

    hw = wide + narrow
    ch = lax.broadcasted_iota(jnp.int32, (6 * heads, chan), 1)
    head, within = ch // hw, ch % hw
    term = lax.broadcasted_iota(jnp.int32, (6 * heads, chan), 0) % (2 * heads)
    spread = jnp.where(term == jnp.where(within >= wide, heads, 0) + head, 1.0, 0.0).astype(BF16)
    cuts = ((0, wide), (wide, gw)) if per == 2 and wide % 128 == 0 else ((0, gw),)
    pieces = [(g, a, b) for g in range(groups) for a, b in cuts]
    step = rows // 2

    @pl.loop(0, rows // step)
    def _(r):
        at = pl.ds(pl.multiple_of(r * step, step), step)
        for d in range(2):
            ex = jnp.dot(exs[d, at, :], spread, preferred_element_type=F32)
            for g, a, b in pieces:
                lanes, blk = slice(g * gw + a, g * gw + b), slice(a, b)
                c = cperm[at, lanes]
                rate, admit = (
                    logistic(jnp.dot(c, wblk[2 * d + k, g, blk, blk], preferred_element_type=F32))
                    for k in range(2)
                )
                ld = jnp.minimum(ex[:, lanes] - rate * (RATE_SCALE * base[d : d + 1, lanes]), 0.0)
                a = jnp.exp(ld)
                bv[d, at, lanes] = jnp.sqrt(jnp.tanh(-ld) * (1.0 + a * a)) * admit * c.astype(F32)
                av[d, at, lanes] = a

    one = jnp.ones((SEG, chan), F32)
    zero = jnp.zeros((SEG, chan), F32)

    def advance(i, carry):
        got = []
        for d in range(2):
            at = pl.ds(pl.multiple_of((i if d == 0 else seglen - 1 - i) * SEG, SEG), SEG)
            a, b = av[d, at, :], bv[d, at, :]
            cum = carry[2 * d] * a
            state = a * carry[2 * d + 1] + b
            av[d, at, :] = cum
            bv[d, at, :] = state
            got += [cum, state]
        return tuple(got)

    ends = lax.fori_loop(0, seglen, advance, (one, zero, one, zero))

    def run(d, entering):
        seq = range(SEG) if d == 0 else range(SEG - 1, -1, -1)
        inside = [None] * SEG
        c = entering
        for s in seq:
            inside[s] = c
            c = ends[2 * d][s : s + 1] * c + ends[2 * d + 1][s : s + 1]
        return jnp.concatenate(inside, axis=0), c

    for d in range(2):
        prod = ends[2 * d][0:1]
        for s in range(1, SEG):
            prod = prod * ends[2 * d][s : s + 1]
        msg[d, 0:1, :] = prod
        msg[d, 1:2, :] = run(d, jnp.zeros((1, chan), F32))[1]
    sent = []
    for k in range(1, n_sp):
        to = lax.rem(sp + k, n_sp)
        c = rcopy(
            msg.at[jnp.where(to > sp, 0, 1)], totals.at[k], tsend.at[k], trecv.at[k], sp=to
        )
        c.start()
        sent.append(c)

    part = lax.broadcasted_iota(jnp.int32, (n_sp, rows), 0)
    who = jnp.zeros((n_sp, rows), jnp.int32)
    for p in range(n_sp):
        who = jnp.where(part == p, order.at(p, 1), who)
    hit0 = jnp.where(routes[0:1, :] == who, 1.0, 0.0)
    hit1 = jnp.where(routes[1:2, :] == who, 1.0, 0.0)
    earlier = jnp.where(r < q, 1.0, 0.0).astype(BF16)
    slots = jnp.dot((hit0 + hit1).astype(BF16), earlier, preferred_element_type=F32)
    pos[...] = jnp.where(hit0 + hit1 > 0.0, slots, -1.0)
    wts[...] = hit0 * rweight[0:1, :] + hit1 * rweight[1:2, :]
    post[...] = jnp.transpose(pos[...])
    wtt[...] = jnp.transpose(wts[...])

    @pl.loop(0, rows // 16)
    def _(r):
        at = pl.ds(pl.multiple_of(r * 16, 16), 16)
        bv[0, at, :] = bv[0, at, :] + bv[1, at, :]
        bv[1, at, :] = jax.nn.gelu(gperm[at, :].astype(F32))

    for c in sent:
        c.wait()
    carries = []
    zrow = jnp.zeros((1, chan), F32)
    c0, c1 = zrow, zrow
    for k in range(n_sp - 1, 0, -1):
        t = totals[k]
        c0 = jnp.where(k <= sp, t[0:1] * c0 + t[1:2], c0)
    for k in range(1, n_sp):
        t = totals[k]
        c1 = jnp.where(k > sp, t[0:1] * c1 + t[1:2], c1)
    for d, c in ((0, c0), (1, c1)):
        inside = run(d, c)[0]
        carries.append(jnp.concatenate([inside, inside], axis=0))

    @pl.loop(0, rows // 16)
    def _(r):
        at = pl.ds(pl.multiple_of(r * 16, 16), 16)
        total = bv[0, at, :] + av[0, at, :] * carries[0] + av[1, at, :] * carries[1]
        mixedp[at, :] = (total * bv[1, at, :]).astype(BF16)

    half, quarter = rows // 2, rows // 4

    def rows_of(i, part):
        return pl.ds(i * half, half) if part is None else pl.ds(i * half + part * quarter, quarter)

    def mixed_slot(i):
        return lambda owner, part: mixed.at[owner, rows_of(i, part)]

    def whole_slot(i):
        return lambda owner, part: whole.at[
            rows_of(i, part), pl.ds(pl.multiple_of(owner * cols, 128), cols)
        ]

    g = [Gather(n_tp, mixed_slot(i), gsend, grecv, base=i * count) for i in range(2)]
    w = [Gather(n_tp, whole_slot(i), nsend, nrecv, base=i * count) for i in range(2)]

    def project(owner, i):
        at = pl.ds(i * half, half)
        resid[at, :] += jnp.dot(mixed[owner, at, :], outw[owner], preferred_element_type=F32)

    def publish(i):
        at = pl.ds(i * half, half)
        whole[at, mine] = (resid[at, :] * gain[...]).astype(BF16)

    def unscramble(i):
        at = pl.ds(i * half, half)
        mixed[tp, at, :] = jnp.dot(
            perm[at, :], mixedp[...], preferred_element_type=F32
        ).astype(BF16)

    unscramble(0)
    g[0].start()
    unscramble(1)
    resid[...] = tokens[...].astype(F32)
    loads[0].wait()
    project(tp, 0)
    project(tp, 1)
    g[0].forward()
    g[1].start()
    for owner in g[0].arrivals():
        project(owner, 0)
    publish(0)
    g[1].forward()
    w[0].start()
    for owner in g[1].arrivals():
        project(owner, 1)
    publish(1)
    w[0].forward()
    r2 = resid[...] * resid[...]
    sqown[...] = lax.dot_general(
        jnp.ones((8, cols), F32), r2, (((1,), (1,)), ((), ())),
        precision=EXACT, preferred_element_type=F32,
    )
    sent = []
    for k in range(1, n_tp):
        c = rcopy(sqown, squares.at[k], ssend.at[k], srecv.at[k], tp=lax.rem(tp + k, n_tp))
        c.start()
        sent.append(c)
    w[1].start()

    slot = lax.broadcasted_iota(jnp.int32, (cap, rows), 0).astype(F32)

    def chosen(p):
        return jnp.where(pos[pl.ds(p, 1), :] == slot, 1.0, 0.0)

    def far_copy(p, sign):
        return rcopy(
            outgoing.at[p], rows_in.at[p, :, mine], dsend.at[p], drecv.at[p], sp=order.at(p, sign)
        )

    def near_copy(p, sign):
        return rcopy(
            outwide.at[p - n_far], rows_in.at[p], dsend.at[p], drecv.at[p], sp=order.at(p, sign)
        )

    def reply(p):
        return rcopy(answer.at[p], returned.at[p], rsend.at[p], rrecv.at[p], sp=order.at(p, -1))

    def scale_copy(p, sign):
        return rcopy(smsg.at[p], sgot.at[p], lsend.at[p], lrecv.at[p], sp=order.at(p, sign))

    def dispatch(p):
        outgoing[p] = jnp.dot(
            chosen(p).astype(BF16), whole[:, mine], preferred_element_type=F32
        ).astype(BF16)
        far_copy(p, 1).start()

    dispatch(0)
    total = sqown[...]
    for k, c in enumerate(sent):
        c.wait()
        total = total + squares[k + 1]
    w[1].forward()
    left = lax.rsqrt(total / (n_tp * cols) + NORM_EPS)
    line = lax.broadcasted_iota(jnp.int32, left.shape, 0)
    terms = jnp.zeros_like(left)
    for i in range(3):
        term = left.astype(BF16).astype(F32)
        terms = jnp.where(line == i, term, terms)
        left = left - term
    srow[...] = jnp.concatenate([terms, jnp.zeros_like(terms)], axis=0).astype(BF16)

    def scales(p):
        return lax.dot_general(
            srow[...], chosen(p).astype(BF16), (((1,), (1,)), ((), ())),
            preferred_element_type=F32,
        ).astype(BF16)

    def column(terms):
        return lax.dot_general(
            terms, jnp.ones((16, 128), BF16), (((0,), (0,)), ((), ())), preferred_element_type=F32
        )

    def tell(p):
        smsg[p] = scales(p)
        scale_copy(p, 1).start()

    tell(0)

    @pl.loop(1, n_far)
    def _(p):
        tell(p)
        dispatch(p)

    scol[...] = column(srow[...])
    for i in range(2):
        g[i].drain()

    def rows_gather(p):
        def place(owner, part):
            if part is None:
                return rows_in.at[p, :, pl.ds(pl.multiple_of(owner * cols, 128), cols)]
            first = pl.multiple_of(owner * cols + part * (cols // 2), 128)
            return rows_in.at[p, :, pl.ds(first, cols // 2)]

        return Gather(n_tp, place, asend, arecv, base=p * count)

    def begin_rows(p):
        far_copy(p, -1).wait_recv()
        rows_gather(p).start()

    def shared_slot(i):
        def place(owner, part):
            at = pl.ds(i * half, half)
            if part is None:
                return shid.at[at, band(owner)]
            return shid.at[at, pl.ds(pl.multiple_of(owner * ff + part * (ff // 2), 128), ff // 2)]

        return place

    shared = [Gather(n_tp, shared_slot(i), csend, crecv, base=i * count) for i in range(2)]

    def shared_units(i):
        at = pl.ds(i * half, half)
        x = whole[at, :]
        s = scol[at, 0:1]
        g = jnp.dot(x, sg[...], preferred_element_type=F32) * s
        u = jnp.dot(x, su[...], preferred_element_type=F32) * s
        shid[at, band(tp)] = (jax.nn.silu(g) * u).astype(BF16)
        shared[i].start()

    for owner in w[0].arrivals():
        pass
    for c in loads[1:]:
        c.wait()
    shared_units(0)
    for owner in w[1].arrivals():
        pass

    def wide_pick(p):
        return jnp.dot(
            chosen(p).astype(BF16), whole[...], preferred_element_type=F32
        ).astype(BF16)

    def near(p):
        outwide[p - n_far] = wide_pick(p)
        tell(p)
        near_copy(p, 1).start()

    if two:
        here = pl.ds(pl.multiple_of(sq.place * ff, 128), ff)

        def give_hidden(p):
            ref = hidden.at[p, :, here]
            return rcopy(ref, ref, bsend.at[p], brecv.at[p], tp=sq.gather)

        def take_hidden(p):
            ref = hidden.at[p, :, pl.ds(pl.multiple_of((1 - sq.place) * ff, 128), ff)]
            return rcopy(ref, ref, bsend.at[p], brecv.at[p], tp=sq.gather)

        def give_part(p):
            return rcopy(psend.at[p], precv.at[p], psem.at[p], prem.at[p], tp=sq.reduce)

    else:
        here = band(tp)

        def hidden_gather(p):
            def place(owner, part):
                return hidden.at[p, :, band(owner)]

            return Gather(n_tp, place, bsend, brecv, base=p * count)

    @pl.loop(n_far, n_sp - 2)
    def _(p):
        near(p)

    shared_units(1)
    shared[0].forward()
    near(n_sp - 2)
    rows_in[n_sp - 1] = wide_pick(n_sp - 1)
    sgot[n_sp - 1] = scales(n_sp - 1)
    shared[1].forward()
    begin_rows(0)
    rows_gather(0).forward()
    begin_rows(1)
    for i in range(2):
        w[i].drain()
    for c in swaps:
        c.wait()

    def answer_with(p, y):
        @pl.when(p == n_sp - 1)
        def _():
            returned[p] = y

        @pl.when(p < n_sp - 1)
        def _():
            answer[p] = y
            reply(p).start()

    def combine(p):
        @pl.when(p < n_sp - 1)
        def _():
            reply(p).wait_recv()

        which = lax.broadcasted_iota(jnp.int32, (rows, n_sp), 1) == p
        where = jnp.sum(jnp.where(which, post[...], 0.0), axis=1, keepdims=True)
        weight = jnp.sum(jnp.where(which, wtt[...], 0.0), axis=1, keepdims=True)
        lane = lax.broadcasted_iota(jnp.int32, (rows, cap), 1).astype(F32)
        hit = jnp.where(where == lane, 1.0, 0.0).astype(BF16)
        resid[...] += weight * jnp.dot(hit, returned[p], preferred_element_type=F32)

    def units(p):

        @pl.when(p < n_far)
        def _():
            for _ in rows_gather(p).arrivals():
                pass

        @pl.when((p >= n_far) & (p < n_sp - 1))
        def _():
            near_copy(p, -1).wait_recv()

        @pl.when(p < n_sp - 1)
        def _():
            scale_copy(p, -1).wait_recv()

        scale = column(sgot[p])[:, 0:1]
        x = rows_in[p]
        g = jnp.dot(x, eg[...], preferred_element_type=F32) * scale
        u = jnp.dot(x, eu[...], preferred_element_type=F32) * scale
        hidden[p, :, here] = (jax.nn.silu(g) * u).astype(BF16)
        if two:
            give_hidden(p).start()
        else:
            hidden_gather(p).start()

    back = 5

    @pl.loop(0, n_sp + 3)
    def _(s):
        @pl.when(s <= n_far)
        def _():
            units(s)

        @pl.when(s + 1 < n_far)
        def _():
            rows_gather(s + 1).forward()

        @pl.when((s >= 1) & (s < n_sp + 1))
        def _():
            p = s - 1
            if two:
                take_hidden(p).wait_recv()
                h = hidden[p]
                psend[p] = jnp.dot(h, ed[1], preferred_element_type=F32).astype(BF16)
                give_part(p).start()
                own[p] = jnp.dot(h, ed[0], preferred_element_type=F32)
            else:
                for _ in hidden_gather(p).arrivals():
                    pass
                answer_with(
                    p, jnp.dot(hidden[p], ed[...], preferred_element_type=F32).astype(BF16)
                )

        @pl.when((s >= n_far) & (s + 1 < n_sp))
        def _():
            units(s + 1)

        @pl.when(s + 2 < n_far)
        def _():
            begin_rows(s + 2)

        if two:
            @pl.when((s >= 2) & (s < n_sp + 2))
            def _():
                p = s - 2
                give_part(p).wait_recv()
                answer_with(p, (own[p] + precv[p].astype(F32)).astype(BF16))

        @pl.when(s == 2)
        def _():
            for i in range(2):
                for _ in shared[i].arrivals():
                    pass

            @pl.loop(0, rows // 128)
            def _(r):
                at = pl.ds(pl.multiple_of(r * 128, 128), 128)
                resid[at, :] += jnp.dot(shid[at, :], sd[...], preferred_element_type=F32)

        @pl.when(s >= back)
        def _():
            combine(s - back)

    for i in range(2):
        shared[i].drain()

    @pl.loop(0, n_sp)
    def _(p):
        if two:
            give_hidden(p).wait_send()
            give_part(p).wait_send()
        else:
            hidden_gather(p).drain()

        @pl.when(p < n_far)
        def _():
            rows_gather(p).drain()
            far_copy(p, 1).wait_send()

        @pl.when((p >= n_far) & (p < n_sp - 1))
        def _():
            near_copy(p, 1).wait_send()

        @pl.when(p < n_sp - 1)
        def _():
            reply(p).wait_send()
            scale_copy(p, 1).wait_send()

    @pl.loop(n_sp + 3 - back, n_sp)
    def _(s):
        combine(s)

    out[...] = resid[...].astype(BF16)


def shards(
    rec_input,
    gate_input,
    conv_weight,
    decay_wide,
    decay_narrow,
    input_wide,
    input_narrow,
    decay_base,
    decay_extra,
    tokens,
    out_weight,
    norm_gain,
    shared_gate,
    shared_up,
    shared_down,
    expert_gate,
    expert_up,
    expert_down,
    routes,
    route_weight,
):
    n_sp, n_tp = lax.axis_size("sp"), lax.axis_size("tp")
    rows, chan = rec_input.shape
    heads, wide, narrow = decay_wide.shape[1], decay_wide.shape[2], decay_narrow.shape[2]
    cols = tokens.shape[1]
    ff = shared_gate.shape[1]
    per = 2 if heads % 2 == 0 else 1
    hw = wide + narrow
    groups, gw = heads // per, per * hw
    cap = 3 * rows * routes.shape[1] // (2 * n_sp)
    direct = 4
    n_far = n_sp - direct
    two = n_tp == 4
    ex = decay_extra.transpose(0, 2, 3, 1)
    vm = pl.BlockSpec(memory_space=pltpu.VMEM)
    hbm = pl.BlockSpec(memory_space=pl.ANY)
    sem = pltpu.SemaphoreType.DMA
    count = 6 if two else n_tp
    down = (2, 2 * ff, cols) if two else (n_tp * ff, cols)
    hid = 2 * ff if two else n_tp * ff
    V = pltpu.VMEM
    pairs = [(2,), (2,), (n_sp,), (2 * count,), (n_tp,), (2 * count,), (n_sp,), (n_far * count,)]
    pairs += [(n_sp,) if two else (n_sp * count,), (n_sp,), (n_sp,), (2 * count,), (n_sp,)]
    ins = (
        rec_input, gate_input, conv_weight, decay_wide, decay_narrow, input_wide, input_narrow,
        decay_base, ex, tokens, norm_gain.reshape(1, cols), routes.T, route_weight.T,
    )
    return pl.pallas_call(
        functools.partial(layer_kernel, n_sp, n_tp, cap, direct),
        name="layer",
        out_shape=jax.ShapeDtypeStruct((rows, cols), BF16),
        in_specs=[hbm] * (len(ins) + 7),
        out_specs=vm,
        scratch_shapes=[V(a.shape, a.dtype) for a in ins] + [
            V((n_tp, chan, cols), BF16), V(shared_gate.shape, BF16), V(shared_up.shape, BF16),
            V(expert_gate.shape[1:], BF16), V(expert_up.shape[1:], BF16), V(down, BF16),
            V((n_tp * ff, cols), BF16),
            V((rows, rows), BF16), V((rows, rows), BF16), V((4, groups, gw, gw), BF16),
            V((2, rows, 6 * heads), BF16),
            V((2, 16, chan), BF16), V((rows, chan), BF16), V((rows, chan), BF16),
            V((2, rows, chan), F32), V((2, rows, chan), F32),
            V((2, 2, chan), F32), V((n_sp, 2, chan), F32), V((rows, chan), BF16),
            V((n_tp, rows, chan), BF16), V((n_tp, 8, rows), F32), V((8, rows), F32),
            V((rows, cols), F32), V((rows, n_tp * cols), BF16),
            V((16, rows), BF16), V((rows, 128), F32), V((n_sp, 16, cap), BF16), V((n_sp, 16, cap), BF16),
            V((n_sp, rows), F32), V((n_sp, rows), F32), V((rows, n_sp), F32), V((rows, n_sp), F32),
            V((n_far, cap, cols), BF16), V((direct - 1, cap, n_tp * cols), BF16),
            V((n_sp, cap, n_tp * cols), BF16), V((n_sp, cap, hid), BF16),
            V((n_sp, cap, cols), F32), V((n_sp, cap, cols), BF16), V((n_sp, cap, cols), BF16),
            V((n_sp, cap, cols), BF16), V((n_sp, cap, cols), BF16),
            V((rows, n_tp * ff), BF16),
            sem((len(ins),)), sem((8,)),
        ] + [sem(s) for s in pairs for _ in range(2)],
        compiler_params=pltpu.CompilerParams(
            collective_id=0, has_side_effects=True, vmem_limit_bytes=60 * 1024 * 1024
        ),
    )(
        *ins, out_weight.reshape(n_tp, chan, cols), shared_gate, shared_up, expert_gate[0], expert_up[0],
        expert_down[0], shared_down,
    )


def solution(mesh):
    placed = (
        P("sp", "tp"),
        P("sp", "tp"),
        P(None, "tp"),
        P(None, "tp", None, None),
        P(None, "tp", None, None),
        P(None, "tp", None, None),
        P(None, "tp", None, None),
        P(None, "tp"),
        P(None, "sp", None, "tp"),
        P("sp", "tp"),
        P(None, "tp"),
        P("tp"),
        P(None, "tp"),
        P(None, "tp"),
        P(None, "tp"),
        P("sp", None, "tp"),
        P("sp", None, "tp"),
        P("sp", None, "tp"),
        P("sp", None),
        P("sp", None),
    )
    return jax.shard_map(
        shards, mesh=mesh, in_specs=placed, out_specs=P("sp", "tp"), check_vma=False
    )
```
